32 devices in a mesh: sp: 8 (over z, y), tp: 4 (over x, core).
Axes of the slice: x: 2, y: 2, z: 4, core: 2. Of those that a mesh axis runs over, the one named last changes fastest.
Arguments:
- tokens: bfloat16 [8192, 2048], P('sp'), may hold values from -6 to 6
- norm_gain: bfloat16 [2048], replicated, may hold values from 0.099609375 to 1.8984375
- query_weight: bfloat16 [2048, 2048], P(None, 'tp'), may hold values from -0.125 to 0.125
- key_weight: bfloat16 [2048, 512], P(None, 'tp'), may hold values from -0.125 to 0.125
- value_weight: bfloat16 [2048, 512], P(None, 'tp'), may hold values from -0.125 to 0.125
- query_gain: float32 [64], replicated, may hold values from 1 to 14
- key_gain: float32 [64], replicated, may hold values from 1 to 14
- sink_logit: float32 [32], P('tp'), may hold values from 4 to 10
- gate_weight: bfloat16 [2048, 4096], P(None, 'tp'), may hold values from -0.125 to 0.125
- inner_weight: bfloat16 [2048, 4096], P(None, 'tp'), may hold values from -0.125 to 0.125
- input_map: bfloat16 [2048, 1024], P(None, 'tp'), may hold values from -0.125 to 0.125
- output_map: bfloat16 [2048, 1024], P(None, 'tp'), may hold values from -0.125 to 0.125
- step_weight: bfloat16 [2048, 2, 64], P(None, None, 'tp'), may hold values from -0.125 to 0.125
- conv_inner: bfloat16 [5, 4096], P(None, 'tp'), may hold values from -2.5 to 2.5
- conv_pair: bfloat16 [5, 2, 1024], P(None, None, 'tp'), may hold values from -2.5 to 2.5
- decay_rate: float32 [2, 64], P(None, 'tp'), may hold values from 3.6621094e-06 to 0.05
- decay_jump: float32 [8192, 2, 64], P('sp', None, 'tp'), may hold values from -1.4001709 to 0
- inner_gain: bfloat16 [4096], P('tp'), may hold values from 0.099609375 to 1.8984375
- attn_out_weight: bfloat16 [2048, 2048], P('tp'), may hold values from -0.25 to 0.25
- ssm_out_weight: bfloat16 [4096, 2048], P('tp'), may hold values from -0.09375 to 0.09375
Outputs:
- mixed: bfloat16 [8192, 2048], P(('sp', 'tp'))
The draws below stay inside these ranges and needn't reach their ends.
All inputs are finite; a program needn't handle non-finite values.
Results may differ from the reference program's by a relative error of at most 0.025.
The reference program's roundings to bfloat16 on the way count: a program that leaves them out, or rounds other values in their place, can miss the bound.
Values may be sent and summed in bfloat16 or wider, within the bound.
A program may use at most 128 MiB of HBM per device.

```python
import math
import jax
import jax.numpy as jnp
from jax import lax

MODEL_WIDTH = 2048
HEAD_SIZE = 64
QUERY_HEADS = 32
KEY_HEADS = 8
SSM_INNER = 4096
SSM_GROUPS = 8
STATE_SIZE = 128
CONV_TAPS = 5
WINDOW = 128
BLOCK_ROWS = 256
LOCAL_TOKENS = 1024
DUALITY_CHANNELS = 64
ORDERED_ENTRIES = 8192
N_TP = 4


def draw_query_gain(key, part):
    gain_key = jax.random.fold_in(key, 11)
    return jax.random.uniform(gain_key, (HEAD_SIZE,), jnp.float32, 1.0, 2.0)


def draw_key_gain(key, part):
    gain_key = jax.random.fold_in(key, 17)
    return jax.random.uniform(gain_key, (HEAD_SIZE,), jnp.float32, 1.0, 2.0)


def draw_decay_rate(key, part):
    coin_key, fast_key, slow_key = jax.random.split(jax.random.fold_in(key, 23), 3)
    shape_pair = (2, DUALITY_CHANNELS)
    fast_rate = jnp.exp(jax.random.uniform(fast_key, shape_pair, jnp.float32, math.log(0.015), math.log(0.05)))
    slow_rate = jnp.exp(jax.random.uniform(slow_key, shape_pair, jnp.float32, math.log(0.05 / ORDERED_ENTRIES), math.log(0.3 / ORDERED_ENTRIES)))
    picked = jax.random.bernoulli(coin_key, 0.5, shape_pair)
    return jnp.where(picked, fast_rate, slow_rate)


def draw_decay_jump(key, part):
    pace_key, spot_key, depth_key = jax.random.split(jax.random.fold_in(key, 37), 3)
    columns = 2 * DUALITY_CHANNELS
    blocks = ORDERED_ENTRIES // BLOCK_ROWS
    pace = jax.random.uniform(pace_key, (blocks, 1, columns), jnp.float32, 0.0, 1.4 / ORDERED_ENTRIES)
    increment_matrix_lines = jnp.broadcast_to(pace, (blocks, BLOCK_ROWS, columns)).reshape(ORDERED_ENTRIES, columns)
    drawn_locations = jax.random.randint(spot_key, (2, columns), 0, ORDERED_ENTRIES, dtype=jnp.int32)
    stack_level_count = jnp.log(jax.random.uniform(depth_key, (2, columns), jnp.float32, 0.5, 0.8))
    entry_ordinal = jnp.arange(ORDERED_ENTRIES, dtype=jnp.int32)[:, None]
    cluster_bunches = jnp.where(entry_ordinal == drawn_locations[0][None, :], stack_level_count[0][None, :], 0.0)
    cluster_bunches = cluster_bunches + jnp.where(entry_ordinal == drawn_locations[1][None, :], stack_level_count[1][None, :], 0.0)
    return (cluster_bunches - increment_matrix_lines).reshape(ORDERED_ENTRIES, 2, DUALITY_CHANNELS)


def shard_levels(key, dims, shards, smallest, high):
    loudness, own = 1.0, jax.random.fold_in(key, 6)
    for dim, shards_of in shards:
        draws = jnp.exp(jax.random.uniform(jax.random.fold_in(own, dim), (shards_of,), jnp.float32, smallest / len(shards), high / len(shards)))
        loudness = loudness * jnp.repeat(draws, dims[dim] // shards_of).reshape([-1 if axis == dim else 1 for axis in range(len(dims))])
    return loudness


def bell_draw(key, extent, width, limit, shards=(), kind=jnp.bfloat16):
    values = jax.random.normal(key, extent, jnp.float32) * width
    if len(shards) > 0:
        values = shard_levels(key, extent, shards, -0.22, 0.18) * values
    return jnp.clip(values, min=-limit, max=limit).astype(kind)


def setup_inputs(seed: int = 0) -> dict:
    splits = jax.random.split(jax.random.key(seed), 21)
    return {
        "tokens": bell_draw(splits[0], (ORDERED_ENTRIES, MODEL_WIDTH), 1.0, 6.0, ((0, 8),)),
        "norm_gain": jnp.clip(1.0 + 0.18 * jax.random.normal(splits[1], (MODEL_WIDTH,), jnp.float32), 0.099609375, 1.8984375).astype(jnp.bfloat16),
        "query_weight": bell_draw(splits[2], (MODEL_WIDTH, QUERY_HEADS * HEAD_SIZE), MODEL_WIDTH ** -0.5, 0.125, ((1, 4),)),
        "key_weight": bell_draw(splits[3], (MODEL_WIDTH, KEY_HEADS * HEAD_SIZE), MODEL_WIDTH ** -0.5, 0.125, ((1, 4),)),
        "value_weight": bell_draw(splits[4], (MODEL_WIDTH, KEY_HEADS * HEAD_SIZE), MODEL_WIDTH ** -0.5, 0.125, ((1, 4),)),
        "query_gain": draw_query_gain(jax.random.fold_in(splits[20], 71), 0),
        "key_gain": draw_key_gain(jax.random.fold_in(splits[20], 71), 0),
        "sink_logit": jnp.clip(4.0 + 6.0 * jax.random.uniform(splits[7], (QUERY_HEADS,), jnp.float32) ** shard_levels(splits[7], (QUERY_HEADS,), ((0, 4),), -0.2, 0.2), 4.0, 10.0),
        "gate_weight": bell_draw(splits[8], (MODEL_WIDTH, SSM_INNER), MODEL_WIDTH ** -0.5, 0.125, ((1, 4),)),
        "inner_weight": bell_draw(splits[9], (MODEL_WIDTH, SSM_INNER), MODEL_WIDTH ** -0.5, 0.125, ((1, 4),)),
        "input_map": bell_draw(splits[10], (MODEL_WIDTH, SSM_GROUPS * STATE_SIZE), MODEL_WIDTH ** -0.5, 0.125, ((1, 4),)),
        "output_map": bell_draw(splits[11], (MODEL_WIDTH, SSM_GROUPS * STATE_SIZE), MODEL_WIDTH ** -0.5, 0.125, ((1, 4),)),
        "step_weight": bell_draw(splits[12], (MODEL_WIDTH, 2, DUALITY_CHANNELS), MODEL_WIDTH ** -0.5, 0.125, ((2, 4),)),
        "conv_inner": bell_draw(splits[13], (CONV_TAPS, SSM_INNER), CONV_TAPS ** -0.5, 2.5, ((1, 4),)),
        "conv_pair": bell_draw(splits[14], (CONV_TAPS, 2, SSM_GROUPS * STATE_SIZE), CONV_TAPS ** -0.5, 2.5, ((2, 4),)),
        "decay_rate": draw_decay_rate(jax.random.fold_in(splits[20], 71), 0),
        "decay_jump": draw_decay_jump(jax.random.fold_in(splits[20], 71), 0),
        "inner_gain": jnp.clip(1.0 + 0.18 * jax.random.normal(splits[17], (SSM_INNER,), jnp.float32), 0.099609375, 1.8984375).astype(jnp.bfloat16),
        "attn_out_weight": bell_draw(splits[18], (QUERY_HEADS * HEAD_SIZE, MODEL_WIDTH), (QUERY_HEADS * HEAD_SIZE // 4) ** -0.5, 0.25, ((0, 4),)),
        "ssm_out_weight": bell_draw(splits[19], (SSM_INNER, MODEL_WIDTH), SSM_INNER ** -0.5, 0.09375, ((0, 4),)),
    }


NORM_EPS = 1e-05
ROPE_BASE = 500000.0
NEG_FILL = -1e+30

def rms_rows(values, scales):
    return values * lax.rsqrt(lax.optimization_barrier(jnp.mean(values * values, axis=-1, keepdims=True)) + NORM_EPS) * scales

def rotate(head_rows, positions):
    head_size = head_rows.shape[-1]
    half_size = head_size // 2
    frequency = ROPE_BASE ** (-jnp.arange(0, head_size, 2, dtype=jnp.float32) / head_size)
    angles = positions.astype(jnp.float32)[:, None] * frequency
    cosine = jnp.cos(angles)[:, None, :]
    sine_part = jnp.sin(angles)[:, None, :]
    first_half = head_rows[..., :half_size]
    second_half = head_rows[..., half_size:]
    return jnp.concatenate([first_half * cosine - second_half * sine_part, second_half * cosine + first_half * sine_part], axis=-1)

def attend(query, keyed, value, sink_logit):
    seq_total = query.shape[0]
    group_ratio = QUERY_HEADS // KEY_HEADS
    qblock = 512 if LOCAL_TOKENS % 512 == 0 else LOCAL_TOKENS
    key_reach = qblock + 2 * WINDOW
    rim_pad = ((WINDOW, WINDOW), (0, 0), (0, 0))
    padded_keys = jnp.pad(keyed, rim_pad)
    padded_values = jnp.pad(value, rim_pad)
    sink_table = sink_logit.astype(jnp.float32).reshape(KEY_HEADS, group_ratio)[:, :, None, None]

    def one_block(block_index):
        first_row = block_index * qblock
        block_query = lax.dynamic_slice_in_dim(query, first_row, qblock, 0)
        block_query = block_query.reshape(qblock, KEY_HEADS, group_ratio, HEAD_SIZE)
        key_part = lax.dynamic_slice_in_dim(padded_keys, first_row, key_reach, 0)
        value_part = lax.dynamic_slice_in_dim(padded_values, first_row, key_reach, 0)
        scores = jnp.einsum('qkrd,skd->krqs', block_query.astype(jnp.float32), key_part.astype(jnp.float32)) * HEAD_SIZE ** (-0.5)
        query_pos = first_row + jnp.arange(qblock, dtype=jnp.int32)
        key_pos = first_row - WINDOW + jnp.arange(key_reach, dtype=jnp.int32)
        allowed = (jnp.abs(query_pos[:, None] - key_pos[None, :]) <= WINDOW) & (key_pos[None, :] >= 0) & (key_pos[None, :] < seq_total)
        scores = jnp.where(allowed, scores, NEG_FILL)
        ceiling = jnp.maximum(lax.optimization_barrier(jnp.max(scores, axis=-1, keepdims=True)), sink_table)
        raised = jnp.exp(scores - ceiling)
        weights = raised / (lax.optimization_barrier(jnp.sum(raised, axis=-1, keepdims=True)) + jnp.exp(sink_table - ceiling))
        weights = lax.optimization_barrier(weights.astype(jnp.bfloat16))
        mixed_rows = jnp.einsum('krqs,skd->qkrd', weights.astype(jnp.float32), value_part.astype(jnp.float32))
        return mixed_rows.astype(jnp.bfloat16).reshape(qblock, QUERY_HEADS * HEAD_SIZE)
    blocks_out = lax.map(one_block, jnp.arange(seq_total // qblock, dtype=jnp.int32))
    return blocks_out.reshape(seq_total, QUERY_HEADS * HEAD_SIZE)

def ssd_pass(scaled, log_decay, in_state, out_state):
    seq_total, groups_all, ssm_ratio, head_size = scaled.shape
    state_size = in_state.shape[-1]
    blocks = seq_total // BLOCK_ROWS
    scaled_blocks = scaled.reshape(blocks, BLOCK_ROWS, groups_all, ssm_ratio, head_size)
    decay_blocks = log_decay.reshape(blocks, BLOCK_ROWS, groups_all, ssm_ratio)
    in_blocks = in_state.reshape(blocks, BLOCK_ROWS, groups_all, state_size)
    out_blocks = out_state.reshape(blocks, BLOCK_ROWS, groups_all, state_size)
    row_order = jnp.arange(BLOCK_ROWS)
    lower_mask = row_order[:, None] >= row_order[None, :]
    highest_precision = lax.Precision.HIGHEST

    def advance(carried, block_parts):
        local_scaled, decay_here, local_input, out_here = block_parts
        inside = jnp.cumsum(jnp.transpose(decay_here, (1, 2, 0)), axis=-1)
        weights_in = jnp.exp(jnp.where(lower_mask, inside[..., :, None] - inside[..., None, :], -jnp.inf))
        intersection = jnp.einsum('sgn,tgn->gst', out_here, local_input, precision=highest_precision)
        within = jnp.einsum('gst,grst,tgrp->sgrp', intersection, weights_in, local_scaled, precision=highest_precision)
        across = jnp.einsum('sgn,grpn,grs->sgrp', out_here, carried, jnp.exp(inside), precision=highest_precision)
        remaining_length = jnp.exp(inside[..., -1:] - inside)
        fresh_state = jnp.einsum('dle,lwd,dlwu->lwue', local_input, remaining_length, local_scaled, precision=highest_precision)
        updated = jnp.exp(inside[..., -1])[..., None, None] * carried + fresh_state
        return (updated, within + across)
    start_state = jnp.zeros((groups_all, ssm_ratio, head_size, state_size), jnp.float32)
    unused, outputs = lax.scan(advance, start_state, (scaled_blocks, decay_blocks, in_blocks, out_blocks))
    return outputs.reshape(seq_total, groups_all, ssm_ratio, head_size)

def reference(tokens, norm_gain, query_weight, key_weight, value_weight, query_gain, key_gain, sink_logit, gate_weight, inner_weight, input_map, output_map, step_weight, conv_inner, conv_pair, decay_rate, decay_jump, inner_gain, attn_out_weight, ssm_out_weight):
    seq_total = tokens.shape[0]
    positions = jnp.arange(seq_total, dtype=jnp.int32)
    normed = rms_rows(tokens.astype(jnp.float32), norm_gain.astype(jnp.float32)).astype(jnp.bfloat16)

    def project(weight):
        result = jnp.dot(normed, weight, preferred_element_type=jnp.float32)
        return lax.optimization_barrier(result.astype(jnp.bfloat16))
    query = project(query_weight).reshape(seq_total, QUERY_HEADS, HEAD_SIZE)
    keyed = project(key_weight).reshape(seq_total, KEY_HEADS, HEAD_SIZE)
    value = project(value_weight).reshape(seq_total, KEY_HEADS, HEAD_SIZE)
    query = rotate(rms_rows(query.astype(jnp.float32), query_gain), positions)
    query = lax.optimization_barrier(query.astype(jnp.bfloat16))
    keyed = rotate(rms_rows(keyed.astype(jnp.float32), key_gain), positions)
    keyed = lax.optimization_barrier(keyed.astype(jnp.bfloat16))
    attn_out = attend(query, keyed, value, sink_logit)
    ssm_ratio = DUALITY_CHANNELS // SSM_GROUPS
    gate_rows = project(gate_weight)
    carried_in = jnp.concatenate([project(inner_weight), project(input_map), project(output_map)], axis=1)
    carried_in = carried_in.astype(jnp.float32)
    conv_table = jnp.concatenate([conv_inner, conv_pair.reshape(CONV_TAPS, -1)], axis=1).astype(jnp.float32)
    half_taps = CONV_TAPS // 2
    rimmed = jnp.pad(carried_in, ((half_taps, half_taps), (0, 0)))
    filtered = rimmed[0:seq_total] * conv_table[0]
    for offset in range(1, CONV_TAPS):
        filtered = filtered + rimmed[offset:offset + seq_total] * conv_table[offset]
    activated = jax.nn.silu(filtered)
    map_width = SSM_GROUPS * STATE_SIZE
    signal = activated[:, :SSM_INNER].reshape(seq_total, SSM_GROUPS, ssm_ratio, HEAD_SIZE)
    in_state = activated[:, SSM_INNER:SSM_INNER + map_width].reshape(seq_total, SSM_GROUPS, STATE_SIZE)
    out_state = activated[:, SSM_INNER + map_width:].reshape(seq_total, SSM_GROUPS, STATE_SIZE)
    step_rows = project(step_weight.reshape(MODEL_WIDTH, 2 * DUALITY_CHANNELS))
    step = jax.nn.softplus(step_rows.astype(jnp.float32)).reshape(seq_total, 2, SSM_GROUPS, ssm_ratio)
    log_decay = -decay_rate.reshape(2, SSM_GROUPS, ssm_ratio) * step + decay_jump.reshape(seq_total, 2, SSM_GROUPS, ssm_ratio)
    forward_y = ssd_pass(signal * step[:, 0, :, :, None], log_decay[:, 0], in_state, out_state)
    backward_y = jnp.flip(ssd_pass(jnp.flip(signal * step[:, 1, :, :, None], 0), jnp.flip(log_decay[:, 1], 0), jnp.flip(in_state, 0), jnp.flip(out_state, 0)), 0)
    combined = (forward_y + backward_y).reshape(seq_total, SSM_INNER) * jax.nn.silu(gate_rows.astype(jnp.float32))
    grouped = rms_rows(combined.reshape(seq_total, SSM_GROUPS, -1), 1.0).reshape(seq_total, SSM_INNER)
    ssm_out = (grouped * inner_gain.astype(jnp.float32)).astype(jnp.bfloat16)
    attn_group = QUERY_HEADS * HEAD_SIZE // N_TP
    ssm_group = SSM_INNER // N_TP
    summed = jnp.zeros((seq_total, MODEL_WIDTH), jnp.float32)
    for group_index in range(N_TP):
        attn_cols = attn_out[:, group_index * attn_group:(group_index + 1) * attn_group]
        ssm_cols = ssm_out[:, group_index * ssm_group:(group_index + 1) * ssm_group]
        partial_sum = jnp.dot(attn_cols, attn_out_weight[group_index * attn_group:(group_index + 1) * attn_group], preferred_element_type=jnp.float32)
        partial_sum = partial_sum + jnp.dot(ssm_cols, ssm_out_weight[group_index * ssm_group:(group_index + 1) * ssm_group], preferred_element_type=jnp.float32)
        rounded = lax.optimization_barrier(partial_sum.astype(jnp.bfloat16))
        summed = summed + rounded.astype(jnp.float32)
    return summed.astype(jnp.bfloat16)
```

```python
import functools

import jax
import jax.numpy as jnp
from jax import lax
from jax.experimental import pallas as pl
from jax.experimental.pallas import tpu as pltpu
from jax.sharding import PartitionSpec as P

STATE_SIZE = 128
WINDOW = 128
CHUNK = 128
HALO = 16

NORM_EPS = 1e-05
ROPE_BASE = 500000.0
NEG_FILL = -1e30
PIECE = 256
MESH = pl.DeviceIdType.MESH


def extended(block, sides, width):
    for axis, dim in sides:
        count = lax.axis_size(axis)
        forward = [(i, i + 1) for i in range(count - 1)]
        backward = [(target, source) for source, target in forward]
        low = lax.ppermute(
            lax.slice_in_dim(block, block.shape[dim] - width, None, axis=dim), axis, forward
        )
        high = lax.ppermute(lax.slice_in_dim(block, 0, width, axis=dim), axis, backward)
        block = jnp.concatenate([low, block, high], axis=dim)
    return block


def rms_rows(values, scales):
    return values * lax.rsqrt(jnp.mean(values * values, axis=-1, keepdims=True) + NORM_EPS) * scales


def rotate(head_rows, positions):
    head_size = head_rows.shape[-1]
    half_size = head_size // 2
    frequency = ROPE_BASE ** (-jnp.arange(0, head_size, 2, dtype=jnp.float32) / head_size)
    angles = positions.astype(jnp.float32)[:, None] * frequency
    cosine = jnp.cos(angles)[:, None, :]
    sine_part = jnp.sin(angles)[:, None, :]
    first_half = head_rows[..., :half_size]
    second_half = head_rows[..., half_size:]
    return jnp.concatenate(
        [
            first_half * cosine - second_half * sine_part,
            second_half * cosine + first_half * sine_part,
        ],
        axis=-1,
    )


def spread(factor, width):
    heads = factor.shape[1]
    row = lax.broadcasted_iota(jnp.int32, (heads, width), 0)
    column = lax.broadcasted_iota(jnp.int32, (heads, width), 1)
    head_size = width // heads
    ones = jnp.where(
        (column >= row * head_size) & (column < (row + 1) * head_size), 1.0, 0.0
    ).astype(jnp.bfloat16)
    return jnp.dot(factor.astype(jnp.bfloat16), ones, preferred_element_type=jnp.float32)


def exact_dot(a, b):
    return jnp.dot(a, b, precision=lax.Precision.HIGHEST, preferred_element_type=jnp.float32)


def triangle(size, lower):
    row = lax.broadcasted_iota(jnp.int32, (size, size), 0)
    column = lax.broadcasted_iota(jnp.int32, (size, size), 1)
    return jnp.where(row >= column if lower else row <= column, 1.0, 0.0)


def states_kernel(
    tap_count, inner, maps, rows_ref, taps_ref, ldf_ref, ldb_ref, stf_ref, stb_ref,
    act_ref, freshf_ref, freshb_ref, endf_ref, endb_ref, spare, reach,
):
    step = pl.program_id(0)
    size = act_ref.shape[0]
    start = pl.multiple_of(step * size, size)
    spare[...] = rows_ref[pl.ds(start, size + 2 * HALO), :].astype(jnp.float32)
    first = HALO - tap_count // 2
    filtered = spare[first : first + size, :] * taps_ref[0:1, :]
    for k in range(1, tap_count):
        filtered = filtered + spare[first + k : first + k + size, :] * taps_ref[k : k + 1, :]
    activated = filtered / (1.0 + jnp.exp(-filtered))
    act_ref[...] = activated.astype(jnp.bfloat16)
    signal = activated[:, :inner]
    ldf, ldb = ldf_ref[...], ldb_ref[...]
    cumf = exact_dot(triangle(size, True), ldf)
    cumb = exact_dot(triangle(size, False), ldb)
    wf = jnp.exp(cumf[size - 1 : size] - cumf) * stf_ref[...]
    wb = jnp.exp(cumb[0:1] - cumb) * stb_ref[...]
    xf = (signal * spread(wf, inner)).astype(jnp.bfloat16)
    xb = (signal * spread(wb, inner)).astype(jnp.bfloat16)
    totf = spread(jnp.exp(jnp.broadcast_to(cumf[size - 1 : size], (8, ldf.shape[1]))), inner)[0:1]
    totb = spread(jnp.exp(jnp.broadcast_to(cumb[0:1], (8, ldb.shape[1]))), inner)[0:1]

    @pl.when(step == 0)
    def _():
        endf_ref[...] = jnp.zeros_like(endf_ref)
        endb_ref[...] = jnp.zeros_like(endb_ref)
        reach[...] = jnp.ones_like(reach)

    groups = maps // STATE_SIZE
    width = inner // groups
    for g in range(groups):
        entry = activated[:, inner + g * STATE_SIZE : inner + (g + 1) * STATE_SIZE]
        entry = jnp.transpose(entry).astype(jnp.bfloat16)
        cols = slice(g * width, (g + 1) * width)
        ff = jnp.dot(entry, xf[:, cols], preferred_element_type=jnp.float32)
        fb = jnp.dot(entry, xb[:, cols], preferred_element_type=jnp.float32)
        freshf_ref[0, :, cols] = ff
        freshb_ref[0, :, cols] = fb
        endf_ref[:, cols] = endf_ref[:, cols] * totf[:, cols] + ff
        endb_ref[:, cols] = endb_ref[:, cols] + reach[0:1, cols] * fb
    reach[...] = reach[...] * totb


def outputs_kernel(
    head_size, inner, maps, act_ref, ldf_ref, ldb_ref, stf_ref, stb_ref, ldft_ref, ldbt_ref,
    stft_ref, stbt_ref, ldball_ref, freshf_ref, freshb_ref, inf_ref, inb_ref, gate_ref, gain_ref,
    out_ref, carryf, enterb, y,
):
    step = pl.program_id(0)
    chunks = pl.num_programs(0)
    size = act_ref.shape[0]
    heads = inner // head_size

    @pl.when(step == 0)
    def _():
        carryf[...] = inf_ref[...]
        enterb[chunks - 1] = inb_ref[...]

        @pl.loop(0, chunks - 1)
        def _(k):
            at = chunks - 1 - k
            part = ldball_ref[pl.ds(pl.multiple_of(at * size, size), size), :]
            tot = jnp.exp(jnp.sum(part, axis=0, keepdims=True))
            tot = spread(jnp.broadcast_to(tot, (8, heads)), inner)[0:1]
            enterb[at - 1] = enterb[at] * tot + freshb_ref[at]

    lower, upper = triangle(size, True), triangle(size, False)
    cumf = exact_dot(lower, ldf_ref[...])
    cumb = exact_dot(upper, ldb_ref[...])
    cumft = exact_dot(ldft_ref[...], upper)
    cumbt = exact_dot(ldbt_ref[...], lower)
    stft, stbt = stft_ref[...], stbt_ref[...]
    row = lax.broadcasted_iota(jnp.int32, (size, size), 0)
    column = lax.broadcasted_iota(jnp.int32, (size, size), 1)
    is_lower, is_diagonal = row >= column, row == column
    groups = maps // STATE_SIZE
    width = inner // groups
    group_heads = heads // groups
    expf = spread(jnp.exp(cumf), inner)
    expb = spread(jnp.exp(cumb), inner)
    lane = lax.broadcasted_iota(jnp.int32, (size, 2 * head_size), 1)
    for g in range(groups):
        cols = slice(g * width, (g + 1) * width)
        entry = act_ref[:, inner + g * STATE_SIZE : inner + (g + 1) * STATE_SIZE]
        leave = act_ref[:, inner + maps + g * STATE_SIZE : inner + maps + (g + 1) * STATE_SIZE]
        crossed = lax.dot_general(
            leave, entry, (((1,), (1,)), ((), ())), preferred_element_type=jnp.float32
        )
        y[:, cols] = (
            jnp.dot(leave, carryf[:, cols].astype(jnp.bfloat16), preferred_element_type=jnp.float32)
            * expf[:, cols]
            + jnp.dot(
                leave, enterb[step, :, cols].astype(jnp.bfloat16),
                preferred_element_type=jnp.float32,
            )
            * expb[:, cols]
        )
        for pair in range(group_heads // 2):
            mats = []
            base = g * group_heads + 2 * pair
            for h in (base, base + 1):
                gap = jnp.where(
                    is_lower,
                    cumf[:, h : h + 1] - cumft[h : h + 1, :],
                    cumb[:, h : h + 1] - cumbt[h : h + 1, :],
                )
                sf, sb = stft[h : h + 1, :], stbt[h : h + 1, :]
                amount = jnp.where(is_diagonal, sf + sb, jnp.where(is_lower, sf, sb))
                mats.append((crossed * jnp.exp(gap) * amount).astype(jnp.bfloat16))
            two = slice(base * head_size, (base + 2) * head_size)
            x = act_ref[:, two]
            zero = jnp.zeros_like(x)
            stacked = jnp.concatenate(
                [jnp.where(lane < head_size, x, zero), jnp.where(lane < head_size, zero, x)], axis=0
            )
            y[:, two] += jnp.dot(
                jnp.concatenate(mats, axis=1), stacked, preferred_element_type=jnp.float32
            )
        gate = gate_ref[:, cols].astype(jnp.float32)
        mixed = y[:, cols] * (gate / (1.0 + jnp.exp(-gate)))
        scale = lax.rsqrt(jnp.mean(mixed * mixed, axis=1, keepdims=True) + NORM_EPS)
        out_ref[:, cols] = (mixed * scale * gain_ref[:, cols]).astype(jnp.bfloat16)
    totf = spread(jnp.exp(jnp.broadcast_to(cumf[size - 1 : size], (8, heads))), inner)[0:1]
    carryf[...] = carryf[...] * totf + freshf_ref[0]


def attend_kernel(head_size, key_heads, place_ref, sink_ref, query_ref, rim_ref, out_ref):
    step = pl.program_id(0)
    size = query_ref.shape[0]
    reach = size + 2 * WINDOW
    heads = query_ref.shape[1] // head_size
    ratio = heads // key_heads
    start = pl.multiple_of(step * size, size)
    row = lax.broadcasted_iota(jnp.int32, (size, reach), 0)
    column = lax.broadcasted_iota(jnp.int32, (size, reach), 1)
    key_pos = place_ref[0] + step * size - WINDOW + column
    allowed = (
        (column >= row) & (column <= row + 2 * WINDOW) & (key_pos >= 0) & (key_pos < place_ref[1])
    )
    scale = head_size ** (-0.5)
    for k in range(key_heads):
        keys = rim_ref[pl.ds(start, reach), k * head_size : (k + 1) * head_size]
        values = rim_ref[
            pl.ds(start, reach), (key_heads + k) * head_size : (key_heads + k + 1) * head_size
        ]
        for r in range(ratio):
            h = k * ratio + r
            cols = slice(h * head_size, (h + 1) * head_size)
            scores = lax.dot_general(
                query_ref[:, cols], keys, (((1,), (1,)), ((), ())),
                preferred_element_type=jnp.float32,
            )
            scores = jnp.where(allowed, scores * scale, NEG_FILL)
            sink = sink_ref[h]
            ceiling = jnp.maximum(jnp.max(scores, axis=1, keepdims=True), sink)
            raised = jnp.exp(scores - ceiling)
            bottom = jnp.sum(raised, axis=1, keepdims=True) + jnp.exp(sink - ceiling)
            weights = (raised * (1.0 / bottom)).astype(jnp.bfloat16)
            out_ref[:, cols] = jnp.dot(
                weights, values, preferred_element_type=jnp.float32
            ).astype(jnp.bfloat16)


def attend(query, rimmed, sink_logit, seq_first, seq_total, head_size, key_heads):
    rows, width = query.shape
    block = WINDOW
    place = jnp.stack([jnp.int32(seq_first), jnp.int32(seq_total)])
    return pl.pallas_call(
        functools.partial(attend_kernel, head_size, key_heads),
        grid=(rows // block,),
        in_specs=[
            pl.BlockSpec(memory_space=pltpu.SMEM),
            pl.BlockSpec(memory_space=pltpu.SMEM),
            pl.BlockSpec((block, width), lambda i: (i, 0)),
            pl.BlockSpec(rimmed.shape, lambda i: (0, 0)),
        ],
        out_specs=pl.BlockSpec((block, width), lambda i: (i, 0)),
        out_shape=jax.ShapeDtypeStruct((rows, width), jnp.bfloat16),
        cost_estimate=pl.CostEstimate(
            flops=4 * rows * 3 * WINDOW * width, bytes_accessed=4 * rows * width,
            transcendentals=rows * 3 * WINDOW * width // head_size,
        ),
        name="attend",
    )(place, sink_logit, query, rimmed)


def combine_kernel(
    count, attn_ref, ssm_ref, attn_w_ref, ssm_w_ref, out_ref, acc, own, mate_out, mate_in,
    far_out, far_in, mate_send, mate_recv, far_send, far_recv,
):
    me = lax.axis_index("tp")
    core = lax.rem(me, 2)
    chip = lax.div(me, 2)
    chips = count // 2
    mate = me + 1 - 2 * core
    rows = out_ref.shape[0]
    pieces, width = own.shape[1], own.shape[3]

    def chip_of(slot):
        return lax.rem(chip + 1 + slot, chips)

    def to_mate(slot, j):
        return pltpu.make_async_remote_copy(
            src_ref=mate_out.at[slot, j], dst_ref=mate_in.at[slot, j],
            send_sem=mate_send.at[slot, j], recv_sem=mate_recv.at[slot, j],
            device_id={"tp": mate}, device_id_type=MESH,
        )

    def to_far(slot, j):
        return pltpu.make_async_remote_copy(
            src_ref=far_out.at[slot, j], dst_ref=far_in.at[slot, j],
            send_sem=far_send.at[slot, j], recv_sem=far_recv.at[slot, j],
            device_id={"tp": 2 * chip_of(slot) + core}, device_id_type=MESH,
        )

    barrier = pltpu.get_barrier_semaphore()
    pl.semaphore_signal(barrier, inc=1, device_id={"tp": mate}, device_id_type=MESH)
    for slot in range(chips - 1):
        pl.semaphore_signal(
            barrier, inc=1, device_id={"tp": 2 * chip_of(slot) + core}, device_id_type=MESH
        )
    pl.semaphore_wait(barrier, chips)

    def compute(slot, j):
        cols = pl.ds(pl.multiple_of(j * width, width), width)
        first = pl.multiple_of(chip_of(slot) * 2 * rows, rows)
        span = pl.ds(first, 2 * rows)
        acc[...] = jnp.dot(
            attn_ref[span, :], attn_w_ref[:, cols], preferred_element_type=jnp.float32
        ) + jnp.dot(ssm_ref[span, :], ssm_w_ref[:, cols], preferred_element_type=jnp.float32)
        other = acc[pl.ds(pl.multiple_of((1 - core) * rows, rows), rows), :]
        mate_out[slot, j] = other.astype(jnp.bfloat16)
        to_mate(slot, j).start()
        mine = acc[pl.ds(pl.multiple_of(core * rows, rows), rows), :]
        own[slot, j] = mine.astype(jnp.bfloat16)

    def forward(slot, j):
        to_mate(slot, j).wait_recv()
        far_out[slot, j] = (
            own[slot, j].astype(jnp.float32) + mate_in[slot, j].astype(jnp.float32)
        ).astype(jnp.bfloat16)
        to_far(slot, j).start()

    last = chips - 1
    for slot in range(chips):
        compute(slot, 0)
        if slot > 0:
            forward(slot - 1, pieces - 1)

        @pl.loop(1, pieces)
        def _(j, slot=slot):
            compute(slot, j)
            if slot < last:
                forward(slot, j - 1)

    @pl.loop(0, pieces)
    def _(j):
        to_mate(last, j).wait_recv()
        total = own[last, j].astype(jnp.float32) + mate_in[last, j].astype(jnp.float32)
        for slot in range(last):
            to_far(slot, j).wait_recv()
            total = total + far_in[slot, j].astype(jnp.float32)
        out_ref[:, pl.ds(pl.multiple_of(j * width, width), width)] = total.astype(jnp.bfloat16)

    @pl.loop(0, pieces)
    def _(j):
        for slot in range(chips):
            to_mate(slot, j).wait_send()
        for slot in range(last):
            to_far(slot, j).wait_send()


def combine(attn_out, ssm_out, attn_weight, ssm_weight):
    count = lax.axis_size("tp")
    chips = count // 2
    total, width = attn_out.shape[0], attn_weight.shape[1]
    rows = total // count
    pieces = width // PIECE
    far = max(chips - 1, 1)
    vmem = pl.BlockSpec(memory_space=pltpu.VMEM)
    depth = attn_out.shape[1] + ssm_out.shape[1]
    return pl.pallas_call(
        functools.partial(combine_kernel, count),
        in_specs=[vmem] * 4,
        out_specs=vmem,
        out_shape=jax.ShapeDtypeStruct((rows, width), jnp.bfloat16),
        scratch_shapes=[
            pltpu.VMEM((2 * rows, PIECE), jnp.float32),
            pltpu.VMEM((chips, pieces, rows, PIECE), jnp.bfloat16),
            pltpu.VMEM((chips, pieces, rows, PIECE), jnp.bfloat16),
            pltpu.VMEM((chips, pieces, rows, PIECE), jnp.bfloat16),
            pltpu.VMEM((far, pieces, rows, PIECE), jnp.bfloat16),
            pltpu.VMEM((far, pieces, rows, PIECE), jnp.bfloat16),
            pltpu.SemaphoreType.DMA((chips, pieces)),
            pltpu.SemaphoreType.DMA((chips, pieces)),
            pltpu.SemaphoreType.DMA((far, pieces)),
            pltpu.SemaphoreType.DMA((far, pieces)),
        ],
        compiler_params=pltpu.CompilerParams(collective_id=3, has_side_effects=True),
        cost_estimate=pl.CostEstimate(
            flops=2 * total * depth * width, bytes_accessed=2 * depth * width, transcendentals=0
        ),
        name="combine",
    )(attn_out, ssm_out, attn_weight, ssm_weight)


def chunk_states(rimmed, taps, tap_count, inner, maps, decay, step):
    rows = rimmed.shape[0] - 2 * HALO
    total, heads, chunks = rimmed.shape[1], decay[0].shape[1], rows // CHUNK
    small = pl.BlockSpec((CHUNK, heads), lambda i: (i, 0))
    fresh = pl.BlockSpec((1, STATE_SIZE, inner), lambda i: (i, 0, 0))
    end = pl.BlockSpec((STATE_SIZE, inner), lambda i: (0, 0))
    fresh_shape = jax.ShapeDtypeStruct((chunks, STATE_SIZE, inner), jnp.float32)
    end_shape = jax.ShapeDtypeStruct((STATE_SIZE, inner), jnp.float32)
    return pl.pallas_call(
        functools.partial(states_kernel, tap_count, inner, maps),
        grid=(chunks,),
        in_specs=[
            pl.BlockSpec(rimmed.shape, lambda i: (0, 0)),
            pl.BlockSpec(taps.shape, lambda i: (0, 0)),
            small, small, small, small,
        ],
        out_specs=[pl.BlockSpec((CHUNK, total), lambda i: (i, 0)), fresh, fresh, end, end],
        out_shape=[
            jax.ShapeDtypeStruct((rows, total), jnp.bfloat16),
            fresh_shape, fresh_shape, end_shape, end_shape,
        ],
        scratch_shapes=[
            pltpu.VMEM((CHUNK + 2 * HALO, total), jnp.float32),
            pltpu.VMEM((8, inner), jnp.float32),
        ],
        cost_estimate=pl.CostEstimate(
            flops=8 * rows * inner * STATE_SIZE, bytes_accessed=16 * rows * inner,
            transcendentals=rows * total,
        ),
        name="chunk_states",
    )(rimmed, taps, *decay, *step)


def chunk_outputs(head_size, inner, maps, act, decay, step, fresh, incoming, gate, gain):
    rows, total = act.shape
    heads, chunks = decay[0].shape[1], rows // CHUNK
    small = pl.BlockSpec((CHUNK, heads), lambda i: (i, 0))
    turned = pl.BlockSpec((heads, CHUNK), lambda i: (0, i))
    whole = pl.BlockSpec((STATE_SIZE, inner), lambda i: (0, 0))
    return pl.pallas_call(
        functools.partial(outputs_kernel, head_size, inner, maps),
        grid=(chunks,),
        in_specs=[
            pl.BlockSpec((CHUNK, total), lambda i: (i, 0)),
            small, small, small, small, turned, turned, turned, turned,
            pl.BlockSpec((rows, heads), lambda i: (0, 0)),
            pl.BlockSpec((1, STATE_SIZE, inner), lambda i: (i, 0, 0)),
            pl.BlockSpec((chunks, STATE_SIZE, inner), lambda i: (0, 0, 0)),
            whole, whole,
            pl.BlockSpec((CHUNK, inner), lambda i: (i, 0)),
            pl.BlockSpec((1, inner), lambda i: (0, 0)),
        ],
        out_specs=pl.BlockSpec((CHUNK, inner), lambda i: (i, 0)),
        out_shape=jax.ShapeDtypeStruct((rows, inner), jnp.bfloat16),
        scratch_shapes=[
            pltpu.VMEM((STATE_SIZE, inner), jnp.float32),
            pltpu.VMEM((chunks, STATE_SIZE, inner), jnp.float32),
            pltpu.VMEM((CHUNK, inner), jnp.float32),
        ],
        cost_estimate=pl.CostEstimate(
            flops=8 * rows * inner * STATE_SIZE, bytes_accessed=16 * rows * inner,
            transcendentals=rows * CHUNK * heads,
        ),
        name="chunk_outputs",
    )(
        act, *decay, *step, decay[0].T, decay[1].T, step[0].T, step[1].T, decay[1],
        fresh[0], fresh[1], incoming[0], incoming[1], gate, gain,
    )


def entering_state(end, total, axis, head_size, reverse):
    count = lax.axis_size(axis)
    states = end.shape[0]

    def moved(packet, distance):
        pairs = [(i, i + distance) for i in range(count - distance)]
        if reverse:
            pairs = [(target, source) for source, target in pairs]
        return lax.ppermute(packet, axis, pairs)

    decay = jnp.broadcast_to(jnp.repeat(jnp.exp(total), head_size)[None, :], (16, end.shape[1]))
    packet = jnp.concatenate([end, decay], axis=0).astype(jnp.bfloat16)
    packet = moved(packet, 1)
    distance = 1
    held = packet.astype(jnp.float32)
    while distance < count - 1:
        arrived = moved(held.astype(jnp.bfloat16), distance).astype(jnp.float32)
        factor = held[states : states + 1]
        added = jnp.concatenate([held[:states], jnp.zeros_like(held[states:])], axis=0)
        held = added + factor * arrived
        distance *= 2
    return held[:states]


def local(
    tokens,
    norm_gain,
    query_weight,
    key_weight,
    value_weight,
    query_gain,
    key_gain,
    sink_logit,
    gate_weight,
    inner_weight,
    input_map,
    output_map,
    step_weight,
    conv_inner,
    conv_pair,
    decay_rate,
    decay_jump,
    inner_gain,
    attn_out_weight,
    ssm_out_weight,
):
    row_total = tokens.shape[0]
    seq_total = row_total * lax.axis_size("sp")
    seq_first = lax.axis_index("sp") * row_total
    positions = seq_first + jnp.arange(row_total, dtype=jnp.int32)
    normed = rms_rows(tokens.astype(jnp.float32), norm_gain.astype(jnp.float32)).astype(
        jnp.bfloat16
    )

    def project(weight):
        result = jnp.dot(normed, weight, preferred_element_type=jnp.float32)
        return lax.optimization_barrier(result.astype(jnp.bfloat16))

    head_size = query_gain.shape[0]
    query = project(query_weight).reshape(row_total, -1, head_size)
    keyed = project(key_weight).reshape(row_total, -1, head_size)
    value = project(value_weight)
    query = rotate(rms_rows(query.astype(jnp.float32), query_gain), positions).astype(jnp.bfloat16)
    keyed = rotate(rms_rows(keyed.astype(jnp.float32), key_gain), positions).astype(jnp.bfloat16)
    key_heads = keyed.shape[1]
    packed = jnp.concatenate([keyed.reshape(row_total, -1), value], axis=1)
    rimmed_keys = extended(packed, (("sp", 0),), WINDOW)
    inner_rows = project(inner_weight)
    inner_width = inner_rows.shape[1]
    map_width = input_map.shape[1]
    carried_in = jnp.concatenate([inner_rows, project(input_map), project(output_map)], axis=1)
    tap_count = conv_inner.shape[0]
    conv_table = jnp.concatenate([conv_inner, conv_pair.reshape(tap_count, -1)], axis=1).astype(
        jnp.float32
    )
    rimmed_rows = extended(carried_in, (("sp", 0),), HALO)
    step_rows = project(step_weight.reshape(step_weight.shape[0], -1))
    step = jax.nn.softplus(step_rows.astype(jnp.float32))
    log_decay = -decay_rate.reshape(1, -1) * step + decay_jump.reshape(row_total, -1)
    heads_here = inner_width // head_size
    steps = (step[:, :heads_here], step[:, heads_here:])
    decays = (log_decay[:, :heads_here], log_decay[:, heads_here:])
    act, fresh_forward, fresh_backward, end_forward, end_backward = chunk_states(
        rimmed_rows, conv_table, tap_count, inner_width, map_width, decays, steps
    )
    from_lower = entering_state(end_forward, jnp.sum(decays[0], axis=0), "sp", head_size, False)
    from_higher = entering_state(end_backward, jnp.sum(decays[1], axis=0), "sp", head_size, True)
    attn_out = attend(
        query.reshape(row_total, -1), rimmed_keys, sink_logit, seq_first, seq_total, head_size,
        key_heads,
    )
    gate_rows = project(gate_weight)
    ssm_out = chunk_outputs(
        head_size, inner_width, map_width, act, decays, steps, (fresh_forward, fresh_backward),
        (from_lower, from_higher), gate_rows, inner_gain.astype(jnp.float32)[None, :],
    )
    return combine(attn_out, ssm_out, attn_out_weight, ssm_out_weight)


def solution(mesh):
    in_specs = (
        P("sp", None),
        P(),
        P(None, "tp"),
        P(None, "tp"),
        P(None, "tp"),
        P(),
        P(),
        P("tp"),
        P(None, "tp"),
        P(None, "tp"),
        P(None, "tp"),
        P(None, "tp"),
        P(None, None, "tp"),
        P(None, "tp"),
        P(None, None, "tp"),
        P(None, "tp"),
        P("sp", None, "tp"),
        P("tp"),
        P("tp", None),
        P("tp", None),
    )
    out_specs = P(("sp", "tp"), None)
    return jax.shard_map(local, mesh=mesh, in_specs=in_specs, out_specs=out_specs, check_vma=False)
```

```python
import functools

import jax
import jax.numpy as jnp
from jax import lax
from jax.experimental import pallas as pl
from jax.experimental.pallas import tpu as pltpu
from jax.sharding import PartitionSpec as P

STATE_SIZE = 128
WINDOW = 128
CHUNK = 128
HALO = 16

NORM_EPS = 1e-05
ROPE_BASE = 500000.0
NEG_FILL = -1e30
PIECE = 256
PACK_ROWS = 16
MESH = pl.DeviceIdType.MESH


def extended(block, sides, width):
    for axis, dim in sides:
        count = lax.axis_size(axis)
        forward = [(i, i + 1) for i in range(count - 1)]
        backward = [(target, source) for source, target in forward]
        low = lax.ppermute(
            lax.slice_in_dim(block, block.shape[dim] - width, None, axis=dim), axis, forward
        )
        high = lax.ppermute(lax.slice_in_dim(block, 0, width, axis=dim), axis, backward)
        block = jnp.concatenate([low, block, high], axis=dim)
    return block


def rms_rows(values, scales):
    return values * lax.rsqrt(jnp.mean(values * values, axis=-1, keepdims=True) + NORM_EPS) * scales


def rotate(head_rows, positions):
    head_size = head_rows.shape[-1]
    half_size = head_size // 2
    frequency = ROPE_BASE ** (-jnp.arange(0, head_size, 2, dtype=jnp.float32) / head_size)
    angles = positions.astype(jnp.float32)[:, None] * frequency
    cosine = jnp.cos(angles)[:, None, :]
    sine_part = jnp.sin(angles)[:, None, :]
    first_half = head_rows[..., :half_size]
    second_half = head_rows[..., half_size:]
    return jnp.concatenate(
        [
            first_half * cosine - second_half * sine_part,
            second_half * cosine + first_half * sine_part,
        ],
        axis=-1,
    )


def spread(factor, width):
    heads = factor.shape[1]
    row = lax.broadcasted_iota(jnp.int32, (heads, width), 0)
    column = lax.broadcasted_iota(jnp.int32, (heads, width), 1)
    head_size = width // heads
    ones = jnp.where(
        (column >= row * head_size) & (column < (row + 1) * head_size), 1.0, 0.0
    ).astype(jnp.bfloat16)
    return jnp.dot(factor.astype(jnp.bfloat16), ones, preferred_element_type=jnp.float32)


def exact_dot(a, b):
    return jnp.dot(a, b, precision=lax.Precision.HIGHEST, preferred_element_type=jnp.float32)


def triangle(size, lower):
    row = lax.broadcasted_iota(jnp.int32, (size, size), 0)
    column = lax.broadcasted_iota(jnp.int32, (size, size), 1)
    return jnp.where(row >= column if lower else row <= column, 1.0, 0.0)


def states_kernel(
    tap_count, inner, maps, rows_ref, taps_ref, ldf_ref, ldb_ref, stf_ref, stb_ref,
    act_ref, freshf_ref, freshb_ref, packf_ref, packb_ref, spare, reach, endf_ref, endb_ref, logs,
):
    step = pl.program_id(0)
    size = act_ref.shape[0]
    start = pl.multiple_of(step * size, size)
    spare[...] = rows_ref[pl.ds(start, size + 2 * HALO), :].astype(jnp.float32)
    first = HALO - tap_count // 2
    filtered = spare[first : first + size, :] * taps_ref[0:1, :]
    for k in range(1, tap_count):
        filtered = filtered + spare[first + k : first + k + size, :] * taps_ref[k : k + 1, :]
    activated = filtered / (1.0 + jnp.exp(-filtered))
    act_ref[...] = activated.astype(jnp.bfloat16)
    signal = activated[:, :inner]
    ldf, ldb = ldf_ref[...], ldb_ref[...]
    cumf = exact_dot(triangle(size, True), ldf)
    cumb = exact_dot(triangle(size, False), ldb)
    wf = jnp.exp(cumf[size - 1 : size] - cumf) * stf_ref[...]
    wb = jnp.exp(cumb[0:1] - cumb) * stb_ref[...]
    xf = (signal * spread(wf, inner)).astype(jnp.bfloat16)
    xb = (signal * spread(wb, inner)).astype(jnp.bfloat16)
    totf = spread(jnp.exp(jnp.broadcast_to(cumf[size - 1 : size], (8, ldf.shape[1]))), inner)[0:1]
    totb = spread(jnp.exp(jnp.broadcast_to(cumb[0:1], (8, ldb.shape[1]))), inner)[0:1]

    @pl.when(step == 0)
    def _():
        endf_ref[...] = jnp.zeros_like(endf_ref)
        endb_ref[...] = jnp.zeros_like(endb_ref)
        reach[...] = jnp.ones_like(reach)
        logs[...] = jnp.zeros_like(logs)

    groups = maps // STATE_SIZE
    width = inner // groups
    for g in range(groups):
        entry = activated[:, inner + g * STATE_SIZE : inner + (g + 1) * STATE_SIZE]
        entry = jnp.transpose(entry).astype(jnp.bfloat16)
        cols = slice(g * width, (g + 1) * width)
        ff = jnp.dot(entry, xf[:, cols], preferred_element_type=jnp.float32)
        fb = jnp.dot(entry, xb[:, cols], preferred_element_type=jnp.float32)
        freshf_ref[0, :, cols] = ff
        freshb_ref[0, :, cols] = fb
        endf_ref[:, cols] = endf_ref[:, cols] * totf[:, cols] + ff
        endb_ref[:, cols] = endb_ref[:, cols] + reach[0:1, cols] * fb
    reach[...] = reach[...] * totb
    logs[0] = logs[0] + cumf[size - 1 : size]
    logs[1] = logs[1] + cumb[0:1]

    @pl.when(step == pl.num_programs(0) - 1)
    def _():
        half = inner // 2
        for d, (end_ref, pack_ref) in enumerate(((endf_ref, packf_ref), (endb_ref, packb_ref))):
            decay = spread(jnp.exp(logs[d]), inner).astype(jnp.bfloat16)
            for side in range(2):
                cols = slice(side * half, (side + 1) * half)
                pack_ref[side, :STATE_SIZE, :] = end_ref[:, cols].astype(jnp.bfloat16)
                pack_ref[side, STATE_SIZE:, :] = jnp.concatenate([decay, decay], axis=0)[:, cols]


def outputs_kernel(
    head_size, inner, maps, act_ref, ldf_ref, ldb_ref, stf_ref, stb_ref, ldft_ref, ldbt_ref,
    stft_ref, stbt_ref, ldball_ref, freshf_ref, freshb_ref, enter_ref, gate_ref, gain_ref,
    out_ref, carryf, enterb, y,
):
    step = pl.program_id(0)
    chunks = pl.num_programs(0)
    size = act_ref.shape[0]
    heads = inner // head_size

    @pl.when(step == 0)
    def _():
        half = inner // 2
        for side in range(2):
            carryf[:, side * half : (side + 1) * half] = enter_ref[0, side]
            enterb[chunks - 1, :, side * half : (side + 1) * half] = enter_ref[1, side]

        @pl.loop(0, chunks - 1)
        def _(k):
            at = chunks - 1 - k
            part = ldball_ref[pl.ds(pl.multiple_of(at * size, size), size), :]
            tot = jnp.exp(jnp.sum(part, axis=0, keepdims=True))
            tot = spread(jnp.broadcast_to(tot, (8, heads)), inner)[0:1]
            enterb[at - 1] = enterb[at] * tot + freshb_ref[at]

    lower, upper = triangle(size, True), triangle(size, False)
    cumf = exact_dot(lower, ldf_ref[...])
    cumb = exact_dot(upper, ldb_ref[...])
    cumft = exact_dot(ldft_ref[...], upper)
    cumbt = exact_dot(ldbt_ref[...], lower)
    stft, stbt = stft_ref[...], stbt_ref[...]
    row = lax.broadcasted_iota(jnp.int32, (size, size), 0)
    column = lax.broadcasted_iota(jnp.int32, (size, size), 1)
    is_lower, is_diagonal = row >= column, row == column
    groups = maps // STATE_SIZE
    width = inner // groups
    group_heads = heads // groups
    expf = spread(jnp.exp(cumf), inner)
    expb = spread(jnp.exp(cumb), inner)
    lane = lax.broadcasted_iota(jnp.int32, (size, 2 * head_size), 1)
    for g in range(groups):
        cols = slice(g * width, (g + 1) * width)
        entry = act_ref[:, inner + g * STATE_SIZE : inner + (g + 1) * STATE_SIZE]
        leave = act_ref[:, inner + maps + g * STATE_SIZE : inner + maps + (g + 1) * STATE_SIZE]
        crossed = lax.dot_general(
            leave, entry, (((1,), (1,)), ((), ())), preferred_element_type=jnp.float32
        )
        y[:, cols] = (
            jnp.dot(leave, carryf[:, cols].astype(jnp.bfloat16), preferred_element_type=jnp.float32)
            * expf[:, cols]
            + jnp.dot(
                leave, enterb[step, :, cols].astype(jnp.bfloat16),
                preferred_element_type=jnp.float32,
            )
            * expb[:, cols]
        )
        for pair in range(group_heads // 2):
            mats = []
            base = g * group_heads + 2 * pair
            for h in (base, base + 1):
                gap = jnp.where(
                    is_lower,
                    cumf[:, h : h + 1] - cumft[h : h + 1, :],
                    cumb[:, h : h + 1] - cumbt[h : h + 1, :],
                )
                sf, sb = stft[h : h + 1, :], stbt[h : h + 1, :]
                amount = jnp.where(is_diagonal, sf + sb, jnp.where(is_lower, sf, sb))
                mats.append((crossed * jnp.exp(gap) * amount).astype(jnp.bfloat16))
            two = slice(base * head_size, (base + 2) * head_size)
            x = act_ref[:, two]
            zero = jnp.zeros_like(x)
            stacked = jnp.concatenate(
                [jnp.where(lane < head_size, x, zero), jnp.where(lane < head_size, zero, x)], axis=0
            )
            y[:, two] += jnp.dot(
                jnp.concatenate(mats, axis=1), stacked, preferred_element_type=jnp.float32
            )
        gate = gate_ref[:, cols].astype(jnp.float32)
        mixed = y[:, cols] * (gate / (1.0 + jnp.exp(-gate)))
        scale = lax.rsqrt(jnp.mean(mixed * mixed, axis=1, keepdims=True) + NORM_EPS)
        out_ref[:, cols] = (mixed * scale * gain_ref[:, cols]).astype(jnp.bfloat16)
    totf = spread(jnp.exp(jnp.broadcast_to(cumf[size - 1 : size], (8, heads))), inner)[0:1]
    carryf[...] = carryf[...] * totf + freshf_ref[0]


def middle_kernel(
    head_size, key_heads, count, sink_ref, query_ref, rim_ref, packf_ref, packb_ref, out_ref,
    enter_ref, scores, raised, bottoms, flipped, turned, bias, mate_in, pair_out, pair_in, gathered,
    reach, back_out, back_in, mate_send, mate_recv, pair_send, pair_recv, back_send, back_recv,
):
    me = lax.axis_index("sp")
    parity = lax.rem(me, 2)
    place = lax.div(me, 2)
    pairs = count // 2
    mate = me + 1 - 2 * parity
    is_even = parity == 0
    packs = (packf_ref, packb_ref)
    states = STATE_SIZE

    def copy(source, target, sends, receives, device):
        return pltpu.make_async_remote_copy(
            src_ref=source, dst_ref=target, send_sem=sends, recv_sem=receives,
            device_id={"sp": device}, device_id_type=MESH,
        )

    def to_mate(d):
        return copy(
            packs[d].at[1 - parity], mate_in.at[d], mate_send.at[d], mate_recv.at[d], mate
        )

    def to_pair(d, k):
        device = me + 2 * k if d == 0 else me - 2 * k
        return copy(
            pair_out.at[d], pair_in.at[d, k - 1], pair_send.at[d, k - 1], pair_recv.at[d, k - 1],
            device,
        )

    def back_to_mate(d):
        return copy(back_out.at[d], back_in.at[d], back_send.at[d], back_recv.at[d], mate)

    def sends_to(d, k):
        return place + k < pairs if d == 0 else place - k >= 0

    def hears_from(d, k):
        return place - k >= 0 if d == 0 else place + k < pairs

    barrier = pltpu.get_barrier_semaphore()
    pl.semaphore_signal(barrier, inc=1, device_id={"sp": mate}, device_id_type=MESH)
    for k in range(1, pairs):
        other = lax.rem(me + 2 * k, count)
        pl.semaphore_signal(barrier, inc=1, device_id={"sp": other}, device_id_type=MESH)
    pl.semaphore_wait(barrier, pairs)
    for d in range(2):
        to_mate(d).start()

    def even_and_odd(d):
        own, other = packs[d][parity].astype(jnp.float32), mate_in[d].astype(jnp.float32)
        return jnp.where(is_even, own, other), jnp.where(is_even, other, own)

    def join_pair():
        for d in range(2):
            to_mate(d).wait_recv()
            even, odd = even_and_odd(d)
            near, far = (odd, even) if d == 0 else (even, odd)
            decay = near[states : states + 1]
            pair_out[d, :states, :] = (near[:states] + decay * far[:states]).astype(jnp.bfloat16)
            pair_out[d, states:, :] = (near[states:] * far[states:]).astype(jnp.bfloat16)
        for k in range(1, pairs):
            for d in range(2):
                @pl.when(sends_to(d, k))
                def _(d=d, k=k):
                    to_pair(d, k).start()

    def join_all():
        gathered[...] = jnp.zeros_like(gathered)
        reach[...] = jnp.ones_like(reach)
        for k in range(1, pairs):
            for d in range(2):
                @pl.when(hears_from(d, k))
                def _(d=d, k=k):
                    to_pair(d, k).wait_recv()
                    came = pair_in[d, k - 1].astype(jnp.float32)
                    gathered[d] = gathered[d] + reach[d, 0:1] * came[:states]
                    reach[d] = reach[d] * came[states : states + 8]
        for d in range(2):
            even, odd = even_and_odd(d)
            base = even if d == 0 else odd
            plain = gathered[d]
            moved = base[:states] + base[states : states + 1] * plain
            plain_is_mine = is_even if d == 0 else jnp.logical_not(is_even)
            enter_ref[d, parity] = jnp.where(plain_is_mine, plain, moved)
            back_out[d] = jnp.where(plain_is_mine, moved, plain).astype(jnp.bfloat16)
            back_to_mate(d).start()

    rows, block = query_ref.shape[0], WINDOW
    span = block + 2 * WINDOW
    blocks = rows // block
    heads = query_ref.shape[1] // head_size
    ratio = heads // key_heads
    values_at = key_heads * head_size
    flipped[...] = jnp.transpose(rim_ref[:, values_at:])
    scale = head_size ** (-0.5)
    key_row = lax.broadcasted_iota(jnp.int32, (span, block), 0)
    query_col = lax.broadcasted_iota(jnp.int32, (span, block), 1)
    in_band = (key_row >= query_col) & (key_row <= query_col + 2 * WINDOW)

    @pl.loop(0, blocks)
    def _(step):
        @pl.when(step == (3 * blocks) // 8)
        def _():
            join_pair()

        @pl.when(step == (7 * blocks) // 8)
        def _():
            join_all()

        start = pl.multiple_of(step * block, block)
        position = me * rows + start - WINDOW + key_row
        bias[...] = jnp.where(
            in_band & (position >= 0) & (position < count * rows), 0.0, NEG_FILL
        )
        tops = []
        for h in range(heads):
            k = h // ratio
            scores[h] = lax.dot_general(
                rim_ref[pl.ds(start, span), k * head_size : (k + 1) * head_size],
                query_ref[pl.ds(start, block), h * head_size : (h + 1) * head_size],
                (((1,), (1,)), ((), ())), preferred_element_type=jnp.float32,
            ) * scale + bias[...]
        for h in range(heads):
            top = jnp.maximum(jnp.max(scores[h], axis=0, keepdims=True), sink_ref[h])
            lifted = jnp.exp(scores[h] - top)
            bottoms[h : h + 1] = jnp.sum(lifted, axis=0, keepdims=True) + jnp.exp(sink_ref[h] - top)
            raised[h] = lifted.astype(jnp.bfloat16)
        for h in range(heads):
            k = h // ratio
            turned[h * head_size : (h + 1) * head_size, :] = jnp.dot(
                flipped[k * head_size : (k + 1) * head_size, pl.ds(start, span)], raised[h],
                preferred_element_type=jnp.float32,
            ) * (1.0 / bottoms[h : h + 1])
        out_ref[pl.ds(start, block), :] = jnp.transpose(turned[...]).astype(jnp.bfloat16)

    for d in range(2):
        back_to_mate(d).wait_recv()
        enter_ref[d, 1 - parity] = back_in[d].astype(jnp.float32)
    for d in range(2):
        to_mate(d).wait_send()
        back_to_mate(d).wait_send()
        for k in range(1, pairs):
            @pl.when(sends_to(d, k))
            def _(d=d, k=k):
                to_pair(d, k).wait_send()


def middle(query, rimmed, sink_logit, pack_forward, pack_backward, head_size, key_heads):
    rows, width = query.shape
    heads = width // head_size
    count = lax.axis_size("sp")
    hops = max(count // 2 - 1, 1)
    _, depth, half = pack_forward.shape
    span = 3 * WINDOW
    vmem = pl.BlockSpec(memory_space=pltpu.VMEM)
    dma = pltpu.SemaphoreType.DMA
    return pl.pallas_call(
        functools.partial(middle_kernel, head_size, key_heads, count),
        in_specs=[pl.BlockSpec(memory_space=pltpu.SMEM), vmem, vmem, vmem, vmem],
        out_specs=[vmem, vmem],
        out_shape=[
            jax.ShapeDtypeStruct((rows, width), jnp.bfloat16),
            jax.ShapeDtypeStruct((2, 2, STATE_SIZE, half), jnp.float32),
        ],
        scratch_shapes=[
            pltpu.VMEM((heads, span, WINDOW), jnp.float32),
            pltpu.VMEM((heads, span, WINDOW), jnp.bfloat16),
            pltpu.VMEM((heads, WINDOW), jnp.float32),
            pltpu.VMEM((key_heads * head_size, rimmed.shape[0]), jnp.bfloat16),
            pltpu.VMEM((width, WINDOW), jnp.float32),
            pltpu.VMEM((span, WINDOW), jnp.float32),
            pltpu.VMEM((2, depth, half), jnp.bfloat16),
            pltpu.VMEM((2, depth, half), jnp.bfloat16),
            pltpu.VMEM((2, hops, depth, half), jnp.bfloat16),
            pltpu.VMEM((2, STATE_SIZE, half), jnp.float32),
            pltpu.VMEM((2, 8, half), jnp.float32),
            pltpu.VMEM((2, STATE_SIZE, half), jnp.bfloat16),
            pltpu.VMEM((2, STATE_SIZE, half), jnp.bfloat16),
            dma((2,)), dma((2,)), dma((2, hops)), dma((2, hops)), dma((2,)), dma((2,)),
        ],
        compiler_params=pltpu.CompilerParams(collective_id=5, has_side_effects=True),
        cost_estimate=pl.CostEstimate(
            flops=4 * rows * span * width, bytes_accessed=4 * rows * width,
            transcendentals=rows * span * heads,
        ),
        name="middle",
    )(sink_logit, query, rimmed, pack_forward, pack_backward)


def combine_kernel(
    count, attn_ref, ssm_ref, attn_w_ref, ssm_w_ref, out_ref, acc, own, mate_out, mate_in,
    far_out, far_in, mate_send, mate_recv, far_send, far_recv,
):
    me = lax.axis_index("tp")
    core = lax.rem(me, 2)
    chip = lax.div(me, 2)
    chips = count // 2
    mate = me + 1 - 2 * core
    rows = out_ref.shape[0]
    pieces, width = own.shape[1], own.shape[3]

    def chip_of(slot):
        return lax.rem(chip + 1 + slot, chips)

    def to_mate(slot, j):
        return pltpu.make_async_remote_copy(
            src_ref=mate_out.at[slot, j], dst_ref=mate_in.at[slot, j],
            send_sem=mate_send.at[slot, j], recv_sem=mate_recv.at[slot, j],
            device_id={"tp": mate}, device_id_type=MESH,
        )

    def to_far(slot, j):
        return pltpu.make_async_remote_copy(
            src_ref=far_out.at[slot, j], dst_ref=far_in.at[slot, j],
            send_sem=far_send.at[slot, j], recv_sem=far_recv.at[slot, j],
            device_id={"tp": 2 * chip_of(slot) + core}, device_id_type=MESH,
        )

    barrier = pltpu.get_barrier_semaphore()
    pl.semaphore_signal(barrier, inc=1, device_id={"tp": mate}, device_id_type=MESH)
    for slot in range(chips - 1):
        pl.semaphore_signal(
            barrier, inc=1, device_id={"tp": 2 * chip_of(slot) + core}, device_id_type=MESH
        )
    pl.semaphore_wait(barrier, chips)

    def compute(slot, j):
        cols = pl.ds(pl.multiple_of(j * width, width), width)
        first = pl.multiple_of(chip_of(slot) * 2 * rows, rows)
        span = pl.ds(first, 2 * rows)
        acc[...] = jnp.dot(
            attn_ref[span, :], attn_w_ref[:, cols], preferred_element_type=jnp.float32
        ) + jnp.dot(ssm_ref[span, :], ssm_w_ref[:, cols], preferred_element_type=jnp.float32)
        other = acc[pl.ds(pl.multiple_of((1 - core) * rows, rows), rows), :]
        mate_out[slot, j] = other.astype(jnp.bfloat16)
        to_mate(slot, j).start()
        mine = acc[pl.ds(pl.multiple_of(core * rows, rows), rows), :]
        own[slot, j] = mine.astype(jnp.bfloat16)

    def forward(slot, j):
        to_mate(slot, j).wait_recv()
        far_out[slot, j] = (
            own[slot, j].astype(jnp.float32) + mate_in[slot, j].astype(jnp.float32)
        ).astype(jnp.bfloat16)
        to_far(slot, j).start()

    last = chips - 1
    for slot in range(chips):
        compute(slot, 0)
        if slot > 0:
            forward(slot - 1, pieces - 1)

        @pl.loop(1, pieces)
        def _(j, slot=slot):
            compute(slot, j)
            if slot < last:
                forward(slot, j - 1)

    @pl.loop(0, pieces)
    def _(j):
        to_mate(last, j).wait_recv()
        total = own[last, j].astype(jnp.float32) + mate_in[last, j].astype(jnp.float32)
        for slot in range(last):
            to_far(slot, j).wait_recv()
            total = total + far_in[slot, j].astype(jnp.float32)
        out_ref[:, pl.ds(pl.multiple_of(j * width, width), width)] = total.astype(jnp.bfloat16)

    @pl.loop(0, pieces)
    def _(j):
        for slot in range(chips):
            to_mate(slot, j).wait_send()
        for slot in range(last):
            to_far(slot, j).wait_send()


def combine(attn_out, ssm_out, attn_weight, ssm_weight):
    count = lax.axis_size("tp")
    chips = count // 2
    total, width = attn_out.shape[0], attn_weight.shape[1]
    rows = total // count
    pieces = width // PIECE
    far = max(chips - 1, 1)
    vmem = pl.BlockSpec(memory_space=pltpu.VMEM)
    depth = attn_out.shape[1] + ssm_out.shape[1]
    return pl.pallas_call(
        functools.partial(combine_kernel, count),
        in_specs=[vmem] * 4,
        out_specs=vmem,
        out_shape=jax.ShapeDtypeStruct((rows, width), jnp.bfloat16),
        scratch_shapes=[
            pltpu.VMEM((2 * rows, PIECE), jnp.float32),
            pltpu.VMEM((chips, pieces, rows, PIECE), jnp.bfloat16),
            pltpu.VMEM((chips, pieces, rows, PIECE), jnp.bfloat16),
            pltpu.VMEM((chips, pieces, rows, PIECE), jnp.bfloat16),
            pltpu.VMEM((far, pieces, rows, PIECE), jnp.bfloat16),
            pltpu.VMEM((far, pieces, rows, PIECE), jnp.bfloat16),
            pltpu.SemaphoreType.DMA((chips, pieces)),
            pltpu.SemaphoreType.DMA((chips, pieces)),
            pltpu.SemaphoreType.DMA((far, pieces)),
            pltpu.SemaphoreType.DMA((far, pieces)),
        ],
        compiler_params=pltpu.CompilerParams(collective_id=3, has_side_effects=True),
        cost_estimate=pl.CostEstimate(
            flops=2 * total * depth * width, bytes_accessed=2 * depth * width, transcendentals=0
        ),
        name="combine",
    )(attn_out, ssm_out, attn_weight, ssm_weight)


def chunk_states(rimmed, taps, tap_count, inner, maps, decay, step):
    rows = rimmed.shape[0] - 2 * HALO
    total, heads, chunks = rimmed.shape[1], decay[0].shape[1], rows // CHUNK
    small = pl.BlockSpec((CHUNK, heads), lambda i: (i, 0))
    fresh = pl.BlockSpec((1, STATE_SIZE, inner), lambda i: (i, 0, 0))
    packed = (2, STATE_SIZE + PACK_ROWS, inner // 2)
    end = pl.BlockSpec(packed, lambda i: (0, 0, 0))
    fresh_shape = jax.ShapeDtypeStruct((chunks, STATE_SIZE, inner), jnp.float32)
    end_shape = jax.ShapeDtypeStruct(packed, jnp.bfloat16)
    return pl.pallas_call(
        functools.partial(states_kernel, tap_count, inner, maps),
        grid=(chunks,),
        in_specs=[
            pl.BlockSpec(rimmed.shape, lambda i: (0, 0)),
            pl.BlockSpec(taps.shape, lambda i: (0, 0)),
            small, small, small, small,
        ],
        out_specs=[pl.BlockSpec((CHUNK, total), lambda i: (i, 0)), fresh, fresh, end, end],
        out_shape=[
            jax.ShapeDtypeStruct((rows, total), jnp.bfloat16),
            fresh_shape, fresh_shape, end_shape, end_shape,
        ],
        scratch_shapes=[
            pltpu.VMEM((CHUNK + 2 * HALO, total), jnp.float32),
            pltpu.VMEM((8, inner), jnp.float32),
            pltpu.VMEM((STATE_SIZE, inner), jnp.float32),
            pltpu.VMEM((STATE_SIZE, inner), jnp.float32),
            pltpu.VMEM((2, 8, heads), jnp.float32),
        ],
        cost_estimate=pl.CostEstimate(
            flops=8 * rows * inner * STATE_SIZE, bytes_accessed=16 * rows * inner,
            transcendentals=rows * total,
        ),
        name="chunk_states",
    )(rimmed, taps, *decay, *step)


def chunk_outputs(head_size, inner, maps, act, decay, step, fresh, incoming, gate, gain):
    rows, total = act.shape
    heads, chunks = decay[0].shape[1], rows // CHUNK
    small = pl.BlockSpec((CHUNK, heads), lambda i: (i, 0))
    turned = pl.BlockSpec((heads, CHUNK), lambda i: (0, i))
    return pl.pallas_call(
        functools.partial(outputs_kernel, head_size, inner, maps),
        grid=(chunks,),
        in_specs=[
            pl.BlockSpec((CHUNK, total), lambda i: (i, 0)),
            small, small, small, small, turned, turned, turned, turned,
            pl.BlockSpec((rows, heads), lambda i: (0, 0)),
            pl.BlockSpec((1, STATE_SIZE, inner), lambda i: (i, 0, 0)),
            pl.BlockSpec((chunks, STATE_SIZE, inner), lambda i: (0, 0, 0)),
            pl.BlockSpec(incoming.shape, lambda i: (0, 0, 0, 0)),
            pl.BlockSpec((CHUNK, inner), lambda i: (i, 0)),
            pl.BlockSpec((1, inner), lambda i: (0, 0)),
        ],
        out_specs=pl.BlockSpec((CHUNK, inner), lambda i: (i, 0)),
        out_shape=jax.ShapeDtypeStruct((rows, inner), jnp.bfloat16),
        scratch_shapes=[
            pltpu.VMEM((STATE_SIZE, inner), jnp.float32),
            pltpu.VMEM((chunks, STATE_SIZE, inner), jnp.float32),
            pltpu.VMEM((CHUNK, inner), jnp.float32),
        ],
        cost_estimate=pl.CostEstimate(
            flops=8 * rows * inner * STATE_SIZE, bytes_accessed=16 * rows * inner,
            transcendentals=rows * CHUNK * heads,
        ),
        name="chunk_outputs",
    )(
        act, *decay, *step, decay[0].T, decay[1].T, step[0].T, step[1].T, decay[1],
        fresh[0], fresh[1], incoming, gate, gain,
    )


def local(
    tokens,
    norm_gain,
    query_weight,
    key_weight,
    value_weight,
    query_gain,
    key_gain,
    sink_logit,
    gate_weight,
    inner_weight,
    input_map,
    output_map,
    step_weight,
    conv_inner,
    conv_pair,
    decay_rate,
    decay_jump,
    inner_gain,
    attn_out_weight,
    ssm_out_weight,
):
    row_total = tokens.shape[0]
    seq_first = lax.axis_index("sp") * row_total
    positions = seq_first + jnp.arange(row_total, dtype=jnp.int32)
    normed = rms_rows(tokens.astype(jnp.float32), norm_gain.astype(jnp.float32)).astype(
        jnp.bfloat16
    )

    def project(weight):
        result = jnp.dot(normed, weight, preferred_element_type=jnp.float32)
        return lax.optimization_barrier(result.astype(jnp.bfloat16))

    head_size = query_gain.shape[0]
    query = project(query_weight).reshape(row_total, -1, head_size)
    keyed = project(key_weight).reshape(row_total, -1, head_size)
    value = project(value_weight)
    query = rotate(rms_rows(query.astype(jnp.float32), query_gain), positions).astype(jnp.bfloat16)
    keyed = rotate(rms_rows(keyed.astype(jnp.float32), key_gain), positions).astype(jnp.bfloat16)
    key_heads = keyed.shape[1]
    packed = jnp.concatenate([keyed.reshape(row_total, -1), value], axis=1)
    rimmed_keys = extended(packed, (("sp", 0),), WINDOW)
    inner_rows = project(inner_weight)
    inner_width = inner_rows.shape[1]
    map_width = input_map.shape[1]
    carried_in = jnp.concatenate([inner_rows, project(input_map), project(output_map)], axis=1)
    tap_count = conv_inner.shape[0]
    conv_table = jnp.concatenate([conv_inner, conv_pair.reshape(tap_count, -1)], axis=1).astype(
        jnp.float32
    )
    rimmed_rows = extended(carried_in, (("sp", 0),), HALO)
    step_rows = project(step_weight.reshape(step_weight.shape[0], -1))
    step = jax.nn.softplus(step_rows.astype(jnp.float32))
    log_decay = -decay_rate.reshape(1, -1) * step + decay_jump.reshape(row_total, -1)
    heads_here = inner_width // head_size
    steps = (step[:, :heads_here], step[:, heads_here:])
    decays = (log_decay[:, :heads_here], log_decay[:, heads_here:])
    act, fresh_forward, fresh_backward, pack_forward, pack_backward = chunk_states(
        rimmed_rows, conv_table, tap_count, inner_width, map_width, decays, steps
    )
    attn_out, incoming = middle(
        query.reshape(row_total, -1), rimmed_keys, sink_logit, pack_forward, pack_backward,
        head_size, key_heads,
    )
    gate_rows = project(gate_weight)
    ssm_out = chunk_outputs(
        head_size, inner_width, map_width, act, decays, steps, (fresh_forward, fresh_backward),
        incoming, gate_rows, inner_gain.astype(jnp.float32)[None, :],
    )
    return combine(attn_out, ssm_out, attn_out_weight, ssm_out_weight)


def solution(mesh):
    in_specs = (
        P("sp", None),
        P(),
        P(None, "tp"),
        P(None, "tp"),
        P(None, "tp"),
        P(),
        P(),
        P("tp"),
        P(None, "tp"),
        P(None, "tp"),
        P(None, "tp"),
        P(None, "tp"),
        P(None, None, "tp"),
        P(None, "tp"),
        P(None, None, "tp"),
        P(None, "tp"),
        P("sp", None, "tp"),
        P("tp"),
        P("tp", None),
        P("tp", None),
    )
    out_specs = P(("sp", "tp"), None)
    return jax.shard_map(local, mesh=mesh, in_specs=in_specs, out_specs=out_specs, check_vma=False)
```

```python
import functools

import jax
import jax.numpy as jnp
import numpy as np
from jax import lax
from jax.experimental import pallas as pl
from jax.experimental.pallas import tpu as pltpu
from jax.sharding import PartitionSpec as P

STATE_SIZE = 128
WINDOW = 128
CHUNK = 128
HALO = 16

NORM_EPS = 1e-05
ROPE_BASE = 500000.0
NEG_FILL = -1e30
PIECE = 256
TILE = 512
MIB = 1 << 20
PACK_ROWS = 16
MESH = pl.DeviceIdType.MESH


def spread(factor, width):
    heads = factor.shape[1]
    row = lax.broadcasted_iota(jnp.int32, (heads, width), 0)
    column = lax.broadcasted_iota(jnp.int32, (heads, width), 1)
    head_size = width // heads
    ones = jnp.where(
        (column >= row * head_size) & (column < (row + 1) * head_size), 1.0, 0.0
    ).astype(jnp.bfloat16)
    return jnp.dot(factor.astype(jnp.bfloat16), ones, preferred_element_type=jnp.float32)


def exact_dot(a, b):
    return jnp.dot(a, b, precision=lax.Precision.HIGHEST, preferred_element_type=jnp.float32)


def triangle(size, lower):
    row = lax.broadcasted_iota(jnp.int32, (size, size), 0)
    column = lax.broadcasted_iota(jnp.int32, (size, size), 1)
    return jnp.where(row >= column if lower else row <= column, 1.0, 0.0)


def project_kernel(
    head_size, heads, key_width, tokens_ref, inner_hbm, in_hbm, out_hbm, key_hbm, value_hbm,
    query_hbm, gate_hbm, step_ref, small_ref, jump_ref, query_ref, keyed_ref, rows_ref, gate_ref,
    table_ref, turned_ref, tokens, normed, inner_w, in_w, out_w, keyed_w, query_w, gate_w, raw,
    cosine, sine, token_sems, weight_sems,
):
    total, depth = tokens.shape
    parts = token_sems.shape[0]
    size = total // parts
    moves = [
        pltpu.make_async_copy(
            tokens_ref.at[pl.ds(i * size, size)], tokens.at[pl.ds(i * size, size)],
            token_sems.at[i],
        )
        for i in range(parts)
    ]
    joined = key_width % 128 == 0
    if joined:
        key_w, value_w = keyed_w.at[:, :key_width], keyed_w.at[:, key_width:]
    else:
        key_w, value_w = keyed_w.at[0], keyed_w.at[1]
    weights = (
        (key_hbm, key_w), (value_hbm, value_w), (query_hbm, query_w), (in_hbm, in_w),
        (out_hbm, out_w), (inner_hbm, inner_w), (gate_hbm, gate_w),
    )
    loads = [
        pltpu.make_async_copy(source, target, weight_sems.at[i])
        for i, (source, target) in enumerate(weights)
    ]
    for move in moves + loads:
        move.start()
    lanes = depth // 128
    frequency, sign = small_ref[lanes + 2 : lanes + 3], small_ref[lanes + 3 : lanes + 4]
    order = lax.broadcasted_iota(jnp.int32, (32, 128), 0)
    first = lax.axis_index("sp") * total
    near = order.astype(jnp.float32) * frequency
    cos_near, sin_near = jnp.cos(near), jnp.sin(near)
    for a in range(0, total, 1024):
        far = (first + a + 32 * order).astype(jnp.float32) * frequency
        cos_far, sin_far = jnp.cos(far), jnp.sin(far)
        for r in range(min(32, (total - a) // 32)):
            c, d = cos_far[r : r + 1], sin_far[r : r + 1]
            span = slice(a + r * 32, a + (r + 1) * 32)
            cosine[span, :] = c * cos_near - d * sin_near
            sine[span, :] = (d * cos_near + c * sin_near) * sign
    for i in range(parts):
        moves[i].wait()

        @pl.loop(0, size // 32)
        def _(r, i=i):
            span = pl.ds(pl.multiple_of(i * size + r * 32, 32), 32)
            squares = jnp.zeros((32, 128), jnp.float32)
            for j in range(lanes):
                x = tokens[span, j * 128 : (j + 1) * 128].astype(jnp.float32)
                squares = squares + x * x
            mean = jnp.sum(squares, axis=-1, keepdims=True) * (1.0 / depth)
            scale = lax.rsqrt(mean + NORM_EPS)
            for j in range(lanes):
                cols = slice(j * 128, (j + 1) * 128)
                x = tokens[span, cols].astype(jnp.float32)
                normed[span, cols] = (x * scale * small_ref[j : j + 1]).astype(jnp.bfloat16)

    def run(weight, target, column, beside=None):
        width = min(weight.shape[1], TILE)
        count = weight.shape[1] // width

        def tile(j):
            at = j * width if count == 1 else pl.multiple_of(j * width, width)
            target[:, pl.ds(column + at, width)] = jnp.dot(
                normed[...], weight[:, pl.ds(at, width)], preferred_element_type=jnp.float32
            ).astype(jnp.bfloat16)
            if beside is not None:
                beside(j, total // count)

        if count == 1:
            tile(0)
        else:
            pl.loop(0, count)(tile)

    raw[:, 2 * heads :] = jnp.zeros((total, 128 - 2 * heads), jnp.float32)
    raw[:, : 2 * heads] = lax.dot_general(
        normed[...], step_ref[...], (((1,), (1,)), ((), ())), preferred_element_type=jnp.float32
    ).astype(jnp.bfloat16).astype(jnp.float32)
    rates = jnp.transpose(jnp.broadcast_to(small_ref[lanes + 4 : lanes + 5], (128, 128)))
    rates = rates[: 2 * heads, 0:1]
    upper, lower = triangle(CHUNK, False), triangle(CHUNK, True)

    def steps(j, length):
        for c in range(length // CHUNK):
            at = pl.multiple_of(j * length + c * CHUNK, CHUNK)
            span = pl.ds(at, CHUNK)
            x = jnp.transpose(raw[span, :])[: 2 * heads]
            step = jnp.maximum(x, 0.0) + jnp.log1p(jnp.exp(-jnp.abs(x)))
            decay = jump_ref[:, span] - rates * step
            filled = jnp.concatenate(
                [
                    exact_dot(decay[:heads], upper), exact_dot(decay[heads:], lower), step,
                    jnp.zeros((128 - 4 * heads, CHUNK), jnp.float32),
                ],
                axis=0,
            )
            turned_ref[:, span] = filled
            table_ref[span, :] = jnp.transpose(filled)

    row = lax.broadcasted_iota(jnp.int32, (256, 128), 0)
    column = lax.broadcasted_iota(jnp.int32, (256, 128), 1)
    same_head = jnp.where(
        lax.rem(row, 128) // head_size == column // head_size, 1.0, 0.0
    ).astype(jnp.bfloat16)
    lane = lax.broadcasted_iota(jnp.int32, (128, 128), 1)
    half = head_size // 2
    first_half = lax.rem(lane, head_size) < half

    def rotate(value, gain_row, cos_here, sin_here):
        square = value * value
        high = square.astype(jnp.bfloat16)
        low = (square - high.astype(jnp.float32)).astype(jnp.bfloat16)
        sums = jnp.dot(
            jnp.concatenate([high, low], axis=1), same_head, preferred_element_type=jnp.float32
        )
        value = value * lax.rsqrt(sums * (1.0 / head_size) + NORM_EPS) * gain_row
        swapped = jnp.where(
            first_half, pltpu.roll(value, 128 - half, 1), pltpu.roll(value, half, 1)
        )
        return (value * cos_here + swapped * sin_here).astype(jnp.bfloat16)

    def heads_of(j, length):
        for i in range(length // 128):
            span = pl.ds(pl.multiple_of(j * length + i * 128, 128), 128)
            cos_here, sin_here = cosine[span, :], sine[span, :]
            for at in range(0, query_ref.shape[1], 128):
                value = query_ref[span, at : at + 128].astype(jnp.float32)
                query_ref[span, at : at + 128] = rotate(
                    value, small_ref[lanes : lanes + 1], cos_here, sin_here
                )
            for at in range(0, key_width, 128):
                packed = keyed_ref[span, at : at + 128]
                keys = rotate(
                    packed.astype(jnp.float32), small_ref[lanes + 1 : lanes + 2], cos_here, sin_here
                )
                keyed_ref[span, at : at + 128] = jnp.where(lane + at < key_width, keys, packed)

    inner, maps = inner_w.shape[1], in_w.shape[1]
    loads[0].wait()
    loads[1].wait()
    if joined:
        run(keyed_w, keyed_ref, 0)
    else:
        run(keyed_w.at[0], keyed_ref, 0)
        run(keyed_w.at[1], keyed_ref, key_width)
    loads[2].wait()
    run(query_w, query_ref, 0)
    loads[3].wait()
    run(in_w, rows_ref, inner)
    loads[4].wait()
    run(out_w, rows_ref, inner + maps)
    loads[5].wait()
    run(inner_w, rows_ref, 0, steps)
    loads[6].wait()
    run(gate_w, gate_ref, 0, heads_of)


def project_all(
    tokens, norm_gain, inner_weight, input_map, output_map, key_weight, value_weight, query_weight,
    gate_weight, step_weight, query_gain, key_gain, decay_rate, decay_jump,
):
    total, depth = tokens.shape
    head_size = query_gain.shape[0]
    half = head_size // 2
    lane = np.arange(128)
    frequency = (ROPE_BASE ** (-2.0 * (lane % half) / head_size)).astype(np.float32)
    sign = np.where(lane % head_size < half, -1.0, 1.0).astype(np.float32)
    repeats = 128 // head_size
    rates = decay_rate.reshape(-1)
    small = jnp.concatenate(
        [
            norm_gain.astype(jnp.float32), jnp.tile(query_gain, repeats) * head_size ** (-0.5),
            jnp.tile(key_gain, repeats), frequency, sign, rates,
            jnp.zeros((4 * 128 - rates.shape[0],), jnp.float32),
        ]
    ).reshape(-1, 128)
    turned_step = jnp.transpose(step_weight, (1, 2, 0)).reshape(-1, depth)
    turned_jump = jnp.transpose(decay_jump, (1, 2, 0)).reshape(-1, total)
    heads = step_weight.shape[2]
    inner, maps = inner_weight.shape[1], input_map.shape[1]
    width, key_width = query_weight.shape[1], key_weight.shape[1]
    whole = pl.BlockSpec(memory_space=pltpu.HBM)
    vmem = pl.BlockSpec(memory_space=pltpu.VMEM)
    big = (inner_weight, input_map, output_map, key_weight, value_weight, query_weight, gate_weight)
    columns = sum(w.shape[1] for w in big)
    keyed_shape = (depth, 2 * key_width) if key_width % 128 == 0 else (2, depth, key_width)

    def shape(*dims, kind=jnp.bfloat16):
        return jax.ShapeDtypeStruct(dims, kind)

    def room(*dims, kind=jnp.bfloat16):
        return pltpu.VMEM(dims, kind)

    return pl.pallas_call(
        functools.partial(project_kernel, head_size, heads, key_width),
        in_specs=[whole] * 8 + [vmem] * 3,
        out_specs=[vmem] * 6,
        out_shape=[
            shape(total, width), shape(total, 2 * key_width), shape(total, inner + 2 * maps),
            shape(total, inner), shape(total, 128, kind=jnp.float32),
            shape(128, total, kind=jnp.float32),
        ],
        scratch_shapes=[
            room(total, depth), room(total, depth), room(*inner_weight.shape),
            room(*input_map.shape), room(*output_map.shape), room(*keyed_shape),
            room(*query_weight.shape), room(*gate_weight.shape),
            room(total, 128, kind=jnp.float32), room(total, 128, kind=jnp.float32),
            room(total, 128, kind=jnp.float32),
            pltpu.SemaphoreType.DMA((8,)), pltpu.SemaphoreType.DMA((7,)),
        ],
        compiler_params=pltpu.CompilerParams(vmem_limit_bytes=52 * MIB),
        cost_estimate=pl.CostEstimate(
            flops=2 * total * depth * columns, bytes_accessed=2 * depth * (columns + total),
            transcendentals=total * 128,
        ),
        name="project",
    )(tokens, *big, turned_step, small, turned_jump)


def convolve_kernel(
    tap_count, inner, maps, heads, count, rows_ref, keyed_ref, taps_ref, table_ref, act_ref,
    freshf_ref, freshb_ref, packf_ref, packb_ref, rim_ref, spare, low_rows, high_rows, low_keys,
    high_keys, endf, endb, sends, receives,
):
    me = lax.axis_index("sp")
    total = rows_ref.shape[0]
    size = CHUNK
    chunks = total // size

    def copies(up):
        device = me + 1 if up else me - 1
        slot = 0 if up else 2
        edge = pl.ds(total - HALO if up else 0, HALO)
        wide = pl.ds(total - WINDOW if up else 0, WINDOW)
        pairs = (
            (rows_ref.at[edge], low_rows if up else high_rows),
            (keyed_ref.at[wide], low_keys if up else high_keys),
        )
        return [
            pltpu.make_async_remote_copy(
                src_ref=source, dst_ref=target, send_sem=sends.at[slot + i],
                recv_sem=receives.at[slot + i], device_id={"sp": device}, device_id_type=MESH,
            )
            for i, (source, target) in enumerate(pairs)
        ]

    barrier = pltpu.get_barrier_semaphore()
    for step in (1, count - 1):
        pl.semaphore_signal(
            barrier, inc=1, device_id={"sp": lax.rem(me + step, count)}, device_id_type=MESH
        )
    pl.semaphore_wait(barrier, 2)
    has_low, has_high = me > 0, me < count - 1

    @pl.when(has_high)
    def _():
        for copy in copies(True):
            copy.start()

    @pl.when(has_low)
    def _():
        for copy in copies(False):
            copy.start()

    @pl.when(jnp.logical_not(has_low))
    def _():
        low_rows[...] = jnp.zeros_like(low_rows)
        low_keys[...] = jnp.zeros_like(low_keys)

    @pl.when(jnp.logical_not(has_high))
    def _():
        high_rows[...] = jnp.zeros_like(high_rows)
        high_keys[...] = jnp.zeros_like(high_keys)

    rim_ref[WINDOW : WINDOW + total, :] = keyed_ref[...]

    @pl.loop(0, chunks)
    def _(turn):
        c = lax.rem(turn + 1, chunks)
        start = pl.multiple_of(c * size, size)
        spare[HALO : HALO + size, :] = rows_ref[pl.ds(start, size), :].astype(jnp.float32)

        @pl.when(turn == chunks - 2)
        def _():
            @pl.when(has_low)
            def _():
                for copy in copies(True):
                    copy.wait_recv()

            @pl.when(has_high)
            def _():
                for copy in copies(False):
                    copy.wait_recv()

        @pl.when(c == 0)
        def _():
            spare[:HALO, :] = low_rows[...].astype(jnp.float32)

        @pl.when(c > 0)
        def _():
            at = pl.multiple_of(start - HALO, HALO)
            spare[:HALO, :] = rows_ref[pl.ds(at, HALO), :].astype(jnp.float32)

        @pl.when(c == chunks - 1)
        def _():
            spare[HALO + size :, :] = high_rows[...].astype(jnp.float32)

        @pl.when(c < chunks - 1)
        def _():
            at = pl.multiple_of(start + size, HALO)
            spare[HALO + size :, :] = rows_ref[pl.ds(at, HALO), :].astype(jnp.float32)

        first = HALO - tap_count // 2
        for at in range(0, inner + 2 * maps, 128):
            cols = slice(at, at + 128)
            filtered = spare[first : first + size, cols] * taps_ref[0:1, cols]
            for k in range(1, tap_count):
                filtered = (
                    filtered + spare[first + k : first + k + size, cols] * taps_ref[k : k + 1, cols]
                )
            act_ref[pl.ds(start, size), cols] = (
                filtered * (1.0 / (1.0 + jnp.exp(-filtered)))
            ).astype(jnp.bfloat16)

    rim_ref[:WINDOW, :] = low_keys[...]
    rim_ref[WINDOW + total :, :] = high_keys[...]
    groups = maps // STATE_SIZE
    width = inner // groups

    @pl.loop(0, chunks)
    def _(c):
        span = pl.ds(pl.multiple_of(c * size, size), size)
        table = table_ref[span, :]
        cumf, cumb = table[:, :heads], table[:, heads : 2 * heads]
        wf = jnp.exp(cumf[size - 1 : size] - cumf) * table[:, 2 * heads : 3 * heads]
        wb = jnp.exp(cumb[0:1] - cumb) * table[:, 3 * heads : 4 * heads]
        signal = act_ref[span, :inner].astype(jnp.float32)
        xf = (signal * spread(wf, inner)).astype(jnp.bfloat16)
        xb = (signal * spread(wb, inner)).astype(jnp.bfloat16)
        for g in range(groups):
            cols = slice(g * width, (g + 1) * width)
            entry = act_ref[span, inner + g * STATE_SIZE : inner + (g + 1) * STATE_SIZE]
            turned = jnp.transpose(entry)
            freshf_ref[c, :, cols] = jnp.dot(turned, xf[:, cols], preferred_element_type=jnp.float32)
            freshb_ref[c, :, cols] = jnp.dot(turned, xb[:, cols], preferred_element_type=jnp.float32)

    endf[...] = jnp.zeros_like(endf)
    endb[...] = jnp.zeros_like(endb)

    def total_decay(c, forward):
        row = c * size + size - 1 if forward else c * size
        at = 0 if forward else heads
        return table_ref[pl.ds(row, 1), :][:, at : at + heads]

    def wide(log_row):
        return spread(jnp.exp(jnp.broadcast_to(log_row, (8, heads))), inner)

    for c in range(chunks):
        endf[...] = endf[...] * wide(total_decay(c, True))[0:1] + freshf_ref[c]
        r = chunks - 1 - c
        endb[...] = endb[...] * wide(total_decay(r, False))[0:1] + freshb_ref[r]
    half = inner // 2
    for forward, end, pack_ref in ((True, endf, packf_ref), (False, endb, packb_ref)):
        logs = total_decay(0, forward)
        for c in range(1, chunks):
            logs = logs + total_decay(c, forward)
        decay = wide(logs).astype(jnp.bfloat16)
        for side in range(2):
            cols = slice(side * half, (side + 1) * half)
            pack_ref[side, :STATE_SIZE, :] = end[:, cols].astype(jnp.bfloat16)
            pack_ref[side, STATE_SIZE:, :] = jnp.concatenate([decay, decay], axis=0)[:, cols]

    @pl.when(has_high)
    def _():
        for copy in copies(True):
            copy.wait_send()

    @pl.when(has_low)
    def _():
        for copy in copies(False):
            copy.wait_send()


def outputs_kernel(
    head_size, inner, maps, act_ref, table_ref, turned_ref, tables_ref, freshf_ref, freshb_ref,
    enter_ref, gate_ref, gain_ref,
    out_ref, carryf, enterb, y,
):
    step = pl.program_id(0)
    chunks = pl.num_programs(0)
    size = act_ref.shape[0]
    heads = inner // head_size

    @pl.when(step == 0)
    def _():
        half = inner // 2
        for side in range(2):
            carryf[:, side * half : (side + 1) * half] = enter_ref[0, side]
            enterb[chunks - 1, :, side * half : (side + 1) * half] = enter_ref[1, side]

        @pl.loop(0, chunks - 1)
        def _(k):
            at = chunks - 1 - k
            part = tables_ref[pl.ds(pl.multiple_of(at * size, size), 8), :]
            tot = jnp.exp(part[0:1, heads : 2 * heads])
            tot = spread(jnp.broadcast_to(tot, (8, heads)), inner)[0:1]
            enterb[at - 1] = enterb[at] * tot + freshb_ref[at]

    cumf, cumb = table_ref[:, :heads], table_ref[:, heads : 2 * heads]
    cumft, cumbt = turned_ref[:heads, :], turned_ref[heads : 2 * heads, :]
    stft, stbt = turned_ref[2 * heads : 3 * heads, :], turned_ref[3 * heads : 4 * heads, :]
    row = lax.broadcasted_iota(jnp.int32, (size, size), 0)
    column = lax.broadcasted_iota(jnp.int32, (size, size), 1)
    is_lower, is_diagonal = row >= column, row == column
    groups = maps // STATE_SIZE
    width = inner // groups
    group_heads = heads // groups
    expf = spread(jnp.exp(cumf), inner)
    expb = spread(jnp.exp(cumb), inner)
    lane = lax.broadcasted_iota(jnp.int32, (size, 2 * head_size), 1)
    for g in range(groups):
        cols = slice(g * width, (g + 1) * width)
        entry = act_ref[:, inner + g * STATE_SIZE : inner + (g + 1) * STATE_SIZE]
        leave = act_ref[:, inner + maps + g * STATE_SIZE : inner + maps + (g + 1) * STATE_SIZE]
        crossed = lax.dot_general(
            leave, entry, (((1,), (1,)), ((), ())), preferred_element_type=jnp.float32
        )
        y[:, cols] = (
            jnp.dot(leave, carryf[:, cols].astype(jnp.bfloat16), preferred_element_type=jnp.float32)
            * expf[:, cols]
            + jnp.dot(
                leave, enterb[step, :, cols].astype(jnp.bfloat16),
                preferred_element_type=jnp.float32,
            )
            * expb[:, cols]
        )
        for pair in range(group_heads // 2):
            mats = []
            base = g * group_heads + 2 * pair
            for h in (base, base + 1):
                gap = jnp.where(
                    is_lower,
                    cumf[:, h : h + 1] - cumft[h : h + 1, :],
                    cumb[:, h : h + 1] - cumbt[h : h + 1, :],
                )
                sf, sb = stft[h : h + 1, :], stbt[h : h + 1, :]
                amount = jnp.where(is_diagonal, sf + sb, jnp.where(is_lower, sf, sb))
                mats.append((crossed * jnp.exp(gap) * amount).astype(jnp.bfloat16))
            two = slice(base * head_size, (base + 2) * head_size)
            x = act_ref[:, two]
            zero = jnp.zeros_like(x)
            stacked = jnp.concatenate(
                [jnp.where(lane < head_size, x, zero), jnp.where(lane < head_size, zero, x)], axis=0
            )
            y[:, two] += jnp.dot(
                jnp.concatenate(mats, axis=1), stacked, preferred_element_type=jnp.float32
            )
        gate = gate_ref[:, cols].astype(jnp.float32)
        mixed = y[:, cols] * (gate / (1.0 + jnp.exp(-gate)))
        scale = lax.rsqrt(jnp.mean(mixed * mixed, axis=1, keepdims=True) + NORM_EPS)
        out_ref[:, cols] = (mixed * scale * gain_ref[:, cols]).astype(jnp.bfloat16)
    totf = spread(jnp.exp(jnp.broadcast_to(cumf[size - 1 : size], (8, heads))), inner)[0:1]
    carryf[...] = carryf[...] * totf + freshf_ref[0]


def middle_kernel(
    head_size, key_heads, count, sink_ref, query_ref, rim_ref, packf_ref, packb_ref, out_ref,
    enter_ref, scores, raised, bottoms, flipped, turned, bias, mate_in, pair_out, pair_in, gathered,
    reach, back_out, back_in, mate_send, mate_recv, pair_send, pair_recv, back_send, back_recv,
):
    me = lax.axis_index("sp")
    parity = lax.rem(me, 2)
    place = lax.div(me, 2)
    pairs = count // 2
    mate = me + 1 - 2 * parity
    is_even = parity == 0
    packs = (packf_ref, packb_ref)
    states = STATE_SIZE

    def copy(source, target, sends, receives, device):
        return pltpu.make_async_remote_copy(
            src_ref=source, dst_ref=target, send_sem=sends, recv_sem=receives,
            device_id={"sp": device}, device_id_type=MESH,
        )

    def to_mate(d):
        return copy(
            packs[d].at[1 - parity], mate_in.at[d], mate_send.at[d], mate_recv.at[d], mate
        )

    def to_pair(d, k):
        device = me + 2 * k if d == 0 else me - 2 * k
        return copy(
            pair_out.at[d], pair_in.at[d, k - 1], pair_send.at[d, k - 1], pair_recv.at[d, k - 1],
            device,
        )

    def back_to_mate(d):
        return copy(back_out.at[d], back_in.at[d], back_send.at[d], back_recv.at[d], mate)

    def sends_to(d, k):
        return place + k < pairs if d == 0 else place - k >= 0

    def hears_from(d, k):
        return place - k >= 0 if d == 0 else place + k < pairs

    barrier = pltpu.get_barrier_semaphore()
    pl.semaphore_signal(barrier, inc=1, device_id={"sp": mate}, device_id_type=MESH)
    for k in range(1, pairs):
        other = lax.rem(me + 2 * k, count)
        pl.semaphore_signal(barrier, inc=1, device_id={"sp": other}, device_id_type=MESH)
    pl.semaphore_wait(barrier, pairs)
    for d in range(2):
        to_mate(d).start()

    def even_and_odd(d):
        own, other = packs[d][parity].astype(jnp.float32), mate_in[d].astype(jnp.float32)
        return jnp.where(is_even, own, other), jnp.where(is_even, other, own)

    def join_pair():
        for d in range(2):
            to_mate(d).wait_recv()
            even, odd = even_and_odd(d)
            near, far = (odd, even) if d == 0 else (even, odd)
            decay = near[states : states + 1]
            pair_out[d, :states, :] = (near[:states] + decay * far[:states]).astype(jnp.bfloat16)
            pair_out[d, states:, :] = (near[states:] * far[states:]).astype(jnp.bfloat16)
        for k in range(1, pairs):
            for d in range(2):
                @pl.when(sends_to(d, k))
                def _(d=d, k=k):
                    to_pair(d, k).start()

    def join_all():
        gathered[...] = jnp.zeros_like(gathered)
        reach[...] = jnp.ones_like(reach)
        for k in range(1, pairs):
            for d in range(2):
                @pl.when(hears_from(d, k))
                def _(d=d, k=k):
                    to_pair(d, k).wait_recv()
                    came = pair_in[d, k - 1].astype(jnp.float32)
                    gathered[d] = gathered[d] + reach[d, 0:1] * came[:states]
                    reach[d] = reach[d] * came[states : states + 8]
        for d in range(2):
            even, odd = even_and_odd(d)
            base = even if d == 0 else odd
            plain = gathered[d]
            moved = base[:states] + base[states : states + 1] * plain
            plain_is_mine = is_even if d == 0 else jnp.logical_not(is_even)
            enter_ref[d, parity] = jnp.where(plain_is_mine, plain, moved)
            back_out[d] = jnp.where(plain_is_mine, moved, plain).astype(jnp.bfloat16)
            back_to_mate(d).start()

    rows, block = query_ref.shape[0], WINDOW
    span = block + 2 * WINDOW
    blocks = rows // block
    heads = query_ref.shape[1] // head_size
    ratio = heads // key_heads
    values_at = key_heads * head_size
    flipped[...] = jnp.transpose(rim_ref[:, values_at:])
    key_row = lax.broadcasted_iota(jnp.int32, (span, block), 0)
    query_col = lax.broadcasted_iota(jnp.int32, (span, block), 1)
    in_band = (key_row >= query_col) & (key_row <= query_col + 2 * WINDOW)

    @pl.loop(0, blocks)
    def _(step):
        @pl.when(step == (3 * blocks) // 8)
        def _():
            join_pair()

        @pl.when(step == (7 * blocks) // 8)
        def _():
            join_all()

        start = pl.multiple_of(step * block, block)
        position = me * rows + start - WINDOW + key_row
        bias[...] = jnp.where(
            in_band & (position >= 0) & (position < count * rows), 0.0, NEG_FILL
        )
        tops = []
        for h in range(heads):
            k = h // ratio
            scores[h] = lax.dot_general(
                rim_ref[pl.ds(start, span), k * head_size : (k + 1) * head_size],
                query_ref[pl.ds(start, block), h * head_size : (h + 1) * head_size],
                (((1,), (1,)), ((), ())), preferred_element_type=jnp.float32,
            ) + bias[...]
        for h in range(heads):
            top = jnp.maximum(jnp.max(scores[h], axis=0, keepdims=True), sink_ref[h])
            lifted = jnp.exp(scores[h] - top)
            bottoms[h : h + 1] = jnp.sum(lifted, axis=0, keepdims=True) + jnp.exp(sink_ref[h] - top)
            raised[h] = lifted.astype(jnp.bfloat16)
        for h in range(heads):
            k = h // ratio
            turned[h * head_size : (h + 1) * head_size, :] = jnp.dot(
                flipped[k * head_size : (k + 1) * head_size, pl.ds(start, span)], raised[h],
                preferred_element_type=jnp.float32,
            ) * (1.0 / bottoms[h : h + 1])
        out_ref[pl.ds(start, block), :] = jnp.transpose(turned[...]).astype(jnp.bfloat16)

    for d in range(2):
        back_to_mate(d).wait_recv()
        enter_ref[d, 1 - parity] = back_in[d].astype(jnp.float32)
    for d in range(2):
        to_mate(d).wait_send()
        back_to_mate(d).wait_send()
        for k in range(1, pairs):
            @pl.when(sends_to(d, k))
            def _(d=d, k=k):
                to_pair(d, k).wait_send()


def middle(query, rimmed, sink_logit, pack_forward, pack_backward, head_size, key_heads):
    rows, width = query.shape
    heads = width // head_size
    count = lax.axis_size("sp")
    hops = max(count // 2 - 1, 1)
    _, depth, half = pack_forward.shape
    span = 3 * WINDOW
    vmem = pl.BlockSpec(memory_space=pltpu.VMEM)
    dma = pltpu.SemaphoreType.DMA
    return pl.pallas_call(
        functools.partial(middle_kernel, head_size, key_heads, count),
        in_specs=[pl.BlockSpec(memory_space=pltpu.SMEM), vmem, vmem, vmem, vmem],
        out_specs=[vmem, vmem],
        out_shape=[
            jax.ShapeDtypeStruct((rows, width), jnp.bfloat16),
            jax.ShapeDtypeStruct((2, 2, STATE_SIZE, half), jnp.float32),
        ],
        scratch_shapes=[
            pltpu.VMEM((heads, span, WINDOW), jnp.float32),
            pltpu.VMEM((heads, span, WINDOW), jnp.bfloat16),
            pltpu.VMEM((heads, WINDOW), jnp.float32),
            pltpu.VMEM((key_heads * head_size, rimmed.shape[0]), jnp.bfloat16),
            pltpu.VMEM((width, WINDOW), jnp.float32),
            pltpu.VMEM((span, WINDOW), jnp.float32),
            pltpu.VMEM((2, depth, half), jnp.bfloat16),
            pltpu.VMEM((2, depth, half), jnp.bfloat16),
            pltpu.VMEM((2, hops, depth, half), jnp.bfloat16),
            pltpu.VMEM((2, STATE_SIZE, half), jnp.float32),
            pltpu.VMEM((2, 8, half), jnp.float32),
            pltpu.VMEM((2, STATE_SIZE, half), jnp.bfloat16),
            pltpu.VMEM((2, STATE_SIZE, half), jnp.bfloat16),
            dma((2,)), dma((2,)), dma((2, hops)), dma((2, hops)), dma((2,)), dma((2,)),
        ],
        compiler_params=pltpu.CompilerParams(
            collective_id=5, has_side_effects=True, vmem_limit_bytes=20 * MIB
        ),
        cost_estimate=pl.CostEstimate(
            flops=4 * rows * span * width, bytes_accessed=4 * rows * width,
            transcendentals=rows * span * heads,
        ),
        name="middle",
    )(sink_logit, query, rimmed, pack_forward, pack_backward)


def combine_kernel(
    count, attn_ref, ssm_ref, attn_w_ref, ssm_w_ref, out_ref, acc, own, mate_out, mate_in,
    far_out, far_in, mate_send, mate_recv, far_send, far_recv,
):
    me = lax.axis_index("tp")
    core = lax.rem(me, 2)
    chip = lax.div(me, 2)
    chips = count // 2
    mate = me + 1 - 2 * core
    rows = out_ref.shape[0]
    pieces, width = own.shape[1], own.shape[3]

    def chip_of(slot):
        return lax.rem(chip + 1 + slot, chips)

    def to_mate(slot, j):
        return pltpu.make_async_remote_copy(
            src_ref=mate_out.at[slot, j], dst_ref=mate_in.at[slot, j],
            send_sem=mate_send.at[slot, j], recv_sem=mate_recv.at[slot, j],
            device_id={"tp": mate}, device_id_type=MESH,
        )

    def to_far(slot, j):
        return pltpu.make_async_remote_copy(
            src_ref=far_out.at[slot, j], dst_ref=far_in.at[slot, j],
            send_sem=far_send.at[slot, j], recv_sem=far_recv.at[slot, j],
            device_id={"tp": 2 * chip_of(slot) + core}, device_id_type=MESH,
        )

    barrier = pltpu.get_barrier_semaphore()
    pl.semaphore_signal(barrier, inc=1, device_id={"tp": mate}, device_id_type=MESH)
    for slot in range(chips - 1):
        pl.semaphore_signal(
            barrier, inc=1, device_id={"tp": 2 * chip_of(slot) + core}, device_id_type=MESH
        )
    pl.semaphore_wait(barrier, chips)

    def compute(slot, j):
        cols = pl.ds(pl.multiple_of(j * width, width), width)
        first = pl.multiple_of(chip_of(slot) * 2 * rows, rows)
        span = pl.ds(first, 2 * rows)
        acc[...] = jnp.dot(
            attn_ref[span, :], attn_w_ref[:, cols], preferred_element_type=jnp.float32
        ) + jnp.dot(ssm_ref[span, :], ssm_w_ref[:, cols], preferred_element_type=jnp.float32)
        other = acc[pl.ds(pl.multiple_of((1 - core) * rows, rows), rows), :]
        mate_out[slot, j] = other.astype(jnp.bfloat16)
        to_mate(slot, j).start()
        mine = acc[pl.ds(pl.multiple_of(core * rows, rows), rows), :]
        own[slot, j] = mine.astype(jnp.bfloat16)

    def forward(slot, j):
        to_mate(slot, j).wait_recv()
        far_out[slot, j] = (
            own[slot, j].astype(jnp.float32) + mate_in[slot, j].astype(jnp.float32)
        ).astype(jnp.bfloat16)
        to_far(slot, j).start()

    last = chips - 1
    for slot in range(chips):
        compute(slot, 0)
        if slot > 0:
            forward(slot - 1, pieces - 1)

        @pl.loop(1, pieces)
        def _(j, slot=slot):
            compute(slot, j)
            if slot < last:
                forward(slot, j - 1)

    @pl.loop(0, pieces)
    def _(j):
        to_mate(last, j).wait_recv()
        total = own[last, j].astype(jnp.float32) + mate_in[last, j].astype(jnp.float32)
        for slot in range(last):
            to_far(slot, j).wait_recv()
            total = total + far_in[slot, j].astype(jnp.float32)
        out_ref[:, pl.ds(pl.multiple_of(j * width, width), width)] = total.astype(jnp.bfloat16)

    @pl.loop(0, pieces)
    def _(j):
        for slot in range(chips):
            to_mate(slot, j).wait_send()
        for slot in range(last):
            to_far(slot, j).wait_send()


def combine(attn_out, ssm_out, attn_weight, ssm_weight):
    count = lax.axis_size("tp")
    chips = count // 2
    total, width = attn_out.shape[0], attn_weight.shape[1]
    rows = total // count
    pieces = width // PIECE
    far = max(chips - 1, 1)
    vmem = pl.BlockSpec(memory_space=pltpu.VMEM)
    depth = attn_out.shape[1] + ssm_out.shape[1]
    return pl.pallas_call(
        functools.partial(combine_kernel, count),
        in_specs=[vmem] * 4,
        out_specs=vmem,
        out_shape=jax.ShapeDtypeStruct((rows, width), jnp.bfloat16),
        scratch_shapes=[
            pltpu.VMEM((2 * rows, PIECE), jnp.float32),
            pltpu.VMEM((chips, pieces, rows, PIECE), jnp.bfloat16),
            pltpu.VMEM((chips, pieces, rows, PIECE), jnp.bfloat16),
            pltpu.VMEM((chips, pieces, rows, PIECE), jnp.bfloat16),
            pltpu.VMEM((far, pieces, rows, PIECE), jnp.bfloat16),
            pltpu.VMEM((far, pieces, rows, PIECE), jnp.bfloat16),
            pltpu.SemaphoreType.DMA((chips, pieces)),
            pltpu.SemaphoreType.DMA((chips, pieces)),
            pltpu.SemaphoreType.DMA((far, pieces)),
            pltpu.SemaphoreType.DMA((far, pieces)),
        ],
        compiler_params=pltpu.CompilerParams(
            collective_id=3, has_side_effects=True, vmem_limit_bytes=24 * MIB
        ),
        cost_estimate=pl.CostEstimate(
            flops=2 * total * depth * width, bytes_accessed=2 * depth * width, transcendentals=0
        ),
        name="combine",
    )(attn_out, ssm_out, attn_weight, ssm_weight)


def convolve(rows, keyed, taps, table, tap_count, inner, maps, heads):
    total, width = rows.shape
    chunks = total // CHUNK
    count = lax.axis_size("sp")
    vmem = pl.BlockSpec(memory_space=pltpu.VMEM)
    fresh = jax.ShapeDtypeStruct((chunks, STATE_SIZE, inner), jnp.float32)
    pack = jax.ShapeDtypeStruct((2, STATE_SIZE + PACK_ROWS, inner // 2), jnp.bfloat16)
    return pl.pallas_call(
        functools.partial(convolve_kernel, tap_count, inner, maps, heads, count),
        in_specs=[vmem] * 4,
        out_specs=[vmem] * 6,
        out_shape=[
            jax.ShapeDtypeStruct((total, width), jnp.bfloat16), fresh, fresh, pack, pack,
            jax.ShapeDtypeStruct((total + 2 * WINDOW, keyed.shape[1]), jnp.bfloat16),
        ],
        scratch_shapes=[
            pltpu.VMEM((CHUNK + 2 * HALO, width), jnp.float32),
            pltpu.VMEM((HALO, width), jnp.bfloat16),
            pltpu.VMEM((HALO, width), jnp.bfloat16),
            pltpu.VMEM((WINDOW, keyed.shape[1]), jnp.bfloat16),
            pltpu.VMEM((WINDOW, keyed.shape[1]), jnp.bfloat16),
            pltpu.VMEM((STATE_SIZE, inner), jnp.float32),
            pltpu.VMEM((STATE_SIZE, inner), jnp.float32),
            pltpu.SemaphoreType.DMA((4,)),
            pltpu.SemaphoreType.DMA((4,)),
        ],
        compiler_params=pltpu.CompilerParams(
            collective_id=4, has_side_effects=True, vmem_limit_bytes=24 * MIB
        ),
        cost_estimate=pl.CostEstimate(
            flops=8 * total * inner * STATE_SIZE, bytes_accessed=8 * total * inner,
            transcendentals=total * width,
        ),
        name="convolve",
    )(rows, keyed, taps, table)


def chunk_outputs(head_size, inner, maps, heads, act, table, turned, fresh, incoming, gate, gain):
    rows, total = act.shape
    chunks = rows // CHUNK
    return pl.pallas_call(
        functools.partial(outputs_kernel, head_size, inner, maps),
        grid=(chunks,),
        in_specs=[
            pl.BlockSpec((CHUNK, total), lambda i: (i, 0)),
            pl.BlockSpec((CHUNK, 128), lambda i: (i, 0)),
            pl.BlockSpec((128, CHUNK), lambda i: (0, i)),
            pl.BlockSpec((rows, 128), lambda i: (0, 0)),
            pl.BlockSpec((1, STATE_SIZE, inner), lambda i: (i, 0, 0)),
            pl.BlockSpec((chunks, STATE_SIZE, inner), lambda i: (0, 0, 0)),
            pl.BlockSpec(incoming.shape, lambda i: (0, 0, 0, 0)),
            pl.BlockSpec((CHUNK, inner), lambda i: (i, 0)),
            pl.BlockSpec((1, inner), lambda i: (0, 0)),
        ],
        out_specs=pl.BlockSpec((CHUNK, inner), lambda i: (i, 0)),
        out_shape=jax.ShapeDtypeStruct((rows, inner), jnp.bfloat16),
        scratch_shapes=[
            pltpu.VMEM((STATE_SIZE, inner), jnp.float32),
            pltpu.VMEM((chunks, STATE_SIZE, inner), jnp.float32),
            pltpu.VMEM((CHUNK, inner), jnp.float32),
        ],
        cost_estimate=pl.CostEstimate(
            flops=8 * rows * inner * STATE_SIZE, bytes_accessed=16 * rows * inner,
            transcendentals=rows * CHUNK * heads,
        ),
        name="chunk_outputs",
    )(act, table, turned, table, fresh[0], fresh[1], incoming, gate, gain)


def local(
    tokens,
    norm_gain,
    query_weight,
    key_weight,
    value_weight,
    query_gain,
    key_gain,
    sink_logit,
    gate_weight,
    inner_weight,
    input_map,
    output_map,
    step_weight,
    conv_inner,
    conv_pair,
    decay_rate,
    decay_jump,
    inner_gain,
    attn_out_weight,
    ssm_out_weight,
):
    head_size = query_gain.shape[0]
    query, keyed, rows, gate_rows, table, turned = project_all(
        tokens, norm_gain, inner_weight, input_map, output_map, key_weight, value_weight,
        query_weight, gate_weight, step_weight, query_gain, key_gain, decay_rate, decay_jump,
    )
    tap_count, inner = conv_inner.shape
    maps = input_map.shape[1]
    heads = inner // head_size
    key_heads = key_weight.shape[1] // head_size
    conv_table = jnp.concatenate([conv_inner, conv_pair.reshape(tap_count, -1)], axis=1).astype(
        jnp.float32
    )
    act, fresh_forward, fresh_backward, pack_forward, pack_backward, rimmed = convolve(
        rows, keyed, conv_table, table, tap_count, inner, maps, heads
    )
    attn_out, incoming = middle(
        query, rimmed, sink_logit, pack_forward, pack_backward, head_size, key_heads
    )
    ssm_out = chunk_outputs(
        head_size, inner, maps, heads, act, table, turned, (fresh_forward, fresh_backward), incoming,
        gate_rows, inner_gain.astype(jnp.float32)[None, :],
    )
    return combine(attn_out, ssm_out, attn_out_weight, ssm_out_weight)


def solution(mesh):
    in_specs = (
        P("sp", None),
        P(),
        P(None, "tp"),
        P(None, "tp"),
        P(None, "tp"),
        P(),
        P(),
        P("tp"),
        P(None, "tp"),
        P(None, "tp"),
        P(None, "tp"),
        P(None, "tp"),
        P(None, None, "tp"),
        P(None, "tp"),
        P(None, None, "tp"),
        P(None, "tp"),
        P("sp", None, "tp"),
        P("tp"),
        P("tp", None),
        P("tp", None),
    )
    out_specs = P(("sp", "tp"), None)
    return jax.shard_map(local, mesh=mesh, in_specs=in_specs, out_specs=out_specs, check_vma=False)
```

```python
import functools

import jax
import jax.numpy as jnp
import numpy as np
from jax import lax
from jax.experimental import pallas as pl
from jax.experimental.pallas import tpu as pltpu
from jax.sharding import PartitionSpec as P

STATE_SIZE = 128
WINDOW = 128
CHUNK = 128
HALO = 16

NORM_EPS = 1e-05
ROPE_BASE = 500000.0
NEG_FILL = -1e30
TILE = 512
MIB = 1 << 20
PROJECT_MIB = 52
CONVOLVE_MIB = 32
MIDDLE_MIB = 30
FINISH_MIB = 28
PACK_ROWS = 16
MESH = pl.DeviceIdType.MESH


def spread(factor, width):
    heads = factor.shape[1]
    row = lax.broadcasted_iota(jnp.int32, (heads, width), 0)
    column = lax.broadcasted_iota(jnp.int32, (heads, width), 1)
    head_size = width // heads
    ones = jnp.where(
        (column >= row * head_size) & (column < (row + 1) * head_size), 1.0, 0.0
    ).astype(jnp.bfloat16)
    return jnp.dot(factor.astype(jnp.bfloat16), ones, preferred_element_type=jnp.float32)


def exact_dot(a, b):
    return jnp.dot(a, b, precision=lax.Precision.HIGHEST, preferred_element_type=jnp.float32)


def triangle(size, lower):
    row = lax.broadcasted_iota(jnp.int32, (size, size), 0)
    column = lax.broadcasted_iota(jnp.int32, (size, size), 1)
    return jnp.where(row >= column if lower else row <= column, 1.0, 0.0)


def project_kernel(
    head_size, heads, key_width, tokens_ref, inner_hbm, in_hbm, out_hbm, key_hbm, value_hbm,
    query_hbm, gate_hbm, step_hbm, jump_hbm, small_ref, query_ref, keyed_ref, rows_ref, gate_ref,
    table_ref, turned_ref, step_ref, jump_ref, tokens, normed, inner_w, in_w, out_w, keyed_w, query_w, gate_w, raw,
    cosine, sine, token_sems, weight_sems,
):
    total, depth = tokens.shape
    parts = token_sems.shape[0]
    size = total // parts
    moves = [
        pltpu.make_async_copy(
            tokens_ref.at[pl.ds(i * size, size)], tokens.at[pl.ds(i * size, size)],
            token_sems.at[i],
        )
        for i in range(parts)
    ]
    joined = key_width % 128 == 0
    if joined:
        key_w, value_w = keyed_w.at[:, :key_width], keyed_w.at[:, key_width:]
    else:
        key_w, value_w = keyed_w.at[0], keyed_w.at[1]
    weights = (
        (key_hbm, key_w), (value_hbm, value_w), (query_hbm, query_w), (in_hbm, in_w),
        (out_hbm, out_w), (inner_hbm, inner_w), (gate_hbm, gate_w), (step_hbm, step_ref),
        (jump_hbm, jump_ref),
    )
    loads = [
        pltpu.make_async_copy(source, target, weight_sems.at[i])
        for i, (source, target) in enumerate(weights)
    ]
    for move in moves + loads[7:] + loads[:7]:
        move.start()
    lanes = depth // 128
    frequency, sign = small_ref[lanes + 2 : lanes + 3], small_ref[lanes + 3 : lanes + 4]
    order = lax.broadcasted_iota(jnp.int32, (32, 128), 0)
    first = lax.axis_index("sp") * total
    near = order.astype(jnp.float32) * frequency
    cos_near, sin_near = jnp.cos(near), jnp.sin(near)
    for a in range(0, total, 1024):
        far = (first + a + 32 * order).astype(jnp.float32) * frequency
        cos_far, sin_far = jnp.cos(far), jnp.sin(far)
        for r in range(min(32, (total - a) // 32)):
            c, d = cos_far[r : r + 1], sin_far[r : r + 1]
            span = slice(a + r * 32, a + (r + 1) * 32)
            cosine[span, :] = c * cos_near - d * sin_near
            sine[span, :] = (d * cos_near + c * sin_near) * sign
    for i in range(parts):
        moves[i].wait()

        @pl.loop(0, size // 32)
        def _(r, i=i):
            span = pl.ds(pl.multiple_of(i * size + r * 32, 32), 32)
            squares = jnp.zeros((32, 128), jnp.float32)
            for j in range(lanes):
                x = tokens[span, j * 128 : (j + 1) * 128].astype(jnp.float32)
                squares = squares + x * x
            mean = jnp.sum(squares, axis=-1, keepdims=True) * (1.0 / depth)
            scale = lax.rsqrt(mean + NORM_EPS)
            for j in range(lanes):
                cols = slice(j * 128, (j + 1) * 128)
                x = tokens[span, cols].astype(jnp.float32)
                normed[span, cols] = (x * scale * small_ref[j : j + 1]).astype(jnp.bfloat16)

    def run(weight, target, column, beside=None):
        width = min(weight.shape[1], TILE)
        count = weight.shape[1] // width

        def tile(j):
            at = j * width if count == 1 else pl.multiple_of(j * width, width)
            target[:, pl.ds(column + at, width)] = jnp.dot(
                normed[...], weight[:, pl.ds(at, width)], preferred_element_type=jnp.float32
            ).astype(jnp.bfloat16)
            if beside is not None:
                beside(j, total // count)

        if count == 1:
            tile(0)
        else:
            pl.loop(0, count)(tile)

    loads[7].wait()
    loads[8].wait()
    raw[:, 2 * heads :] = jnp.zeros((total, 128 - 2 * heads), jnp.float32)
    raw[:, : 2 * heads] = lax.dot_general(
        normed[...], step_ref[...], (((1,), (1,)), ((), ())), preferred_element_type=jnp.float32
    ).astype(jnp.bfloat16).astype(jnp.float32)
    rates = jnp.transpose(jnp.broadcast_to(small_ref[lanes + 4 : lanes + 5], (128, 128)))
    rates = rates[: 2 * heads, 0:1]
    upper, lower = triangle(CHUNK, False), triangle(CHUNK, True)

    def steps(j, length):
        for c in range(length // CHUNK):
            at = pl.multiple_of(j * length + c * CHUNK, CHUNK)
            span = pl.ds(at, CHUNK)
            x = jnp.transpose(raw[span, :])[: 2 * heads]
            step = jnp.maximum(x, 0.0) + jnp.log1p(jnp.exp(-jnp.abs(x)))
            decay = jump_ref[:, span] - rates * step
            filled = jnp.concatenate(
                [
                    exact_dot(decay[:heads], upper), exact_dot(decay[heads:], lower), step,
                    jnp.zeros((128 - 4 * heads, CHUNK), jnp.float32),
                ],
                axis=0,
            )
            turned_ref[:, span] = filled
            table_ref[span, :] = jnp.transpose(filled)

    row = lax.broadcasted_iota(jnp.int32, (256, 128), 0)
    column = lax.broadcasted_iota(jnp.int32, (256, 128), 1)
    same_head = jnp.where(
        lax.rem(row, 128) // head_size == column // head_size, 1.0, 0.0
    ).astype(jnp.bfloat16)
    lane = lax.broadcasted_iota(jnp.int32, (128, 128), 1)
    half = head_size // 2
    first_half = lax.rem(lane, head_size) < half

    def rotate(value, gain_row, cos_here, sin_here):
        square = value * value
        high = square.astype(jnp.bfloat16)
        low = (square - high.astype(jnp.float32)).astype(jnp.bfloat16)
        sums = jnp.dot(
            jnp.concatenate([high, low], axis=1), same_head, preferred_element_type=jnp.float32
        )
        value = value * lax.rsqrt(sums * (1.0 / head_size) + NORM_EPS) * gain_row
        swapped = jnp.where(
            first_half, pltpu.roll(value, 128 - half, 1), pltpu.roll(value, half, 1)
        )
        return (value * cos_here + swapped * sin_here).astype(jnp.bfloat16)

    def heads_of(j, length):
        for i in range(length // 128):
            span = pl.ds(pl.multiple_of(j * length + i * 128, 128), 128)
            cos_here, sin_here = cosine[span, :], sine[span, :]
            for at in range(0, query_ref.shape[1], 128):
                value = query_ref[span, at : at + 128].astype(jnp.float32)
                query_ref[span, at : at + 128] = rotate(
                    value, small_ref[lanes : lanes + 1], cos_here, sin_here
                )
            for at in range(0, key_width, 128):
                packed = keyed_ref[span, at : at + 128]
                keys = rotate(
                    packed.astype(jnp.float32), small_ref[lanes + 1 : lanes + 2], cos_here, sin_here
                )
                keyed_ref[span, at : at + 128] = jnp.where(lane + at < key_width, keys, packed)

    inner, maps = inner_w.shape[1], in_w.shape[1]
    loads[0].wait()
    loads[1].wait()
    if joined:
        run(keyed_w, keyed_ref, 0)
    else:
        run(keyed_w.at[0], keyed_ref, 0)
        run(keyed_w.at[1], keyed_ref, key_width)
    loads[2].wait()
    run(query_w, query_ref, 0)
    loads[3].wait()
    run(in_w, rows_ref, inner)
    loads[4].wait()
    run(out_w, rows_ref, inner + maps)
    loads[5].wait()
    run(inner_w, rows_ref, 0, steps)
    loads[6].wait()
    run(gate_w, gate_ref, 0, heads_of)


def project_all(
    tokens, norm_gain, inner_weight, input_map, output_map, key_weight, value_weight, query_weight,
    gate_weight, step_weight, query_gain, key_gain, decay_rate, decay_jump,
):
    total, depth = tokens.shape
    head_size = query_gain.shape[0]
    half = head_size // 2
    lane = np.arange(128)
    frequency = (ROPE_BASE ** (-2.0 * (lane % half) / head_size)).astype(np.float32)
    sign = np.where(lane % head_size < half, -1.0, 1.0).astype(np.float32)
    repeats = 128 // head_size
    rates = decay_rate.reshape(-1)
    small = jnp.concatenate(
        [
            norm_gain.astype(jnp.float32), jnp.tile(query_gain, repeats) * head_size ** (-0.5),
            jnp.tile(key_gain, repeats), frequency, sign, rates,
            jnp.zeros((4 * 128 - rates.shape[0],), jnp.float32),
        ]
    ).reshape(-1, 128)
    turned_step = jnp.transpose(step_weight, (1, 2, 0)).reshape(-1, depth)
    turned_jump = jnp.transpose(decay_jump, (1, 2, 0)).reshape(-1, total)
    heads = step_weight.shape[2]
    inner, maps = inner_weight.shape[1], input_map.shape[1]
    width, key_width = query_weight.shape[1], key_weight.shape[1]
    whole = pl.BlockSpec(memory_space=pltpu.HBM)
    vmem = pl.BlockSpec(memory_space=pltpu.VMEM)
    big = (inner_weight, input_map, output_map, key_weight, value_weight, query_weight, gate_weight)
    columns = sum(w.shape[1] for w in big)
    keyed_shape = (depth, 2 * key_width) if key_width % 128 == 0 else (2, depth, key_width)

    def shape(*dims, kind=jnp.bfloat16):
        return jax.ShapeDtypeStruct(dims, kind)

    def room(*dims, kind=jnp.bfloat16):
        return pltpu.VMEM(dims, kind)

    return pl.pallas_call(
        functools.partial(project_kernel, head_size, heads, key_width),
        in_specs=[whole] * 10 + [vmem],
        out_specs=[vmem] * 6,
        out_shape=[
            shape(total, width), shape(total, 2 * key_width), shape(total, inner + 2 * maps),
            shape(total, inner), shape(total, 128, kind=jnp.float32),
            shape(128, total, kind=jnp.float32),
        ],
        scratch_shapes=[
            room(*turned_step.shape), room(*turned_jump.shape, kind=jnp.float32),
            room(total, depth), room(total, depth), room(*inner_weight.shape),
            room(*input_map.shape), room(*output_map.shape), room(*keyed_shape),
            room(*query_weight.shape), room(*gate_weight.shape),
            room(total, 128, kind=jnp.float32), room(total, 128, kind=jnp.float32),
            room(total, 128, kind=jnp.float32),
            pltpu.SemaphoreType.DMA((8,)), pltpu.SemaphoreType.DMA((9,)),
        ],
        compiler_params=pltpu.CompilerParams(vmem_limit_bytes=PROJECT_MIB * MIB),
        cost_estimate=pl.CostEstimate(
            flops=2 * total * depth * columns, bytes_accessed=2 * depth * (columns + total),
            transcendentals=total * 128,
        ),
        name="project",
    )(tokens, *big, turned_step, turned_jump, small)


def convolve_kernel(
    tap_count, inner, maps, heads, count, rows_ref, keyed_ref, taps_ref, table_ref, act_ref,
    local_ref, reach_ref, packf_ref, packb_ref, rim_ref, freshf_ref, freshb_ref, spare, low_rows, high_rows, low_keys,
    high_keys, endf, endb, sends, receives,
):
    me = lax.axis_index("sp")
    total = rows_ref.shape[0]
    size = CHUNK
    chunks = total // size

    def copies(up):
        device = me + 1 if up else me - 1
        slot = 0 if up else 2
        edge = pl.ds(total - HALO if up else 0, HALO)
        wide = pl.ds(total - WINDOW if up else 0, WINDOW)
        pairs = (
            (rows_ref.at[edge], low_rows if up else high_rows),
            (keyed_ref.at[wide], low_keys if up else high_keys),
        )
        return [
            pltpu.make_async_remote_copy(
                src_ref=source, dst_ref=target, send_sem=sends.at[slot + i],
                recv_sem=receives.at[slot + i], device_id={"sp": device}, device_id_type=MESH,
            )
            for i, (source, target) in enumerate(pairs)
        ]

    barrier = pltpu.get_barrier_semaphore()
    for step in (1, count - 1):
        pl.semaphore_signal(
            barrier, inc=1, device_id={"sp": lax.rem(me + step, count)}, device_id_type=MESH
        )
    pl.semaphore_wait(barrier, 2)
    has_low, has_high = me > 0, me < count - 1

    @pl.when(has_high)
    def _():
        for copy in copies(True):
            copy.start()

    @pl.when(has_low)
    def _():
        for copy in copies(False):
            copy.start()

    @pl.when(jnp.logical_not(has_low))
    def _():
        low_rows[...] = jnp.zeros_like(low_rows)
        low_keys[...] = jnp.zeros_like(low_keys)

    @pl.when(jnp.logical_not(has_high))
    def _():
        high_rows[...] = jnp.zeros_like(high_rows)
        high_keys[...] = jnp.zeros_like(high_keys)

    rim_ref[WINDOW : WINDOW + total, :] = keyed_ref[...]

    @pl.loop(0, chunks)
    def _(turn):
        c = lax.rem(turn + 1, chunks)
        start = pl.multiple_of(c * size, size)
        spare[HALO : HALO + size, :] = rows_ref[pl.ds(start, size), :].astype(jnp.float32)

        @pl.when(turn == chunks - 2)
        def _():
            @pl.when(has_low)
            def _():
                for copy in copies(True):
                    copy.wait_recv()

            @pl.when(has_high)
            def _():
                for copy in copies(False):
                    copy.wait_recv()

        @pl.when(c == 0)
        def _():
            spare[:HALO, :] = low_rows[...].astype(jnp.float32)

        @pl.when(c > 0)
        def _():
            at = pl.multiple_of(start - HALO, HALO)
            spare[:HALO, :] = rows_ref[pl.ds(at, HALO), :].astype(jnp.float32)

        @pl.when(c == chunks - 1)
        def _():
            spare[HALO + size :, :] = high_rows[...].astype(jnp.float32)

        @pl.when(c < chunks - 1)
        def _():
            at = pl.multiple_of(start + size, HALO)
            spare[HALO + size :, :] = rows_ref[pl.ds(at, HALO), :].astype(jnp.float32)

        first = HALO - tap_count // 2
        for at in range(0, inner + 2 * maps, 128):
            cols = slice(at, at + 128)
            filtered = spare[first : first + size, cols] * taps_ref[0:1, cols]
            for k in range(1, tap_count):
                filtered = (
                    filtered + spare[first + k : first + k + size, cols] * taps_ref[k : k + 1, cols]
                )
            act_ref[pl.ds(start, size), cols] = (
                filtered * (1.0 / (1.0 + jnp.exp(-filtered)))
            ).astype(jnp.bfloat16)

    rim_ref[:WINDOW, :] = low_keys[...]
    rim_ref[WINDOW + total :, :] = high_keys[...]
    groups = maps // STATE_SIZE
    width = inner // groups

    @pl.loop(0, chunks)
    def _(c):
        span = pl.ds(pl.multiple_of(c * size, size), size)
        table = table_ref[span, :]
        cumf, cumb = table[:, :heads], table[:, heads : 2 * heads]
        wf = jnp.exp(cumf[size - 1 : size] - cumf) * table[:, 2 * heads : 3 * heads]
        wb = jnp.exp(cumb[0:1] - cumb) * table[:, 3 * heads : 4 * heads]
        signal = act_ref[span, :inner].astype(jnp.float32)
        xf = (signal * spread(wf, inner)).astype(jnp.bfloat16)
        xb = (signal * spread(wb, inner)).astype(jnp.bfloat16)
        for g in range(groups):
            cols = slice(g * width, (g + 1) * width)
            entry = act_ref[span, inner + g * STATE_SIZE : inner + (g + 1) * STATE_SIZE]
            turned = jnp.transpose(entry)
            freshf_ref[c, :, cols] = jnp.dot(turned, xf[:, cols], preferred_element_type=jnp.float32)
            freshb_ref[c, :, cols] = jnp.dot(turned, xb[:, cols], preferred_element_type=jnp.float32)

    endf[...] = jnp.zeros_like(endf)
    endb[...] = jnp.zeros_like(endb)

    def total_decay(c, forward):
        row = c * size + size - 1 if forward else c * size
        at = 0 if forward else heads
        return table_ref[pl.ds(row, 1), :][:, at : at + heads]

    def wide(log_row):
        return spread(jnp.exp(jnp.broadcast_to(log_row, (8, heads))), inner)

    logsf, logsb = jnp.zeros((1, heads), jnp.float32), jnp.zeros((1, heads), jnp.float32)
    for c in range(chunks):
        local_ref[0, c] = endf[...].astype(jnp.bfloat16)
        reach_ref[0, c] = wide(logsf)
        logsf = logsf + total_decay(c, True)
        endf[...] = endf[...] * wide(total_decay(c, True))[0:1] + freshf_ref[c]
        r = chunks - 1 - c
        local_ref[1, r] = endb[...].astype(jnp.bfloat16)
        reach_ref[1, r] = wide(logsb)
        logsb = logsb + total_decay(r, False)
        endb[...] = endb[...] * wide(total_decay(r, False))[0:1] + freshb_ref[r]
    half = inner // 2
    for logs, end, pack_ref in ((logsf, endf, packf_ref), (logsb, endb, packb_ref)):
        decay = wide(logs).astype(jnp.bfloat16)
        for side in range(2):
            cols = slice(side * half, (side + 1) * half)
            pack_ref[side, :STATE_SIZE, :] = end[:, cols].astype(jnp.bfloat16)
            pack_ref[side, STATE_SIZE:, :] = jnp.concatenate([decay, decay], axis=0)[:, cols]

    @pl.when(has_high)
    def _():
        for copy in copies(True):
            copy.wait_send()

    @pl.when(has_low)
    def _():
        for copy in copies(False):
            copy.wait_send()


def middle_kernel(
    head_size, key_heads, count, inner, maps, sink_ref, query_ref, rim_ref, packf_ref, packb_ref,
    act_ref, table_ref, turned_ref, out_ref, enter_ref, inside_ref, scores, raised, bottoms, flipped, turned, bias, mate_in, pair_out, pair_in, gathered,
    reach, back_out, back_in, mate_send, mate_recv, pair_send, pair_recv, back_send, back_recv,
):
    me = lax.axis_index("sp")
    parity = lax.rem(me, 2)
    place = lax.div(me, 2)
    pairs = count // 2
    mate = me + 1 - 2 * parity
    is_even = parity == 0
    packs = (packf_ref, packb_ref)
    states = STATE_SIZE

    def copy(source, target, sends, receives, device):
        return pltpu.make_async_remote_copy(
            src_ref=source, dst_ref=target, send_sem=sends, recv_sem=receives,
            device_id={"sp": device}, device_id_type=MESH,
        )

    def to_mate(d):
        return copy(
            packs[d].at[1 - parity], mate_in.at[d], mate_send.at[d], mate_recv.at[d], mate
        )

    def to_pair(d, k):
        device = me + 2 * k if d == 0 else me - 2 * k
        return copy(
            pair_out.at[d], pair_in.at[d, k - 1], pair_send.at[d, k - 1], pair_recv.at[d, k - 1],
            device,
        )

    def back_to_mate(d):
        return copy(back_out.at[d], back_in.at[d], back_send.at[d], back_recv.at[d], mate)

    def sends_to(d, k):
        return place + k < pairs if d == 0 else place - k >= 0

    def hears_from(d, k):
        return place - k >= 0 if d == 0 else place + k < pairs

    barrier = pltpu.get_barrier_semaphore()
    pl.semaphore_signal(barrier, inc=1, device_id={"sp": mate}, device_id_type=MESH)
    for k in range(1, pairs):
        other = lax.rem(me + 2 * k, count)
        pl.semaphore_signal(barrier, inc=1, device_id={"sp": other}, device_id_type=MESH)
    pl.semaphore_wait(barrier, pairs)
    for d in range(2):
        to_mate(d).start()

    def even_and_odd(d):
        own, other = packs[d][parity].astype(jnp.float32), mate_in[d].astype(jnp.float32)
        return jnp.where(is_even, own, other), jnp.where(is_even, other, own)

    def join_pair():
        for d in range(2):
            to_mate(d).wait_recv()
            even, odd = even_and_odd(d)
            near, far = (odd, even) if d == 0 else (even, odd)
            decay = near[states : states + 1]
            pair_out[d, :states, :] = (near[:states] + decay * far[:states]).astype(jnp.bfloat16)
            pair_out[d, states:, :] = (near[states:] * far[states:]).astype(jnp.bfloat16)
        for k in range(1, pairs):
            for d in range(2):
                @pl.when(sends_to(d, k))
                def _(d=d, k=k):
                    to_pair(d, k).start()

    def join_all():
        gathered[...] = jnp.zeros_like(gathered)
        reach[...] = jnp.ones_like(reach)
        for k in range(1, pairs):
            for d in range(2):
                @pl.when(hears_from(d, k))
                def _(d=d, k=k):
                    to_pair(d, k).wait_recv()
                    came = pair_in[d, k - 1].astype(jnp.float32)
                    gathered[d] = gathered[d] + reach[d, 0:1] * came[:states]
                    reach[d] = reach[d] * came[states : states + 8]
        for d in range(2):
            even, odd = even_and_odd(d)
            base = even if d == 0 else odd
            plain = gathered[d]
            moved = base[:states] + base[states : states + 1] * plain
            plain_is_mine = is_even if d == 0 else jnp.logical_not(is_even)
            enter_ref[d, parity] = jnp.where(plain_is_mine, plain, moved)
            back_out[d] = jnp.where(plain_is_mine, moved, plain).astype(jnp.bfloat16)
            back_to_mate(d).start()

    rows, block = query_ref.shape[0], WINDOW
    span = block + 2 * WINDOW
    blocks = rows // block
    heads = query_ref.shape[1] // head_size
    ratio = heads // key_heads
    values_at = key_heads * head_size
    flipped[...] = jnp.transpose(rim_ref[:, values_at:])
    key_row = lax.broadcasted_iota(jnp.int32, (span, block), 0)
    query_col = lax.broadcasted_iota(jnp.int32, (span, block), 1)
    in_band = (key_row >= query_col) & (key_row <= query_col + 2 * WINDOW)

    groups = maps // STATE_SIZE
    ssm_heads = inner // head_size
    chunk_row = lax.broadcasted_iota(jnp.int32, (CHUNK, CHUNK), 0)
    chunk_col = lax.broadcasted_iota(jnp.int32, (CHUNK, CHUNK), 1)
    is_lower, is_diagonal = chunk_row >= chunk_col, chunk_row == chunk_col
    lane = lax.broadcasted_iota(jnp.int32, (CHUNK, 2 * head_size), 1)

    def inside_chunk(c):
        at = pl.multiple_of(c * CHUNK, CHUNK)
        span = pl.ds(at, CHUNK)
        table = table_ref[span, :]
        for g in range(groups):
            entry = act_ref[span, inner + g * STATE_SIZE : inner + (g + 1) * STATE_SIZE]
            leave = act_ref[
                span, inner + maps + g * STATE_SIZE : inner + maps + (g + 1) * STATE_SIZE
            ]
            crossed = lax.dot_general(
                leave, entry, (((1,), (1,)), ((), ())), preferred_element_type=jnp.float32
            )
            each = ssm_heads // groups
            for pair in range(each // 2):
                mats = []
                base = g * each + 2 * pair
                for h in (base, base + 1):
                    low, high = h, ssm_heads + h
                    gap = jnp.where(
                        is_lower,
                        table[:, low : low + 1] - turned_ref[low : low + 1, span],
                        table[:, high : high + 1] - turned_ref[high : high + 1, span],
                    )
                    sf = turned_ref[2 * ssm_heads + h : 2 * ssm_heads + h + 1, span]
                    sb = turned_ref[3 * ssm_heads + h : 3 * ssm_heads + h + 1, span]
                    amount = jnp.where(is_diagonal, sf + sb, jnp.where(is_lower, sf, sb))
                    mats.append((crossed * jnp.exp(gap) * amount).astype(jnp.bfloat16))
                two = slice(base * head_size, (base + 2) * head_size)
                x = act_ref[span, two]
                zero = jnp.zeros_like(x)
                stacked = jnp.concatenate(
                    [jnp.where(lane < head_size, x, zero), jnp.where(lane < head_size, zero, x)],
                    axis=0,
                )
                inside_ref[span, two] = jnp.dot(
                    jnp.concatenate(mats, axis=1), stacked, preferred_element_type=jnp.float32
                )

    @pl.loop(0, blocks)
    def _(step):
        inside_chunk(step)

        @pl.when(step == (3 * blocks) // 8)
        def _():
            join_pair()

        @pl.when(step == (7 * blocks) // 8)
        def _():
            join_all()

        start = pl.multiple_of(step * block, block)
        position = me * rows + start - WINDOW + key_row
        bias[...] = jnp.where(
            in_band & (position >= 0) & (position < count * rows), 0.0, NEG_FILL
        )
        tops = []
        for h in range(heads):
            k = h // ratio
            scores[h] = lax.dot_general(
                rim_ref[pl.ds(start, span), k * head_size : (k + 1) * head_size],
                query_ref[pl.ds(start, block), h * head_size : (h + 1) * head_size],
                (((1,), (1,)), ((), ())), preferred_element_type=jnp.float32,
            ) + bias[...]
        for h in range(heads):
            top = jnp.maximum(jnp.max(scores[h], axis=0, keepdims=True), sink_ref[h])
            lifted = jnp.exp(scores[h] - top)
            bottoms[h : h + 1] = jnp.sum(lifted, axis=0, keepdims=True) + jnp.exp(sink_ref[h] - top)
            raised[h] = lifted.astype(jnp.bfloat16)
        for h in range(heads):
            k = h // ratio
            turned[h * head_size : (h + 1) * head_size, :] = jnp.dot(
                flipped[k * head_size : (k + 1) * head_size, pl.ds(start, span)], raised[h],
                preferred_element_type=jnp.float32,
            ) * (1.0 / bottoms[h : h + 1])
        out_ref[pl.ds(start, block), :] = jnp.transpose(turned[...]).astype(jnp.bfloat16)

    for d in range(2):
        back_to_mate(d).wait_recv()
        enter_ref[d, 1 - parity] = back_in[d].astype(jnp.float32)
    for d in range(2):
        to_mate(d).wait_send()
        back_to_mate(d).wait_send()
        for k in range(1, pairs):
            @pl.when(sends_to(d, k))
            def _(d=d, k=k):
                to_pair(d, k).wait_send()


def middle(
    query, rimmed, sink_logit, pack_forward, pack_backward, act, table, turned, head_size, key_heads,
    inner, maps,
):
    rows, width = query.shape
    heads = width // head_size
    count = lax.axis_size("sp")
    hops = max(count // 2 - 1, 1)
    _, depth, half = pack_forward.shape
    span = 3 * WINDOW
    vmem = pl.BlockSpec(memory_space=pltpu.VMEM)
    dma = pltpu.SemaphoreType.DMA
    return pl.pallas_call(
        functools.partial(middle_kernel, head_size, key_heads, count, inner, maps),
        in_specs=[pl.BlockSpec(memory_space=pltpu.SMEM)] + [vmem] * 7,
        out_specs=[vmem] * 3,
        out_shape=[
            jax.ShapeDtypeStruct((rows, width), jnp.bfloat16),
            jax.ShapeDtypeStruct((2, 2, STATE_SIZE, half), jnp.float32),
            jax.ShapeDtypeStruct((rows, inner), jnp.float32),
        ],
        scratch_shapes=[
            pltpu.VMEM((heads, span, WINDOW), jnp.float32),
            pltpu.VMEM((heads, span, WINDOW), jnp.bfloat16),
            pltpu.VMEM((heads, WINDOW), jnp.float32),
            pltpu.VMEM((key_heads * head_size, rimmed.shape[0]), jnp.bfloat16),
            pltpu.VMEM((width, WINDOW), jnp.float32),
            pltpu.VMEM((span, WINDOW), jnp.float32),
            pltpu.VMEM((2, depth, half), jnp.bfloat16),
            pltpu.VMEM((2, depth, half), jnp.bfloat16),
            pltpu.VMEM((2, hops, depth, half), jnp.bfloat16),
            pltpu.VMEM((2, STATE_SIZE, half), jnp.float32),
            pltpu.VMEM((2, 8, half), jnp.float32),
            pltpu.VMEM((2, STATE_SIZE, half), jnp.bfloat16),
            pltpu.VMEM((2, STATE_SIZE, half), jnp.bfloat16),
            dma((2,)), dma((2,)), dma((2, hops)), dma((2, hops)), dma((2,)), dma((2,)),
        ],
        compiler_params=pltpu.CompilerParams(
            collective_id=5, has_side_effects=True, vmem_limit_bytes=MIDDLE_MIB * MIB
        ),
        cost_estimate=pl.CostEstimate(
            flops=4 * rows * span * width, bytes_accessed=4 * rows * width,
            transcendentals=rows * span * heads,
        ),
        name="middle",
    )(sink_logit, query, rimmed, pack_forward, pack_backward, act, table, turned)


def convolve(rows, keyed, taps, table, tap_count, inner, maps, heads):
    total, width = rows.shape
    chunks = total // CHUNK
    count = lax.axis_size("sp")
    vmem = pl.BlockSpec(memory_space=pltpu.VMEM)
    local_shape = jax.ShapeDtypeStruct((2, chunks, STATE_SIZE, inner), jnp.bfloat16)
    reach_shape = jax.ShapeDtypeStruct((2, chunks, 8, inner), jnp.float32)
    pack = jax.ShapeDtypeStruct((2, STATE_SIZE + PACK_ROWS, inner // 2), jnp.bfloat16)
    return pl.pallas_call(
        functools.partial(convolve_kernel, tap_count, inner, maps, heads, count),
        in_specs=[vmem] * 4,
        out_specs=[vmem] * 6,
        out_shape=[
            jax.ShapeDtypeStruct((total, width), jnp.bfloat16), local_shape, reach_shape, pack, pack,
            jax.ShapeDtypeStruct((total + 2 * WINDOW, keyed.shape[1]), jnp.bfloat16),
        ],
        scratch_shapes=[
            pltpu.VMEM((chunks, STATE_SIZE, inner), jnp.float32),
            pltpu.VMEM((chunks, STATE_SIZE, inner), jnp.float32),
            pltpu.VMEM((CHUNK + 2 * HALO, width), jnp.float32),
            pltpu.VMEM((HALO, width), jnp.bfloat16),
            pltpu.VMEM((HALO, width), jnp.bfloat16),
            pltpu.VMEM((WINDOW, keyed.shape[1]), jnp.bfloat16),
            pltpu.VMEM((WINDOW, keyed.shape[1]), jnp.bfloat16),
            pltpu.VMEM((STATE_SIZE, inner), jnp.float32),
            pltpu.VMEM((STATE_SIZE, inner), jnp.float32),
            pltpu.SemaphoreType.DMA((4,)),
            pltpu.SemaphoreType.DMA((4,)),
        ],
        compiler_params=pltpu.CompilerParams(
            collective_id=4, has_side_effects=True, vmem_limit_bytes=CONVOLVE_MIB * MIB
        ),
        cost_estimate=pl.CostEstimate(
            flops=8 * total * inner * STATE_SIZE, bytes_accessed=8 * total * inner,
            transcendentals=total * width,
        ),
        name="convolve",
    )(rows, keyed, taps, table)


def finish_kernel(
    head_size, inner, maps, heads, count, act_ref, table_ref, local_ref, reach_ref, enter_ref,
    inside_ref, gate_ref, gain_ref, attn_ref, attn_hbm, ssm_hbm, out_ref, attn_w, ssm_w, ssm,
    carries, own, mate_out, mate_in, far_out, far_in, home, home_out, home_in, load_sems, mate_send,
    mate_recv, far_send, far_recv, home_send, home_recv,
):
    loads = [
        pltpu.make_async_copy(attn_hbm, attn_w, load_sems.at[0]),
        pltpu.make_async_copy(ssm_hbm, ssm_w, load_sems.at[1]),
    ]
    for load in loads:
        load.start()
    me = lax.axis_index("tp")
    core = lax.rem(me, 2)
    chip = lax.div(me, 2)
    chips = count // 2
    mate = me + 1 - 2 * core
    size = CHUNK
    wide = ssm_w.shape[1]
    side = wide // 2
    each = home.shape[0]
    per_chip = 2 * each
    far_steps = (chips - 1) * per_chip
    groups = maps // STATE_SIZE
    width = inner // groups
    half = inner // 2

    def chip_of(slot):
        return lax.rem(chip + 1 + slot, chips)

    def remote(source, target, sends, receives, device):
        return pltpu.make_async_remote_copy(
            src_ref=source, dst_ref=target, send_sem=sends, recv_sem=receives,
            device_id={"tp": device}, device_id_type=MESH,
        )

    def to_mate(t):
        return remote(mate_out.at[t], mate_in.at[t], mate_send.at[t], mate_recv.at[t], mate)

    def to_far(t):
        slot, i = lax.div(t, per_chip), lax.rem(t, per_chip)
        owner, at = lax.div(i, each), lax.rem(i, each)
        return remote(
            far_out.at[t], far_in.at[slot, core, at], far_send.at[t], far_recv.at[slot, core, at],
            2 * chip_of(slot) + owner,
        )

    def from_far(slot, part, at):
        return remote(
            far_out.at[0], far_in.at[slot, part, at], far_send.at[0], far_recv.at[slot, part, at],
            mate,
        )

    def to_home(i):
        return remote(home_out.at[i], home_in.at[i], home_send.at[i], home_recv.at[i], mate)

    barrier = pltpu.get_barrier_semaphore()
    pl.semaphore_signal(barrier, inc=1, device_id={"tp": mate}, device_id_type=MESH)
    for slot in range(chips - 1):
        for other in range(2):
            pl.semaphore_signal(
                barrier, inc=1, device_id={"tp": 2 * chip_of(slot) + other}, device_id_type=MESH
            )
    pl.semaphore_wait(barrier, 1 + 2 * (chips - 1))

    def rows_of(c):
        span = pl.ds(pl.multiple_of(c * size, size), size)
        for d in range(2):
            for part in range(2):
                cols = slice(part * half, (part + 1) * half)
                carries[d, :, cols] = (
                    local_ref[d, c, :, cols].astype(jnp.float32)
                    + reach_ref[d, c, 0:1, cols] * enter_ref[d, part]
                ).astype(jnp.bfloat16)
        table = table_ref[span, :]
        expf = spread(jnp.exp(table[:, :heads]), inner)
        expb = spread(jnp.exp(table[:, heads : 2 * heads]), inner)
        for g in range(groups):
            cols = slice(g * width, (g + 1) * width)
            first = inner + maps + g * STATE_SIZE
            leave = act_ref[span, first : first + STATE_SIZE]
            y = (
                inside_ref[span, cols]
                + jnp.dot(leave, carries[0, :, cols], preferred_element_type=jnp.float32)
                * expf[:, cols]
                + jnp.dot(leave, carries[1, :, cols], preferred_element_type=jnp.float32)
                * expb[:, cols]
            )
            gate = gate_ref[span, cols].astype(jnp.float32)
            mixed = y * (gate * (1.0 / (1.0 + jnp.exp(-gate))))
            scale = lax.rsqrt(jnp.mean(mixed * mixed, axis=1, keepdims=True) + NORM_EPS)
            ssm[:, cols] = (mixed * scale * gain_ref[:, cols]).astype(jnp.bfloat16)
        return span

    def product(span, cols):
        return (
            jnp.dot(attn_ref[span, :], attn_w[:, cols], preferred_element_type=jnp.float32)
            + jnp.dot(ssm[...], ssm_w[:, cols], preferred_element_type=jnp.float32)
        ).astype(jnp.bfloat16)

    def forward(t):
        to_mate(t).wait_recv()
        far_out[t] = (own[t].astype(jnp.float32) + mate_in[t].astype(jnp.float32)).astype(
            jnp.bfloat16
        )
        to_far(t).start()

    for load in loads:
        load.wait()

    @pl.loop(0, far_steps)
    def _(t):
        slot, i = lax.div(t, per_chip), lax.rem(t, per_chip)
        span = rows_of(chip_of(slot) * per_chip + i)
        mate_out[t] = product(span, pl.ds(pl.multiple_of((1 - core) * side, side), side))
        to_mate(t).start()
        own[t] = product(span, pl.ds(pl.multiple_of(core * side, side), side))

        @pl.when(t > 0)
        def _():
            forward(t - 1)

    @pl.loop(0, per_chip)
    def _(u):
        i = lax.rem(u, each)
        owner = jnp.where(u < each, 1 - core, core)
        span = rows_of((2 * chip + owner) * each + i)
        for part in range(2):
            cols = slice(part * side, (part + 1) * side)
            home[i, :, cols] = product(span, cols)

        if far_steps > 0:
            @pl.when(u == 0)
            def _():
                forward(far_steps - 1)

        @pl.when(u < each)
        def _():
            home_out[i] = home[i]
            to_home(i).start()

    for i in range(each):
        to_home(i).wait_recv()
        for part in range(2):
            cols = slice(part * side, (part + 1) * side)
            total = home[i, :, cols].astype(jnp.float32) + home_in[i, :, cols].astype(jnp.float32)
            for slot in range(chips - 1):
                from_far(slot, part, i).wait_recv()
                total = total + far_in[slot, part, i].astype(jnp.float32)
            out_ref[i * size : (i + 1) * size, cols] = total.astype(jnp.bfloat16)

    @pl.loop(0, far_steps)
    def _(t):
        to_mate(t).wait_send()
        to_far(t).wait_send()

    for i in range(each):
        to_home(i).wait_send()


def finish(
    head_size, inner, maps, heads, act, table, local_states, reach, incoming, inside, gate, gain,
    attn_out, attn_weight, ssm_weight,
):
    count = lax.axis_size("tp")
    chips = count // 2
    total, width = attn_out.shape[0], attn_weight.shape[1]
    each = total // count // CHUNK
    far = max(chips - 1, 1)
    steps = far * 2 * each
    depth = attn_weight.shape[0] + ssm_weight.shape[0]
    vmem = pl.BlockSpec(memory_space=pltpu.VMEM)
    dma = pltpu.SemaphoreType.DMA

    def room(*dims):
        return pltpu.VMEM(dims, jnp.bfloat16)

    return pl.pallas_call(
        functools.partial(finish_kernel, head_size, inner, maps, heads, count),
        in_specs=[vmem] * 9 + [pl.BlockSpec(memory_space=pl.ANY)] * 2,
        out_specs=vmem,
        out_shape=jax.ShapeDtypeStruct((total // count, width), jnp.bfloat16),
        scratch_shapes=[
            room(*attn_weight.shape), room(*ssm_weight.shape), room(CHUNK, inner),
            room(2, STATE_SIZE, inner), room(steps, CHUNK, width // 2),
            room(steps, CHUNK, width // 2), room(steps, CHUNK, width // 2),
            room(steps, CHUNK, width // 2), room(far, 2, each, CHUNK, width // 2),
            room(each, CHUNK, width), room(each, CHUNK, width), room(each, CHUNK, width),
            dma((2,)), dma((steps,)), dma((steps,)), dma((steps,)), dma((far, 2, each)),
            dma((each,)), dma((each,)),
        ],
        compiler_params=pltpu.CompilerParams(
            collective_id=3, has_side_effects=True, vmem_limit_bytes=FINISH_MIB * MIB
        ),
        cost_estimate=pl.CostEstimate(
            flops=2 * total * depth * width, bytes_accessed=2 * depth * width, transcendentals=0
        ),
        name="finish",
    )(
        act, table, local_states, reach, incoming, inside, gate, gain, attn_out, attn_weight,
        ssm_weight,
    )


def local(
    tokens,
    norm_gain,
    query_weight,
    key_weight,
    value_weight,
    query_gain,
    key_gain,
    sink_logit,
    gate_weight,
    inner_weight,
    input_map,
    output_map,
    step_weight,
    conv_inner,
    conv_pair,
    decay_rate,
    decay_jump,
    inner_gain,
    attn_out_weight,
    ssm_out_weight,
):
    head_size = query_gain.shape[0]
    query, keyed, rows, gate_rows, table, turned = project_all(
        tokens, norm_gain, inner_weight, input_map, output_map, key_weight, value_weight,
        query_weight, gate_weight, step_weight, query_gain, key_gain, decay_rate, decay_jump,
    )
    tap_count, inner = conv_inner.shape
    maps = input_map.shape[1]
    heads = inner // head_size
    key_heads = key_weight.shape[1] // head_size
    conv_table = jnp.concatenate([conv_inner, conv_pair.reshape(tap_count, -1)], axis=1).astype(
        jnp.float32
    )
    act, local_states, reach, pack_forward, pack_backward, rimmed = convolve(
        rows, keyed, conv_table, table, tap_count, inner, maps, heads
    )
    attn_out, incoming, inside = middle(
        query, rimmed, sink_logit, pack_forward, pack_backward, act, table, turned, head_size,
        key_heads, inner, maps,
    )
    return finish(
        head_size, inner, maps, heads, act, table, local_states, reach, incoming, inside, gate_rows,
        inner_gain.astype(jnp.float32)[None, :], attn_out, attn_out_weight, ssm_out_weight,
    )


def solution(mesh):
    in_specs = (
        P("sp", None),
        P(),
        P(None, "tp"),
        P(None, "tp"),
        P(None, "tp"),
        P(),
        P(),
        P("tp"),
        P(None, "tp"),
        P(None, "tp"),
        P(None, "tp"),
        P(None, "tp"),
        P(None, None, "tp"),
        P(None, "tp"),
        P(None, None, "tp"),
        P(None, "tp"),
        P("sp", None, "tp"),
        P("tp"),
        P("tp", None),
        P("tp", None),
    )
    out_specs = P(("sp", "tp"), None)
    return jax.shard_map(local, mesh=mesh, in_specs=in_specs, out_specs=out_specs, check_vma=False)
```

```python
import functools

import jax
import jax.numpy as jnp
import numpy as np
from jax import lax
from jax.experimental import pallas as pl
from jax.experimental.pallas import tpu as pltpu
from jax.sharding import PartitionSpec as P

STATE_SIZE = 128
WINDOW = 128
CHUNK = 128
HALO = 16

NORM_EPS = 1e-05
ROPE_BASE = 500000.0
NEG_FILL = -1e30
TILE = 512
ROWS = 256
MIB = 1 << 20
PROJECT_MIB = 52
CONVOLVE_MIB = 32
MIDDLE_MIB = 30
FINISH_MIB = 28
PACK_ROWS = 16
MESH = pl.DeviceIdType.MESH


def spread(factor, width):
    heads = factor.shape[1]
    row = lax.broadcasted_iota(jnp.int32, (heads, width), 0)
    column = lax.broadcasted_iota(jnp.int32, (heads, width), 1)
    head_size = width // heads
    ones = jnp.where(
        (column >= row * head_size) & (column < (row + 1) * head_size), 1.0, 0.0
    ).astype(jnp.bfloat16)
    return jnp.dot(factor.astype(jnp.bfloat16), ones, preferred_element_type=jnp.float32)


def exact_dot(a, b):
    return jnp.dot(a, b, precision=lax.Precision.HIGHEST, preferred_element_type=jnp.float32)


def triangle(size, lower):
    row = lax.broadcasted_iota(jnp.int32, (size, size), 0)
    column = lax.broadcasted_iota(jnp.int32, (size, size), 1)
    return jnp.where(row >= column if lower else row <= column, 1.0, 0.0)


def project_kernel(
    head_size, heads, key_width, tokens_ref, inner_hbm, in_hbm, out_hbm, key_hbm, value_hbm,
    query_hbm, gate_hbm, step_hbm, jump_hbm, small_ref,
    waves_ref, query_gain_ref, key_gain_ref, rate_ref, query_ref, keyed_ref, rows_ref, gate_ref,
    table_ref, turned_ref, step_ref, jump_ref, tokens, normed, inner_w, in_w, out_w, keyed_w, query_w, gate_w, raw,
    cosine, sine, token_sems, weight_sems,
):
    total, depth = tokens.shape
    parts = token_sems.shape[0]
    size = total // parts
    moves = [
        pltpu.make_async_copy(
            tokens_ref.at[pl.ds(i * size, size)], tokens.at[pl.ds(i * size, size)],
            token_sems.at[i],
        )
        for i in range(parts)
    ]
    joined = key_width % 128 == 0
    if joined:
        key_w, value_w = keyed_w.at[:, :key_width], keyed_w.at[:, key_width:]
    else:
        key_w, value_w = keyed_w.at[0], keyed_w.at[1]
    weights = (
        (key_hbm, key_w), (value_hbm, value_w), (query_hbm, query_w), (in_hbm, in_w),
        (out_hbm, out_w), (inner_hbm, inner_w), (gate_hbm, gate_w), (step_hbm, step_ref),
        (jump_hbm, jump_ref),
    )
    loads = [
        pltpu.make_async_copy(source, target, weight_sems.at[i])
        for i, (source, target) in enumerate(weights)
    ]
    for move in moves + loads[7:] + loads[:7]:
        move.start()
    lanes = depth // 128
    frequency, sign = waves_ref[0:1], waves_ref[1:2]
    repeats = 128 // head_size
    query_gain = jnp.concatenate([query_gain_ref[...] * head_size ** (-0.5)] * repeats, axis=1)
    key_gain = jnp.concatenate([key_gain_ref[...]] * repeats, axis=1)
    order = lax.broadcasted_iota(jnp.int32, (32, 128), 0)
    first = lax.axis_index("sp") * total
    near = order.astype(jnp.float32) * frequency
    cos_near, sin_near = jnp.cos(near), jnp.sin(near)
    for a in range(0, total, 1024):
        far = (first + a + 32 * order).astype(jnp.float32) * frequency
        cos_far, sin_far = jnp.cos(far), jnp.sin(far)
        for r in range(min(32, (total - a) // 32)):
            c, d = cos_far[r : r + 1], sin_far[r : r + 1]
            span = slice(a + r * 32, a + (r + 1) * 32)
            cosine[span, :] = c * cos_near - d * sin_near
            sine[span, :] = (d * cos_near + c * sin_near) * sign
    for i in range(parts):
        moves[i].wait()

        @pl.loop(0, size // 32)
        def _(r, i=i):
            span = pl.ds(pl.multiple_of(i * size + r * 32, 32), 32)
            squares = jnp.zeros((32, 128), jnp.float32)
            for j in range(lanes):
                x = tokens[span, j * 128 : (j + 1) * 128].astype(jnp.float32)
                squares = squares + x * x
            mean = jnp.sum(squares, axis=-1, keepdims=True) * (1.0 / depth)
            scale = lax.rsqrt(mean + NORM_EPS)
            for j in range(lanes):
                cols = slice(j * 128, (j + 1) * 128)
                x = tokens[span, cols].astype(jnp.float32)
                normed[span, cols] = (x * scale * small_ref[j : j + 1]).astype(jnp.bfloat16)

    def run(weight, target, column, beside=None):
        width = min(weight.shape[1], TILE)
        count = weight.shape[1] // width

        def tile(j):
            at = j * width if count == 1 else pl.multiple_of(j * width, width)
            share = total // count
            for m in range(0, total, ROWS):
                target[m : m + ROWS, pl.ds(column + at, width)] = jnp.dot(
                    normed[m : m + ROWS, :], weight[:, pl.ds(at, width)],
                    preferred_element_type=jnp.float32,
                ).astype(jnp.bfloat16)
                if beside is not None:
                    beside(j * share + m // count, ROWS // count)

        if count == 1:
            tile(0)
        else:
            pl.loop(0, count)(tile)

    loads[7].wait()
    loads[8].wait()
    raw[:, 2 * heads :] = jnp.zeros((total, 128 - 2 * heads), jnp.float32)
    raw[:, : 2 * heads] = lax.dot_general(
        normed[...], step_ref[...], (((1,), (1,)), ((), ())), preferred_element_type=jnp.float32
    ).astype(jnp.bfloat16).astype(jnp.float32)
    rates = jnp.concatenate(
        [rate_ref[0:1], rate_ref[1:2], jnp.zeros((1, 128 - 2 * heads), jnp.float32)], axis=1
    )
    rates = jnp.transpose(jnp.broadcast_to(rates, (128, 128)))
    rates = rates[: 2 * heads, 0:1]
    upper, lower = triangle(CHUNK, False), triangle(CHUNK, True)

    def steps(first_row, length):
        for c in range(length // CHUNK):
            at = pl.multiple_of(first_row + c * CHUNK, CHUNK)
            span = pl.ds(at, CHUNK)
            x = jnp.transpose(raw[span, :])[: 2 * heads]
            step = jnp.maximum(x, 0.0) + jnp.log1p(jnp.exp(-jnp.abs(x)))
            decay = jump_ref[:, span] - rates * step
            filled = jnp.concatenate(
                [
                    exact_dot(decay[:heads], upper), exact_dot(decay[heads:], lower), step,
                    jnp.zeros((128 - 4 * heads, CHUNK), jnp.float32),
                ],
                axis=0,
            )
            turned_ref[:, span] = filled
            table_ref[span, :] = jnp.transpose(filled)

    row = lax.broadcasted_iota(jnp.int32, (256, 128), 0)
    column = lax.broadcasted_iota(jnp.int32, (256, 128), 1)
    same_head = jnp.where(
        lax.rem(row, 128) // head_size == column // head_size, 1.0, 0.0
    ).astype(jnp.bfloat16)
    lane = lax.broadcasted_iota(jnp.int32, (128, 128), 1)
    half = head_size // 2
    first_half = lax.rem(lane, head_size) < half

    def rotate(value, gain_row, cos_here, sin_here):
        square = value * value
        high = square.astype(jnp.bfloat16)
        low = (square - high.astype(jnp.float32)).astype(jnp.bfloat16)
        sums = jnp.dot(
            jnp.concatenate([high, low], axis=1), same_head, preferred_element_type=jnp.float32
        )
        value = value * lax.rsqrt(sums * (1.0 / head_size) + NORM_EPS) * gain_row
        swapped = jnp.where(
            first_half, pltpu.roll(value, 128 - half, 1), pltpu.roll(value, half, 1)
        )
        return (value * cos_here + swapped * sin_here).astype(jnp.bfloat16)

    def heads_of(first_row, length):
        for i in range(length // 128):
            span = pl.ds(pl.multiple_of(first_row + i * 128, 128), 128)
            cos_here, sin_here = cosine[span, :], sine[span, :]
            for at in range(0, query_ref.shape[1], 128):
                value = query_ref[span, at : at + 128].astype(jnp.float32)
                query_ref[span, at : at + 128] = rotate(
                    value, query_gain, cos_here, sin_here
                )
            for at in range(0, key_width, 128):
                packed = keyed_ref[span, at : at + 128]
                keys = rotate(
                    packed.astype(jnp.float32), key_gain, cos_here, sin_here
                )
                keyed_ref[span, at : at + 128] = jnp.where(lane + at < key_width, keys, packed)

    inner, maps = inner_w.shape[1], in_w.shape[1]
    loads[0].wait()
    loads[1].wait()
    if joined:
        run(keyed_w, keyed_ref, 0)
    else:
        run(keyed_w.at[0], keyed_ref, 0)
        run(keyed_w.at[1], keyed_ref, key_width)
    loads[2].wait()
    run(query_w, query_ref, 0)
    loads[3].wait()
    run(in_w, rows_ref, inner)
    loads[4].wait()
    run(out_w, rows_ref, inner + maps)
    loads[5].wait()
    run(inner_w, rows_ref, 0, steps)
    loads[6].wait()
    run(gate_w, gate_ref, 0, heads_of)


def project_all(
    tokens, norm_gain, inner_weight, input_map, output_map, key_weight, value_weight, query_weight,
    gate_weight, step_weight, query_gain, key_gain, decay_rate, decay_jump,
):
    total, depth = tokens.shape
    head_size = query_gain.shape[0]
    half = head_size // 2
    lane = np.arange(128)
    frequency = (ROPE_BASE ** (-2.0 * (lane % half) / head_size)).astype(np.float32)
    sign = np.where(lane % head_size < half, -1.0, 1.0).astype(np.float32)
    waves = jnp.asarray(np.stack([frequency, sign]))
    small = norm_gain.astype(jnp.float32).reshape(-1, 128)
    turned_step = jnp.transpose(step_weight, (1, 2, 0)).reshape(-1, depth)
    turned_jump = jnp.transpose(decay_jump, (1, 2, 0)).reshape(-1, total)
    heads = step_weight.shape[2]
    inner, maps = inner_weight.shape[1], input_map.shape[1]
    width, key_width = query_weight.shape[1], key_weight.shape[1]
    whole = pl.BlockSpec(memory_space=pltpu.HBM)
    vmem = pl.BlockSpec(memory_space=pltpu.VMEM)
    big = (inner_weight, input_map, output_map, key_weight, value_weight, query_weight, gate_weight)
    columns = sum(w.shape[1] for w in big)
    keyed_shape = (depth, 2 * key_width) if key_width % 128 == 0 else (2, depth, key_width)

    def shape(*dims, kind=jnp.bfloat16):
        return jax.ShapeDtypeStruct(dims, kind)

    def room(*dims, kind=jnp.bfloat16):
        return pltpu.VMEM(dims, kind)

    return pl.pallas_call(
        functools.partial(project_kernel, head_size, heads, key_width),
        in_specs=[whole] * 10 + [vmem] * 5,
        out_specs=[vmem] * 6,
        out_shape=[
            shape(total, width), shape(total, 2 * key_width), shape(total, inner + 2 * maps),
            shape(total, inner), shape(total, 128, kind=jnp.float32),
            shape(128, total, kind=jnp.float32),
        ],
        scratch_shapes=[
            room(*turned_step.shape), room(*turned_jump.shape, kind=jnp.float32),
            room(total, depth), room(total, depth), room(*inner_weight.shape),
            room(*input_map.shape), room(*output_map.shape), room(*keyed_shape),
            room(*query_weight.shape), room(*gate_weight.shape),
            room(total, 128, kind=jnp.float32), room(total, 128, kind=jnp.float32),
            room(total, 128, kind=jnp.float32),
            pltpu.SemaphoreType.DMA((8,)), pltpu.SemaphoreType.DMA((9,)),
        ],
        compiler_params=pltpu.CompilerParams(vmem_limit_bytes=PROJECT_MIB * MIB),
        cost_estimate=pl.CostEstimate(
            flops=2 * total * depth * columns, bytes_accessed=2 * depth * (columns + total),
            transcendentals=total * 128,
        ),
        name="project",
    )(
        tokens, *big, turned_step, turned_jump, small, waves, query_gain[None], key_gain[None],
        decay_rate,
    )


def convolve_kernel(
    tap_count, inner, maps, heads, count, rows_ref, keyed_ref, taps_ref, table_ref, act_ref,
    local_ref, reach_ref, packf_ref, packb_ref, rim_ref, freshf_ref, freshb_ref, spare, low_rows, high_rows, low_keys,
    high_keys, endf, endb, sends, receives,
):
    me = lax.axis_index("sp")
    total = rows_ref.shape[0]
    size = CHUNK
    chunks = total // size

    def copies(up):
        device = me + 1 if up else me - 1
        slot = 0 if up else 2
        edge = pl.ds(total - HALO if up else 0, HALO)
        wide = pl.ds(total - WINDOW if up else 0, WINDOW)
        pairs = (
            (rows_ref.at[edge], low_rows if up else high_rows),
            (keyed_ref.at[wide], low_keys if up else high_keys),
        )
        return [
            pltpu.make_async_remote_copy(
                src_ref=source, dst_ref=target, send_sem=sends.at[slot + i],
                recv_sem=receives.at[slot + i], device_id={"sp": device}, device_id_type=MESH,
            )
            for i, (source, target) in enumerate(pairs)
        ]

    barrier = pltpu.get_barrier_semaphore()
    for step in (1, count - 1):
        pl.semaphore_signal(
            barrier, inc=1, device_id={"sp": lax.rem(me + step, count)}, device_id_type=MESH
        )
    pl.semaphore_wait(barrier, 2)
    has_low, has_high = me > 0, me < count - 1

    @pl.when(has_high)
    def _():
        for copy in copies(True):
            copy.start()

    @pl.when(has_low)
    def _():
        for copy in copies(False):
            copy.start()

    @pl.when(jnp.logical_not(has_low))
    def _():
        low_rows[...] = jnp.zeros_like(low_rows)
        low_keys[...] = jnp.zeros_like(low_keys)

    @pl.when(jnp.logical_not(has_high))
    def _():
        high_rows[...] = jnp.zeros_like(high_rows)
        high_keys[...] = jnp.zeros_like(high_keys)

    rim_ref[WINDOW : WINDOW + total, :] = keyed_ref[...]

    @pl.loop(0, chunks)
    def _(turn):
        c = lax.rem(turn + 1, chunks)
        start = pl.multiple_of(c * size, size)
        spare[HALO : HALO + size, :] = rows_ref[pl.ds(start, size), :].astype(jnp.float32)

        @pl.when(turn == chunks - 2)
        def _():
            @pl.when(has_low)
            def _():
                for copy in copies(True):
                    copy.wait_recv()

            @pl.when(has_high)
            def _():
                for copy in copies(False):
                    copy.wait_recv()

        @pl.when(c == 0)
        def _():
            spare[:HALO, :] = low_rows[...].astype(jnp.float32)

        @pl.when(c > 0)
        def _():
            at = pl.multiple_of(start - HALO, HALO)
            spare[:HALO, :] = rows_ref[pl.ds(at, HALO), :].astype(jnp.float32)

        @pl.when(c == chunks - 1)
        def _():
            spare[HALO + size :, :] = high_rows[...].astype(jnp.float32)

        @pl.when(c < chunks - 1)
        def _():
            at = pl.multiple_of(start + size, HALO)
            spare[HALO + size :, :] = rows_ref[pl.ds(at, HALO), :].astype(jnp.float32)

        first = HALO - tap_count // 2
        for at in range(0, inner + 2 * maps, 128):
            cols = slice(at, at + 128)
            filtered = spare[first : first + size, cols] * taps_ref[0:1, cols]
            for k in range(1, tap_count):
                filtered = (
                    filtered + spare[first + k : first + k + size, cols] * taps_ref[k : k + 1, cols]
                )
            act_ref[pl.ds(start, size), cols] = (
                filtered * (1.0 / (1.0 + jnp.exp(-filtered)))
            ).astype(jnp.bfloat16)

    rim_ref[:WINDOW, :] = low_keys[...]
    rim_ref[WINDOW + total :, :] = high_keys[...]
    groups = maps // STATE_SIZE
    width = inner // groups

    @pl.loop(0, chunks)
    def _(c):
        span = pl.ds(pl.multiple_of(c * size, size), size)
        table = table_ref[span, :]
        cumf, cumb = table[:, :heads], table[:, heads : 2 * heads]
        wf = jnp.exp(cumf[size - 1 : size] - cumf) * table[:, 2 * heads : 3 * heads]
        wb = jnp.exp(cumb[0:1] - cumb) * table[:, 3 * heads : 4 * heads]
        signal = act_ref[span, :inner].astype(jnp.float32)
        xf = (signal * spread(wf, inner)).astype(jnp.bfloat16)
        xb = (signal * spread(wb, inner)).astype(jnp.bfloat16)
        for g in range(groups):
            cols = slice(g * width, (g + 1) * width)
            entry = act_ref[span, inner + g * STATE_SIZE : inner + (g + 1) * STATE_SIZE]
            turned = jnp.transpose(entry)
            freshf_ref[c, :, cols] = jnp.dot(turned, xf[:, cols], preferred_element_type=jnp.float32)
            freshb_ref[c, :, cols] = jnp.dot(turned, xb[:, cols], preferred_element_type=jnp.float32)

    endf[...] = jnp.zeros_like(endf)
    endb[...] = jnp.zeros_like(endb)

    def total_decay(c, forward):
        row = c * size + size - 1 if forward else c * size
        at = 0 if forward else heads
        return table_ref[pl.ds(row, 1), :][:, at : at + heads]

    def wide(log_row):
        return spread(jnp.exp(jnp.broadcast_to(log_row, (8, heads))), inner)

    logsf, logsb = jnp.zeros((1, heads), jnp.float32), jnp.zeros((1, heads), jnp.float32)
    for c in range(chunks):
        local_ref[0, c] = endf[...].astype(jnp.bfloat16)
        reach_ref[0, c] = wide(logsf)
        logsf = logsf + total_decay(c, True)
        endf[...] = endf[...] * wide(total_decay(c, True))[0:1] + freshf_ref[c]
        r = chunks - 1 - c
        local_ref[1, r] = endb[...].astype(jnp.bfloat16)
        reach_ref[1, r] = wide(logsb)
        logsb = logsb + total_decay(r, False)
        endb[...] = endb[...] * wide(total_decay(r, False))[0:1] + freshb_ref[r]
    half = inner // 2
    for logs, end, pack_ref in ((logsf, endf, packf_ref), (logsb, endb, packb_ref)):
        decay = wide(logs).astype(jnp.bfloat16)
        for side in range(2):
            cols = slice(side * half, (side + 1) * half)
            pack_ref[side, :STATE_SIZE, :] = end[:, cols].astype(jnp.bfloat16)
            pack_ref[side, STATE_SIZE:, :] = jnp.concatenate([decay, decay], axis=0)[:, cols]

    @pl.when(has_high)
    def _():
        for copy in copies(True):
            copy.wait_send()

    @pl.when(has_low)
    def _():
        for copy in copies(False):
            copy.wait_send()


def middle_kernel(
    head_size, key_heads, count, inner, maps, sink_ref, query_ref, rim_ref, packf_ref, packb_ref,
    act_ref, table_ref, turned_ref, out_ref, enter_ref, inside_ref, scores, raised, bottoms, flipped, turned, bias, mate_in, pair_out, pair_in, gathered,
    reach, back_out, back_in, mate_send, mate_recv, pair_send, pair_recv, back_send, back_recv,
):
    me = lax.axis_index("sp")
    parity = lax.rem(me, 2)
    place = lax.div(me, 2)
    pairs = count // 2
    mate = me + 1 - 2 * parity
    is_even = parity == 0
    packs = (packf_ref, packb_ref)
    states = STATE_SIZE

    def copy(source, target, sends, receives, device):
        return pltpu.make_async_remote_copy(
            src_ref=source, dst_ref=target, send_sem=sends, recv_sem=receives,
            device_id={"sp": device}, device_id_type=MESH,
        )

    def to_mate(d):
        return copy(
            packs[d].at[1 - parity], mate_in.at[d], mate_send.at[d], mate_recv.at[d], mate
        )

    def to_pair(d, k):
        device = me + 2 * k if d == 0 else me - 2 * k
        return copy(
            pair_out.at[d], pair_in.at[d, k - 1], pair_send.at[d, k - 1], pair_recv.at[d, k - 1],
            device,
        )

    def back_to_mate(d):
        return copy(back_out.at[d], back_in.at[d], back_send.at[d], back_recv.at[d], mate)

    def sends_to(d, k):
        return place + k < pairs if d == 0 else place - k >= 0

    def hears_from(d, k):
        return place - k >= 0 if d == 0 else place + k < pairs

    barrier = pltpu.get_barrier_semaphore()
    pl.semaphore_signal(barrier, inc=1, device_id={"sp": mate}, device_id_type=MESH)
    for k in range(1, pairs):
        other = lax.rem(me + 2 * k, count)
        pl.semaphore_signal(barrier, inc=1, device_id={"sp": other}, device_id_type=MESH)
    pl.semaphore_wait(barrier, pairs)
    for d in range(2):
        to_mate(d).start()

    def even_and_odd(d):
        own, other = packs[d][parity].astype(jnp.float32), mate_in[d].astype(jnp.float32)
        return jnp.where(is_even, own, other), jnp.where(is_even, other, own)

    def join_pair():
        for d in range(2):
            to_mate(d).wait_recv()
            even, odd = even_and_odd(d)
            near, far = (odd, even) if d == 0 else (even, odd)
            decay = near[states : states + 1]
            pair_out[d, :states, :] = (near[:states] + decay * far[:states]).astype(jnp.bfloat16)
            pair_out[d, states:, :] = (near[states:] * far[states:]).astype(jnp.bfloat16)
        for k in range(1, pairs):
            for d in range(2):
                @pl.when(sends_to(d, k))
                def _(d=d, k=k):
                    to_pair(d, k).start()

    def join_all():
        gathered[...] = jnp.zeros_like(gathered)
        reach[...] = jnp.ones_like(reach)
        for k in range(1, pairs):
            for d in range(2):
                @pl.when(hears_from(d, k))
                def _(d=d, k=k):
                    to_pair(d, k).wait_recv()
                    came = pair_in[d, k - 1].astype(jnp.float32)
                    gathered[d] = gathered[d] + reach[d, 0:1] * came[:states]
                    reach[d] = reach[d] * came[states : states + 8]
        for d in range(2):
            even, odd = even_and_odd(d)
            base = even if d == 0 else odd
            plain = gathered[d]
            moved = base[:states] + base[states : states + 1] * plain
            plain_is_mine = is_even if d == 0 else jnp.logical_not(is_even)
            enter_ref[d, parity] = jnp.where(plain_is_mine, plain, moved)
            back_out[d] = jnp.where(plain_is_mine, moved, plain).astype(jnp.bfloat16)
            back_to_mate(d).start()

    rows, block = query_ref.shape[0], WINDOW
    span = block + 2 * WINDOW
    blocks = rows // block
    heads = query_ref.shape[1] // head_size
    ratio = heads // key_heads
    values_at = key_heads * head_size
    flipped[...] = jnp.transpose(rim_ref[:, values_at:])
    key_row = lax.broadcasted_iota(jnp.int32, (span, block), 0)
    query_col = lax.broadcasted_iota(jnp.int32, (span, block), 1)
    in_band = (key_row >= query_col) & (key_row <= query_col + 2 * WINDOW)

    groups = maps // STATE_SIZE
    ssm_heads = inner // head_size
    chunk_row = lax.broadcasted_iota(jnp.int32, (CHUNK, CHUNK), 0)
    chunk_col = lax.broadcasted_iota(jnp.int32, (CHUNK, CHUNK), 1)
    is_lower, is_diagonal = chunk_row >= chunk_col, chunk_row == chunk_col
    lane = lax.broadcasted_iota(jnp.int32, (CHUNK, 2 * head_size), 1)

    def inside_chunk(c):
        at = pl.multiple_of(c * CHUNK, CHUNK)
        span = pl.ds(at, CHUNK)
        table = table_ref[span, :]
        for g in range(groups):
            entry = act_ref[span, inner + g * STATE_SIZE : inner + (g + 1) * STATE_SIZE]
            leave = act_ref[
                span, inner + maps + g * STATE_SIZE : inner + maps + (g + 1) * STATE_SIZE
            ]
            crossed = lax.dot_general(
                leave, entry, (((1,), (1,)), ((), ())), preferred_element_type=jnp.float32
            )
            each = ssm_heads // groups
            for pair in range(each // 2):
                mats = []
                base = g * each + 2 * pair
                for h in (base, base + 1):
                    low, high = h, ssm_heads + h
                    gap = jnp.where(
                        is_lower,
                        table[:, low : low + 1] - turned_ref[low : low + 1, span],
                        table[:, high : high + 1] - turned_ref[high : high + 1, span],
                    )
                    sf = turned_ref[2 * ssm_heads + h : 2 * ssm_heads + h + 1, span]
                    sb = turned_ref[3 * ssm_heads + h : 3 * ssm_heads + h + 1, span]
                    amount = jnp.where(is_diagonal, sf + sb, jnp.where(is_lower, sf, sb))
                    mats.append((crossed * jnp.exp(gap) * amount).astype(jnp.bfloat16))
                two = slice(base * head_size, (base + 2) * head_size)
                x = act_ref[span, two]
                zero = jnp.zeros_like(x)
                stacked = jnp.concatenate(
                    [jnp.where(lane < head_size, x, zero), jnp.where(lane < head_size, zero, x)],
                    axis=0,
                )
                inside_ref[span, two] = jnp.dot(
                    jnp.concatenate(mats, axis=1), stacked, preferred_element_type=jnp.float32
                )

    @pl.loop(0, blocks)
    def _(step):
        inside_chunk(step)

        @pl.when(step == (3 * blocks) // 8)
        def _():
            join_pair()

        @pl.when(step == (7 * blocks) // 8)
        def _():
            join_all()

        start = pl.multiple_of(step * block, block)
        position = me * rows + start - WINDOW + key_row
        bias[...] = jnp.where(
            in_band & (position >= 0) & (position < count * rows), 0.0, NEG_FILL
        )
        tops = []
        for h in range(heads):
            k = h // ratio
            scores[h] = lax.dot_general(
                rim_ref[pl.ds(start, span), k * head_size : (k + 1) * head_size],
                query_ref[pl.ds(start, block), h * head_size : (h + 1) * head_size],
                (((1,), (1,)), ((), ())), preferred_element_type=jnp.float32,
            ) + bias[...]
        for h in range(heads):
            top = jnp.maximum(jnp.max(scores[h], axis=0, keepdims=True), sink_ref[h])
            lifted = jnp.exp(scores[h] - top)
            bottoms[h : h + 1] = jnp.sum(lifted, axis=0, keepdims=True) + jnp.exp(sink_ref[h] - top)
            raised[h] = lifted.astype(jnp.bfloat16)
        for h in range(heads):
            k = h // ratio
            turned[h * head_size : (h + 1) * head_size, :] = jnp.dot(
                flipped[k * head_size : (k + 1) * head_size, pl.ds(start, span)], raised[h],
                preferred_element_type=jnp.float32,
            ) * (1.0 / bottoms[h : h + 1])
        out_ref[pl.ds(start, block), :] = jnp.transpose(turned[...]).astype(jnp.bfloat16)

    for d in range(2):
        back_to_mate(d).wait_recv()
        enter_ref[d, 1 - parity] = back_in[d].astype(jnp.float32)
    for d in range(2):
        to_mate(d).wait_send()
        back_to_mate(d).wait_send()
        for k in range(1, pairs):
            @pl.when(sends_to(d, k))
            def _(d=d, k=k):
                to_pair(d, k).wait_send()


def middle(
    query, rimmed, sink_logit, pack_forward, pack_backward, act, table, turned, head_size, key_heads,
    inner, maps,
):
    rows, width = query.shape
    heads = width // head_size
    count = lax.axis_size("sp")
    hops = max(count // 2 - 1, 1)
    _, depth, half = pack_forward.shape
    span = 3 * WINDOW
    vmem = pl.BlockSpec(memory_space=pltpu.VMEM)
    dma = pltpu.SemaphoreType.DMA
    return pl.pallas_call(
        functools.partial(middle_kernel, head_size, key_heads, count, inner, maps),
        in_specs=[pl.BlockSpec(memory_space=pltpu.SMEM)] + [vmem] * 7,
        out_specs=[vmem] * 3,
        out_shape=[
            jax.ShapeDtypeStruct((rows, width), jnp.bfloat16),
            jax.ShapeDtypeStruct((2, 2, STATE_SIZE, half), jnp.float32),
            jax.ShapeDtypeStruct((rows, inner), jnp.float32),
        ],
        scratch_shapes=[
            pltpu.VMEM((heads, span, WINDOW), jnp.float32),
            pltpu.VMEM((heads, span, WINDOW), jnp.bfloat16),
            pltpu.VMEM((heads, WINDOW), jnp.float32),
            pltpu.VMEM((key_heads * head_size, rimmed.shape[0]), jnp.bfloat16),
            pltpu.VMEM((width, WINDOW), jnp.float32),
            pltpu.VMEM((span, WINDOW), jnp.float32),
            pltpu.VMEM((2, depth, half), jnp.bfloat16),
            pltpu.VMEM((2, depth, half), jnp.bfloat16),
            pltpu.VMEM((2, hops, depth, half), jnp.bfloat16),
            pltpu.VMEM((2, STATE_SIZE, half), jnp.float32),
            pltpu.VMEM((2, 8, half), jnp.float32),
            pltpu.VMEM((2, STATE_SIZE, half), jnp.bfloat16),
            pltpu.VMEM((2, STATE_SIZE, half), jnp.bfloat16),
            dma((2,)), dma((2,)), dma((2, hops)), dma((2, hops)), dma((2,)), dma((2,)),
        ],
        compiler_params=pltpu.CompilerParams(
            collective_id=5, has_side_effects=True, vmem_limit_bytes=MIDDLE_MIB * MIB
        ),
        cost_estimate=pl.CostEstimate(
            flops=4 * rows * span * width, bytes_accessed=4 * rows * width,
            transcendentals=rows * span * heads,
        ),
        name="middle",
    )(sink_logit, query, rimmed, pack_forward, pack_backward, act, table, turned)


def convolve(rows, keyed, taps, table, tap_count, inner, maps, heads):
    total, width = rows.shape
    chunks = total // CHUNK
    count = lax.axis_size("sp")
    vmem = pl.BlockSpec(memory_space=pltpu.VMEM)
    local_shape = jax.ShapeDtypeStruct((2, chunks, STATE_SIZE, inner), jnp.bfloat16)
    reach_shape = jax.ShapeDtypeStruct((2, chunks, 8, inner), jnp.float32)
    pack = jax.ShapeDtypeStruct((2, STATE_SIZE + PACK_ROWS, inner // 2), jnp.bfloat16)
    return pl.pallas_call(
        functools.partial(convolve_kernel, tap_count, inner, maps, heads, count),
        in_specs=[vmem] * 4,
        out_specs=[vmem] * 6,
        out_shape=[
            jax.ShapeDtypeStruct((total, width), jnp.bfloat16), local_shape, reach_shape, pack, pack,
            jax.ShapeDtypeStruct((total + 2 * WINDOW, keyed.shape[1]), jnp.bfloat16),
        ],
        scratch_shapes=[
            pltpu.VMEM((chunks, STATE_SIZE, inner), jnp.float32),
            pltpu.VMEM((chunks, STATE_SIZE, inner), jnp.float32),
            pltpu.VMEM((CHUNK + 2 * HALO, width), jnp.float32),
            pltpu.VMEM((HALO, width), jnp.bfloat16),
            pltpu.VMEM((HALO, width), jnp.bfloat16),
            pltpu.VMEM((WINDOW, keyed.shape[1]), jnp.bfloat16),
            pltpu.VMEM((WINDOW, keyed.shape[1]), jnp.bfloat16),
            pltpu.VMEM((STATE_SIZE, inner), jnp.float32),
            pltpu.VMEM((STATE_SIZE, inner), jnp.float32),
            pltpu.SemaphoreType.DMA((4,)),
            pltpu.SemaphoreType.DMA((4,)),
        ],
        compiler_params=pltpu.CompilerParams(
            collective_id=4, has_side_effects=True, vmem_limit_bytes=CONVOLVE_MIB * MIB
        ),
        cost_estimate=pl.CostEstimate(
            flops=8 * total * inner * STATE_SIZE, bytes_accessed=8 * total * inner,
            transcendentals=total * width,
        ),
        name="convolve",
    )(rows, keyed, taps, table)


def finish_kernel(
    head_size, inner, maps, heads, count, act_ref, table_ref, local_ref, reach_ref, enter_ref,
    inside_ref, gate_ref, gain_ref, attn_ref, attn_hbm, ssm_hbm, out_ref, attn_w, ssm_w, ssm,
    carries, own, mate_out, mate_in, far_out, far_in, home, home_out, home_in, load_sems, mate_send,
    mate_recv, far_send, far_recv, home_send, home_recv,
):
    loads = [
        pltpu.make_async_copy(attn_hbm, attn_w, load_sems.at[0]),
        pltpu.make_async_copy(ssm_hbm, ssm_w, load_sems.at[1]),
    ]
    for load in loads:
        load.start()
    me = lax.axis_index("tp")
    core = lax.rem(me, 2)
    chip = lax.div(me, 2)
    chips = count // 2
    mate = me + 1 - 2 * core
    size = CHUNK
    wide = ssm_w.shape[1]
    side = wide // 2
    each = home.shape[0]
    per_chip = 2 * each
    far_steps = (chips - 1) * per_chip
    groups = maps // STATE_SIZE
    width = inner // groups
    half = inner // 2

    def chip_of(slot):
        return lax.rem(chip + 1 + slot, chips)

    def remote(source, target, sends, receives, device):
        return pltpu.make_async_remote_copy(
            src_ref=source, dst_ref=target, send_sem=sends, recv_sem=receives,
            device_id={"tp": device}, device_id_type=MESH,
        )

    def to_mate(t):
        return remote(mate_out.at[t], mate_in.at[t], mate_send.at[t], mate_recv.at[t], mate)

    def to_far(t):
        slot, i = lax.div(t, per_chip), lax.rem(t, per_chip)
        owner, at = lax.div(i, each), lax.rem(i, each)
        return remote(
            far_out.at[t], far_in.at[slot, core, at], far_send.at[t], far_recv.at[slot, core, at],
            2 * chip_of(slot) + owner,
        )

    def from_far(slot, part, at):
        return remote(
            far_out.at[0], far_in.at[slot, part, at], far_send.at[0], far_recv.at[slot, part, at],
            mate,
        )

    def to_home(i):
        return remote(home_out.at[i], home_in.at[i], home_send.at[i], home_recv.at[i], mate)

    barrier = pltpu.get_barrier_semaphore()
    pl.semaphore_signal(barrier, inc=1, device_id={"tp": mate}, device_id_type=MESH)
    for slot in range(chips - 1):
        for other in range(2):
            pl.semaphore_signal(
                barrier, inc=1, device_id={"tp": 2 * chip_of(slot) + other}, device_id_type=MESH
            )
    pl.semaphore_wait(barrier, 1 + 2 * (chips - 1))

    def rows_of(c):
        span = pl.ds(pl.multiple_of(c * size, size), size)
        for d in range(2):
            for part in range(2):
                cols = slice(part * half, (part + 1) * half)
                carries[d, :, cols] = (
                    local_ref[d, c, :, cols].astype(jnp.float32)
                    + reach_ref[d, c, 0:1, cols] * enter_ref[d, part]
                ).astype(jnp.bfloat16)
        table = table_ref[span, :]
        expf = spread(jnp.exp(table[:, :heads]), inner)
        expb = spread(jnp.exp(table[:, heads : 2 * heads]), inner)
        for g in range(groups):
            cols = slice(g * width, (g + 1) * width)
            first = inner + maps + g * STATE_SIZE
            leave = act_ref[span, first : first + STATE_SIZE]
            y = (
                inside_ref[span, cols]
                + jnp.dot(leave, carries[0, :, cols], preferred_element_type=jnp.float32)
                * expf[:, cols]
                + jnp.dot(leave, carries[1, :, cols], preferred_element_type=jnp.float32)
                * expb[:, cols]
            )
            gate = gate_ref[span, cols].astype(jnp.float32)
            mixed = y * (gate * (1.0 / (1.0 + jnp.exp(-gate))))
            scale = lax.rsqrt(jnp.mean(mixed * mixed, axis=1, keepdims=True) + NORM_EPS)
            ssm[:, cols] = (mixed * scale * gain_ref[:, cols]).astype(jnp.bfloat16)
        return span

    def product(span, cols):
        return (
            jnp.dot(attn_ref[span, :], attn_w[:, cols], preferred_element_type=jnp.float32)
            + jnp.dot(ssm[...], ssm_w[:, cols], preferred_element_type=jnp.float32)
        ).astype(jnp.bfloat16)

    def forward(t):
        to_mate(t).wait_recv()
        far_out[t] = (own[t].astype(jnp.float32) + mate_in[t].astype(jnp.float32)).astype(
            jnp.bfloat16
        )
        to_far(t).start()

    for load in loads:
        load.wait()

    @pl.loop(0, far_steps)
    def _(t):
        slot, i = lax.div(t, per_chip), lax.rem(t, per_chip)
        span = rows_of(chip_of(slot) * per_chip + i)
        mate_out[t] = product(span, pl.ds(pl.multiple_of((1 - core) * side, side), side))
        to_mate(t).start()
        own[t] = product(span, pl.ds(pl.multiple_of(core * side, side), side))

        @pl.when(t > 0)
        def _():
            forward(t - 1)

    @pl.loop(0, per_chip)
    def _(u):
        i = lax.rem(u, each)
        owner = jnp.where(u < each, 1 - core, core)
        span = rows_of((2 * chip + owner) * each + i)
        for part in range(2):
            cols = slice(part * side, (part + 1) * side)
            home[i, :, cols] = product(span, cols)

        if far_steps > 0:
            @pl.when(u == 0)
            def _():
                forward(far_steps - 1)

        @pl.when(u < each)
        def _():
            home_out[i] = home[i]
            to_home(i).start()

    for i in range(each):
        to_home(i).wait_recv()
        for part in range(2):
            cols = slice(part * side, (part + 1) * side)
            total = home[i, :, cols].astype(jnp.float32) + home_in[i, :, cols].astype(jnp.float32)
            for slot in range(chips - 1):
                from_far(slot, part, i).wait_recv()
                total = total + far_in[slot, part, i].astype(jnp.float32)
            out_ref[i * size : (i + 1) * size, cols] = total.astype(jnp.bfloat16)

    @pl.loop(0, far_steps)
    def _(t):
        to_mate(t).wait_send()
        to_far(t).wait_send()

    for i in range(each):
        to_home(i).wait_send()


def finish(
    head_size, inner, maps, heads, act, table, local_states, reach, incoming, inside, gate, gain,
    attn_out, attn_weight, ssm_weight,
):
    count = lax.axis_size("tp")
    chips = count // 2
    total, width = attn_out.shape[0], attn_weight.shape[1]
    each = total // count // CHUNK
    far = max(chips - 1, 1)
    steps = far * 2 * each
    depth = attn_weight.shape[0] + ssm_weight.shape[0]
    vmem = pl.BlockSpec(memory_space=pltpu.VMEM)
    dma = pltpu.SemaphoreType.DMA

    def room(*dims):
        return pltpu.VMEM(dims, jnp.bfloat16)

    return pl.pallas_call(
        functools.partial(finish_kernel, head_size, inner, maps, heads, count),
        in_specs=[vmem] * 9 + [pl.BlockSpec(memory_space=pl.ANY)] * 2,
        out_specs=vmem,
        out_shape=jax.ShapeDtypeStruct((total // count, width), jnp.bfloat16),
        scratch_shapes=[
            room(*attn_weight.shape), room(*ssm_weight.shape), room(CHUNK, inner),
            room(2, STATE_SIZE, inner), room(steps, CHUNK, width // 2),
            room(steps, CHUNK, width // 2), room(steps, CHUNK, width // 2),
            room(steps, CHUNK, width // 2), room(far, 2, each, CHUNK, width // 2),
            room(each, CHUNK, width), room(each, CHUNK, width), room(each, CHUNK, width),
            dma((2,)), dma((steps,)), dma((steps,)), dma((steps,)), dma((far, 2, each)),
            dma((each,)), dma((each,)),
        ],
        compiler_params=pltpu.CompilerParams(
            collective_id=3, has_side_effects=True, vmem_limit_bytes=FINISH_MIB * MIB
        ),
        cost_estimate=pl.CostEstimate(
            flops=2 * total * depth * width, bytes_accessed=2 * depth * width, transcendentals=0
        ),
        name="finish",
    )(
        act, table, local_states, reach, incoming, inside, gate, gain, attn_out, attn_weight,
        ssm_weight,
    )


def local(
    tokens,
    norm_gain,
    query_weight,
    key_weight,
    value_weight,
    query_gain,
    key_gain,
    sink_logit,
    gate_weight,
    inner_weight,
    input_map,
    output_map,
    step_weight,
    conv_inner,
    conv_pair,
    decay_rate,
    decay_jump,
    inner_gain,
    attn_out_weight,
    ssm_out_weight,
):
    head_size = query_gain.shape[0]
    query, keyed, rows, gate_rows, table, turned = project_all(
        tokens, norm_gain, inner_weight, input_map, output_map, key_weight, value_weight,
        query_weight, gate_weight, step_weight, query_gain, key_gain, decay_rate, decay_jump,
    )
    tap_count, inner = conv_inner.shape
    maps = input_map.shape[1]
    heads = inner // head_size
    key_heads = key_weight.shape[1] // head_size
    conv_table = jnp.concatenate([conv_inner, conv_pair.reshape(tap_count, -1)], axis=1).astype(
        jnp.float32
    )
    act, local_states, reach, pack_forward, pack_backward, rimmed = convolve(
        rows, keyed, conv_table, table, tap_count, inner, maps, heads
    )
    attn_out, incoming, inside = middle(
        query, rimmed, sink_logit, pack_forward, pack_backward, act, table, turned, head_size,
        key_heads, inner, maps,
    )
    return finish(
        head_size, inner, maps, heads, act, table, local_states, reach, incoming, inside, gate_rows,
        inner_gain.astype(jnp.float32)[None, :], attn_out, attn_out_weight, ssm_out_weight,
    )


def solution(mesh):
    in_specs = (
        P("sp", None),
        P(),
        P(None, "tp"),
        P(None, "tp"),
        P(None, "tp"),
        P(),
        P(),
        P("tp"),
        P(None, "tp"),
        P(None, "tp"),
        P(None, "tp"),
        P(None, "tp"),
        P(None, None, "tp"),
        P(None, "tp"),
        P(None, None, "tp"),
        P(None, "tp"),
        P("sp", None, "tp"),
        P("tp"),
        P("tp", None),
        P("tp", None),
    )
    out_specs = P(("sp", "tp"), None)
    return jax.shard_map(local, mesh=mesh, in_specs=in_specs, out_specs=out_specs, check_vma=False)
```
